512 devices in a mesh: tp: 64 (over z, y), dp: 8 (over x, core).
Axes of the slice: x: 4, y: 4, z: 16, core: 2. Of those that a mesh axis runs over, the one named last changes fastest.
Arguments:
- tokens: bfloat16 [192, 4096], P('tp', 'dp'), may hold values from -6 to 6
- lengths: int32 [48], P('dp'), may hold values from 1 to 4, 84 in all
- norm_gain: float32 [2, 4096], P(None, 'dp'), may hold values from 0.1 to 1.9
- gate_weight: bfloat16 [2, 4096, 8192], P(None, 'dp', 'tp'), may hold values from -0.09375 to 0.09375
- value_weight: bfloat16 [2, 4096, 8192], P(None, 'dp', 'tp'), may hold values from -0.09375 to 0.09375
- vector_weight: bfloat16 [2, 4096, 2, 2048], P(None, 'dp', None, 'tp'), may hold values from -0.09375 to 0.09375
- step_weight: bfloat16 [2, 4096, 128], P(None, 'dp'), may hold values from -0.09375 to 0.09375
- step_bias: float32 [2, 128], P(None, 'tp'), may hold values from -3 to 0
- decay_rate: float32 [2, 128], P(None, 'tp'), may hold values from 0.003 to 1
- value_taps: bfloat16 [2, 4, 8192], P(None, None, 'tp'), may hold values from -3 to 3
- vector_taps: bfloat16 [2, 4, 2, 2048], P(None, None, None, 'tp'), may hold values from -3 to 3
- out_weight: bfloat16 [2, 8192, 4096], P(None, 'tp', 'dp'), may hold values from -0.0625 to 0.0625
- recurrent_state: float32 [2, 48, 128, 64, 128], P(None, 'dp', 'tp'), may hold values from -4 to 4
- value_history: bfloat16 [2, 48, 3, 8192], P(None, 'dp', None, 'tp'), may hold values from -6 to 6
- vector_history: bfloat16 [2, 48, 3, 2, 2048], P(None, 'dp', None, None, 'tp'), may hold values from -6 to 6
Outputs:
- next_tokens: bfloat16 [192, 4096], P('tp', 'dp')
- next_state: float32 [2, 48, 128, 64, 128], P(None, 'dp', 'tp')
- next_value_history: bfloat16 [2, 48, 3, 8192], P(None, 'dp', None, 'tp')
- next_vector_history: bfloat16 [2, 48, 3, 2, 2048], P(None, 'dp', None, None, 'tp')
The draws below stay inside these ranges and needn't reach their ends.
Inputs may be any that keep to these rules, and one draw needn't show every extreme that they name: `lengths`: the number of live new tokens of each sequence; some sequences have more than twice the mean.
All inputs are finite; a program needn't handle non-finite values. No bound on the sum of `lengths` on one device may be relied on, other than what follows from the above.
Results may differ from the reference program's by a relative error of at most 0.029.
Values may be sent and summed in bfloat16 or wider, within the bound.
No kernel may reach another device: no remote copies, remote signals or barrier semaphores. Data moves between devices by JAX's collectives and lax.ppermute only.
A program may use at most 64 MiB of HBM per device.

```python
import math
import jax
import jax.numpy as jnp
import numpy as np
from jax import lax

D = 4096
HEADS = 128
HEAD_DIM = 64
STATE = 128
GROUPS = 16
CONV = 4
NEW = 4
LAYERS = 2
SEQS = 48
TOKENS = 192


def steps_of(rng, shape, shards, least, top_value):
    loudness, own = 1.0, jax.random.fold_in(rng, 6)
    for position, shards_of in shards:
        draws = jnp.exp(jax.random.uniform(jax.random.fold_in(own, position), (shards_of,), jnp.float32, least / len(shards), top_value / len(shards)))
        loudness = loudness * jnp.repeat(draws, shape[position] // shards_of).reshape([-1 if axis == position else 1 for axis in range(len(shape))])
    return loudness


def length_profile(amount, total, reach, slope):
    weights = [(1 << 20) // math.isqrt(grade ** slope) + 1 for grade in range(2, amount + 1)]
    spare, counts = total - reach - (amount - 1), [1] * (amount - 1)
    while spare > 0:
        movable = [i for i in range(amount - 1) if counts[i] < reach]
        pool, budget = sum([weights[i] for i in movable]), spare
        for i in movable:
            addition = min(reach - counts[i], max(1, budget * weights[i] // pool), spare)
            counts[i] = counts[i] + addition
            spare = spare - addition
    return np.array([reach] + counts)


def ragged(own_key, number_of, total, reach, lean):
    if number_of == 2:
        one = jax.random.randint(own_key, (), max(1, total - reach), min(reach, total - 1) + 1)
        return jnp.stack([one, total - one])
    sizes = jnp.asarray(length_profile(number_of, total, reach, lean), jnp.int32)
    couples = (number_of - 1) // 2
    donor, receiver = sizes[1:1 + 2 * couples:2], sizes[2:2 + 2 * couples:2]
    slack = jnp.minimum(donor - 1, reach - receiver)
    passed = jax.random.randint(jax.random.fold_in(own_key, 1), (couples,), 0, 1 << 20) % (slack + 1)
    sizes = sizes.at[1:1 + 2 * couples:2].set(donor - passed).at[2:2 + 2 * couples:2].set(receiver + passed)
    return sizes[jax.random.permutation(jax.random.fold_in(own_key, 2), number_of)]


def scatter_about(key, extent, deviation, most, shards=(), kind=jnp.bfloat16):
    values = jax.random.normal(key, extent, jnp.float32) * deviation
    if len(shards) > 0:
        values = steps_of(key, extent, shards, -0.22, 0.18) * values
    return jnp.clip(values, min=-most, max=most).astype(kind)


def setup_inputs(seed: int = 0) -> dict:
    arg_keys = jax.random.split(jax.random.key(seed), 16)
    return {
        "tokens": scatter_about(arg_keys[0], (TOKENS, D), 1.0, 6.0, ((0, 64), (1, 8))),
        "lengths": ragged(arg_keys[1], SEQS, max(7 * SEQS // 4, SEQS + NEW - 1), NEW, 2).astype(jnp.int32),
        "norm_gain": jnp.clip(1.0 + 0.18 * jax.random.normal(arg_keys[2], (LAYERS, D), jnp.float32), 0.1, 1.9),
        "gate_weight": scatter_about(arg_keys[3], (LAYERS, D, HEADS * HEAD_DIM), D ** -0.5, 0.09375, ((1, 8), (2, 64))),
        "value_weight": scatter_about(arg_keys[4], (LAYERS, D, HEADS * HEAD_DIM), D ** -0.5, 0.09375, ((1, 8), (2, 64))),
        "vector_weight": scatter_about(arg_keys[5], (LAYERS, D, 2, GROUPS * STATE), D ** -0.5, 0.09375, ((1, 8), (3, 64))),
        "step_weight": scatter_about(arg_keys[6], (LAYERS, D, HEADS), D ** -0.5, 0.09375, ((1, 8),)),
        "step_bias": jnp.clip(-3.0 + 3.0 * jax.random.uniform(arg_keys[7], (LAYERS, HEADS), jnp.float32) ** steps_of(arg_keys[7], (LAYERS, HEADS), ((1, 64),), -0.2, 0.2), -3.0, 0.0),
        "decay_rate": jnp.clip(jnp.exp(math.log(1.0) - 5.809143 * jax.random.uniform(arg_keys[8], (LAYERS, HEADS), jnp.float32) ** steps_of(arg_keys[8], (LAYERS, HEADS), ((1, 64),), -0.2, 0.2)), 0.003, 1.0),
        "value_taps": scatter_about(arg_keys[9], (LAYERS, CONV, HEADS * HEAD_DIM), 0.5, 3.0, ((2, 64),)),
        "vector_taps": scatter_about(arg_keys[10], (LAYERS, CONV, 2, GROUPS * STATE), 0.5, 3.0, ((3, 64),)),
        "out_weight": scatter_about(arg_keys[11], (LAYERS, HEADS * HEAD_DIM, D), (HEADS * HEAD_DIM) ** -0.5, 0.0625, ((1, 64), (2, 8))),
        "recurrent_state": scatter_about(arg_keys[12], (LAYERS, SEQS, HEADS, HEAD_DIM, STATE), 0.5, 4.0, ((1, 8), (2, 64)), jnp.float32),
        "value_history": scatter_about(arg_keys[13], (LAYERS, SEQS, CONV - 1, HEADS * HEAD_DIM), 1.0, 6.0, ((1, 8), (3, 64))),
        "vector_history": scatter_about(arg_keys[14], (LAYERS, SEQS, CONV - 1, 2, GROUPS * STATE), 1.0, 6.0, ((1, 8), (4, 64))),
    }


norm_floor = 0.1
highest = lax.Precision.HIGHEST

def short_conv(history, fresh_rows, conv_taps):
    padded = jnp.concatenate([history, fresh_rows], axis=1)
    block_len = fresh_rows.shape[1]
    summed = jnp.zeros(fresh_rows.shape, jnp.float32)
    for offset in range(conv_taps.shape[0]):
        summed = summed + padded[:, offset:offset + block_len].astype(jnp.float32) * conv_taps[offset].astype(jnp.float32)
    return (jax.nn.silu(summed), padded)

def state_block(values, write_vec, read_vec, step_sizes, rate_vec, carried_state):
    block_len = values.shape[1]
    cumulative = jnp.cumsum(step_sizes * rate_vec, axis=1)
    causal = jnp.tril(jnp.ones((block_len, block_len), dtype=bool))[None, :, :, None, None]
    log_gap = cumulative[:, :, None] - cumulative[:, None, :]
    decays = jnp.where(causal, jnp.exp(-jnp.where(causal, log_gap, 0.0)), 0.0)
    scores = jnp.einsum('stgn,sugn->stug', read_vec, write_vec, precision=highest)
    weights = scores[..., None] * decays * step_sizes[:, None]
    within = jnp.einsum('stugr,sugrp->stgrp', weights, values, precision=highest)
    carried = jnp.einsum('stgn,sgrpn->stgrp', read_vec, carried_state, precision=highest) * jnp.exp(-cumulative)[..., None]
    ending = jnp.exp(cumulative - cumulative[:, -1:]) * step_sizes
    weighted = values * ending[..., None]
    fresh_state = jnp.einsum('sugrp,sugn->sgrpn', weighted, write_vec, precision=highest)
    next_state = carried_state * jnp.exp(-cumulative[:, -1])[..., None, None] + fresh_state
    return (within + carried, next_state)

def mixer_block(tokens, lengths, gain, gate_weight, value_weight, vector_weight, step_weight, step_bias, decay_rate, value_taps, vector_taps, out_weight, recurrent_state, value_history, vector_history):
    seq_count = lengths.shape[0]
    widened = tokens.astype(jnp.float32)
    scaling = lax.rsqrt(lax.optimization_barrier(jnp.mean(widened * widened, axis=1, keepdims=True)) + norm_floor)
    normed = (widened * gain).astype(jnp.bfloat16)

    def project(weight):
        return (jnp.dot(normed, weight, preferred_element_type=jnp.float32) * scaling).astype(jnp.bfloat16)
    gate = project(gate_weight)
    value_in = project(value_weight)
    vector_in = project(vector_weight.reshape(vector_weight.shape[0], -1))
    step_in = project(step_weight)
    live_mask = (jnp.arange(NEW, dtype=jnp.int32)[None, :] < lengths[:, None]).astype(jnp.float32)
    head_count = step_bias.shape[0]
    group_count = vector_weight.shape[2] // STATE
    per_group = head_count // group_count
    step_sizes = jax.nn.softplus(step_in.astype(jnp.float32).reshape(seq_count, NEW, head_count) + step_bias) * live_mask[:, :, None]
    value_conv, padded_value = short_conv(value_history, value_in.reshape(seq_count, NEW, -1), value_taps)
    vector_conv, padded_vector = short_conv(vector_history, vector_in.reshape(seq_count, NEW, 2, -1), vector_taps)
    write_vec = jnp.swapaxes(vector_conv[:, :, 0].reshape(seq_count, NEW, STATE, group_count), 2, 3)
    read_vec = jnp.swapaxes(vector_conv[:, :, 1].reshape(seq_count, NEW, STATE, group_count), 2, 3)
    output, next_state = state_block(value_conv.reshape(seq_count, NEW, group_count, per_group, HEAD_DIM), write_vec, read_vec, step_sizes.reshape(seq_count, NEW, group_count, per_group), decay_rate.reshape(group_count, per_group), recurrent_state.reshape(seq_count, group_count, per_group, HEAD_DIM, STATE))
    gated = output.reshape(seq_count, NEW, -1) * jax.nn.silu(gate.astype(jnp.float32).reshape(seq_count, NEW, -1)) * live_mask[:, :, None]
    mixed = gated.reshape(seq_count * NEW, -1).astype(jnp.bfloat16)
    update = jnp.dot(mixed, out_weight, preferred_element_type=jnp.float32)
    block_out = (widened + update).astype(jnp.bfloat16)
    kept_rows = lengths[:, None] + jnp.arange(CONV - 1, dtype=jnp.int32)[None, :]
    next_value = jnp.take_along_axis(padded_value, kept_rows[:, :, None], axis=1)
    next_vector = jnp.take_along_axis(padded_vector, kept_rows[:, :, None, None], axis=1)
    return (block_out, next_state.reshape(recurrent_state.shape), next_value, next_vector)

def reference(tokens, lengths, norm_gain, gate_weight, value_weight, vector_weight, step_weight, step_bias, decay_rate, value_taps, vector_taps, out_weight, recurrent_state, value_history, vector_history):
    current = tokens
    state_list, value_list, vector_list = ([], [], [])
    for ordinal in range(LAYERS):
        current, new_state, new_value, new_vector = mixer_block(current, lengths, norm_gain[ordinal], gate_weight[ordinal], value_weight[ordinal], vector_weight[ordinal], step_weight[ordinal], step_bias[ordinal], decay_rate[ordinal], value_taps[ordinal], vector_taps[ordinal], out_weight[ordinal], recurrent_state[ordinal], value_history[ordinal], vector_history[ordinal])
        state_list.append(new_state)
        value_list.append(new_value)
        vector_list.append(new_vector)
    return (current, jnp.stack(state_list), jnp.stack(value_list), jnp.stack(vector_list))
```

```python
import jax
import jax.numpy as jnp
from jax import lax
from jax.sharding import Mesh, PartitionSpec as P

D = 4096
HEADS = 128
HEAD_DIM = 64
STATE = 128
GROUPS = 16
CONV = 4
NEW = 4
LAYERS = 2
norm_floor = 0.1

ZN, YN, DN = 16, 4, 8
SEQ = 6
bf16 = jnp.bfloat16
f32 = jnp.float32
COLS = 640


def exchange(pieces, axis):
    return lax.all_to_all(pieces, axis, 0, 0, tiled=True)


def copies(value, peers):
    return jnp.broadcast_to(value[None], (peers, *value.shape))


def short_conv(history, fresh_rows, conv_taps):
    padded = jnp.concatenate([history, fresh_rows], axis=1)
    summed = jnp.zeros(fresh_rows.shape, f32)
    for offset in range(CONV):
        summed = summed + padded[:, offset : offset + NEW].astype(f32) * conv_taps[offset].astype(
            f32
        )
    return (jax.nn.silu(summed), padded)


def project(rows, gain, gate_w, value_w, vector_w, step_w, square_lane):
    widened = rows.astype(f32)
    squares = jnp.sum(widened * widened, axis=1, keepdims=True)
    normed = (widened * gain[None]).astype(bf16)
    gate = jnp.einsum("td,ydc->tyc", normed, gate_w, preferred_element_type=f32)
    value = jnp.einsum("td,ydc->tyc", normed, value_w, preferred_element_type=f32)
    vector = jnp.einsum("td,cd->tc", normed, vector_w, preferred_element_type=f32)
    step = jnp.dot(normed, step_w, preferred_element_type=f32)
    lane = jnp.arange(HEADS, dtype=jnp.int32)[None]
    extra = jnp.where(lane == square_lane, squares, step)
    width = gate_w.shape[0]
    shared = jnp.concatenate([vector, extra], axis=1).astype(bf16)
    parts = [gate.astype(bf16), value.astype(bf16)]
    parts.append(jnp.broadcast_to(shared[:, None], (rows.shape[0], width, shared.shape[1])))
    return jnp.concatenate(parts, axis=2)


def middle(total, head_start, square_lane, live_mask, picker, bias, rate, history, taps, vhist, vtaps, state):
    squares = lax.dynamic_slice_in_dim(total, 512 + square_lane, 1, 1)
    scaling = lax.rsqrt(squares / D + norm_floor)
    scaled = (total * scaling).astype(bf16)
    gate = scaled[:, :128]
    value_in = scaled[:, 128:256]
    vector_in = scaled[:, 256:512]
    step_in = lax.dynamic_slice_in_dim(scaled, 512 + head_start, 2, 1)
    step = (
        jax.nn.softplus(step_in.astype(f32).reshape(SEQ, NEW, 2) + bias) * live_mask[:, :, None]
    )
    value_conv, padded_value = short_conv(history, value_in.reshape(SEQ, NEW, 128), taps)
    vector_conv, padded_vector = short_conv(vhist, vector_in.reshape(SEQ, NEW, 256), vtaps)
    write = vector_conv[:, :, :128]
    read = vector_conv[:, :, 128:]
    values = value_conv.reshape(SEQ, NEW, 2, HEAD_DIM)
    cumulative = jnp.cumsum(step * rate, axis=1)
    causal = jnp.tril(jnp.ones((NEW, NEW), dtype=bool))[None, :, :, None]
    log_gap = cumulative[:, :, None] - cumulative[:, None, :]
    decays = jnp.where(causal, jnp.exp(-jnp.where(causal, log_gap, 0.0)), 0.0)
    scores = jnp.einsum("stn,sun->stu", read, write)
    weights = scores[..., None] * decays * step[:, None]
    within = jnp.einsum("stur,surp->strp", weights, values)
    carried = jnp.einsum("stn,srpn->strp", read, state) * jnp.exp(-cumulative)[..., None]
    ending = jnp.exp(cumulative - cumulative[:, -1:]) * step
    weighted = values * ending[..., None]
    fresh = jnp.einsum("surp,sun->srpn", weighted, write)
    next_state = state * jnp.exp(-cumulative[:, -1])[..., None, None] + fresh
    output = (within + carried).reshape(SEQ, NEW, 128)
    gated = (
        output * jax.nn.silu(gate.astype(f32).reshape(SEQ, NEW, 128)) * live_mask[:, :, None]
    )
    mixed = gated.astype(bf16)
    next_value = jnp.einsum(
        "sjk,skc->sjc", picker, padded_value, preferred_element_type=f32
    ).astype(bf16)
    next_vector = jnp.einsum(
        "sjk,skc->sjc", picker, padded_vector, preferred_element_type=f32
    ).astype(bf16)
    return mixed, next_state, next_value, next_vector


def send_mixed(mixed):
    rows = mixed.reshape(2, YN, 3, 128).transpose(1, 0, 2, 3)
    rows = jnp.pad(rows, ((0, 0), (0, 0), (0, 1), (0, 0))).reshape(YN, 1, 8, 128)
    rows = jnp.broadcast_to(rows, (YN, DN, 8, 128)).reshape(YN * DN, 8, 128)
    return exchange(rows, ("y", "dp")).reshape(YN, DN * 8, 128)


def body(
    tokens,
    lengths,
    norm_gain,
    gate_weight,
    value_weight,
    vector_weight,
    step_weight,
    step_bias,
    decay_rate,
    value_taps,
    vector_taps,
    out_weight,
    recurrent_state,
    value_history,
    vector_history,
):
    z = lax.axis_index("z")
    y = lax.axis_index("y")
    head_start = 8 * z + 2 * y
    square_lane = (8 * z + 64) % HEADS
    live_mask = (jnp.arange(NEW, dtype=jnp.int32)[None, :] < lengths[:, None]).astype(f32)
    kept_rows = lengths[:, None] + jnp.arange(CONV - 1, dtype=jnp.int32)[None, :]
    picker = (
        kept_rows[:, :, None] == jnp.arange(CONV - 1 + NEW, dtype=jnp.int32)[None, None, :]
    ).astype(bf16)

    vector_cols = vector_weight.transpose(0, 2, 3, 1).reshape(2, 2, 2, GROUPS, 512)
    vector_cols = vector_cols.transpose(3, 0, 1, 2, 4).reshape(GROUPS, 8, 512)
    small = jnp.concatenate([vector_history.reshape(72, 32), vector_taps.reshape(16, 32)], axis=0)
    small = small.reshape(88, 2, GROUPS).transpose(2, 1, 0).reshape(GROUPS, 1, 176)
    small = jnp.pad(small, ((0, 0), (0, 0), (0, 512 - 176)))
    first = jnp.concatenate(
        [copies(tokens, ZN), vector_cols[:, :4], small, vector_cols[:, 4:]], axis=1
    )
    first = exchange(first, "z")
    own_out = exchange(copies(out_weight[0], YN), "y")
    plane = exchange(copies(first[:, :8], YN), "y")

    def lanes(w):
        return w.reshape(4, 128, 128).transpose(1, 0, 2).reshape(128, 512)

    later = jnp.concatenate(
        [
            lanes(gate_weight[1]),
            lanes(value_weight[1]),
            out_weight[1],
            first[:, 8:].reshape(64, 512),
        ],
        axis=0,
    )
    later = exchange(copies(later, YN), "y")

    whole = plane[:, :, :3].transpose(1, 0, 2, 3).reshape(192, 512)
    vector_w = [
        plane[:, :, 3:7].reshape(YN, ZN, 2, 2, 512).transpose(2, 1, 0, 3, 4).reshape(256, 512),
        later[:, 384:].reshape(YN, ZN, 2, 2, 512).transpose(2, 1, 0, 3, 4).reshape(256, 512),
    ]
    small = plane[:, :, 7, :176].reshape(YN, ZN, 2, 88).transpose(3, 1, 0, 2).reshape(88, 128)
    vhist = small[:72].reshape(2, SEQ, 3, 256)
    vtaps = small[72:].reshape(2, CONV, 256)

    def mid(total, layer):
        return middle(
            total,
            head_start,
            square_lane,
            live_mask,
            picker,
            step_bias[layer],
            decay_rate[layer],
            value_history[layer],
            value_taps[layer],
            vhist[layer],
            vtaps[layer],
            recurrent_state[layer],
        )

    part = project(
        whole,
        norm_gain[0],
        gate_weight[:1],
        value_weight[:1],
        vector_w[0],
        step_weight[0],
        square_lane,
    )
    part = exchange(part.reshape(DN, 24, COLS), "dp")
    total = jnp.sum(part.astype(f32), axis=0)
    mixed, state0, value0, vector0 = mid(total, 0)
    mixed = send_mixed(mixed)
    update = jnp.einsum("ytc,ycf->tf", mixed, own_out, preferred_element_type=f32)
    update = exchange(update.astype(bf16).reshape(ZN, 4, 512), "z")
    update = jnp.sum(update.astype(f32), axis=0)[:3]
    token_rows = (tokens.astype(f32) + update).astype(bf16)

    quarter = exchange(copies(jnp.pad(token_rows, ((0, 1), (0, 0))), ZN), "z").reshape(64, 512)

    def unlanes(w):
        return w.reshape(YN, 128, 4, 128).transpose(0, 2, 1, 3).reshape(YN, 512, 128)

    part = project(
        quarter,
        norm_gain[1],
        unlanes(later[:, :128]),
        unlanes(later[:, 128:256]),
        vector_w[1],
        step_weight[1],
        square_lane,
    )
    part = part.reshape(DN, 8, YN, COLS).transpose(2, 0, 1, 3).reshape(YN * DN, 8, COLS)
    part = exchange(part, ("y", "dp")).reshape(YN, DN, 8, COLS)
    total = jnp.sum(part.astype(f32), axis=1).reshape(YN, 2, 4, COLS)[:, :, :3]
    total = total.transpose(1, 0, 2, 3).reshape(24, COLS)
    mixed, state1, value1, vector1 = mid(total, 1)
    mixed = send_mixed(mixed)
    update = jnp.einsum("ytc,ycf->tf", mixed, later[:, 256:384], preferred_element_type=f32)
    update = update.astype(bf16).reshape(ZN, 4, 512)
    returned = jnp.stack([vector0, vector1]).reshape(72, ZN, YN, 2)
    returned = lax.dynamic_index_in_dim(returned, y, 2, keepdims=False)
    returned = returned.reshape(36, 2, ZN, 2).transpose(2, 3, 0, 1).reshape(ZN, 1, 144)
    returned = jnp.pad(returned, ((0, 0), (0, 0), (0, 512 - 144)))
    update = exchange(jnp.concatenate([update[:, :3], returned], axis=1), "z")
    token_rows = (
        token_rows.astype(f32) + jnp.sum(update[:, :3].astype(f32), axis=0)
    ).astype(bf16)
    returned = update[:, 3, :144].reshape(GROUPS, 2, 72).transpose(2, 1, 0)
    next_vector = returned.reshape(2, SEQ, 3, 2, 32)
    return (
        token_rows,
        jnp.stack([state0, state1]),
        jnp.stack([value0, value1]),
        next_vector,
    )


def solution(mesh):
    grid = Mesh(mesh.devices.reshape(ZN, YN, DN), ("z", "y", "dp"))
    tp = ("z", "y")
    return jax.shard_map(
        body,
        mesh=grid,
        in_specs=(
            P(tp, "dp"),
            P("dp"),
            P(None, "dp"),
            P(None, "dp", tp),
            P(None, "dp", tp),
            P(None, "dp", None, tp),
            P(None, "dp", None),
            P(None, tp),
            P(None, tp),
            P(None, None, tp),
            P(None, None, None, tp),
            P(None, tp, "dp"),
            P(None, "dp", tp, None, None),
            P(None, "dp", None, tp),
            P(None, "dp", None, None, tp),
        ),
        out_specs=(
            P(tp, "dp"),
            P(None, "dp", tp, None, None),
            P(None, "dp", None, tp),
            P(None, "dp", None, None, tp),
        ),
        check_vma=False,
    )
```

```python
import functools

import jax
import jax.numpy as jnp
from jax import lax
from jax.experimental import pallas as pl
from jax.experimental.pallas import tpu as pltpu
from jax.sharding import Mesh, PartitionSpec as P

D = 4096
HEADS = 128
HEAD_DIM = 64
STATE = 128
GROUPS = 16
CONV = 4
NEW = 4
LAYERS = 2
norm_floor = 0.1

ZN, YN, DN = 16, 4, 8
SEQ = 6
bf16 = jnp.bfloat16
f32 = jnp.float32
COLS = 640


def exchange(pieces, axis):
    return lax.all_to_all(pieces, axis, 0, 0, tiled=True)


def copies(value, peers):
    return jnp.broadcast_to(value[None], (peers, *value.shape))


def short_conv(history, fresh_rows, conv_taps):
    padded = jnp.concatenate([history, fresh_rows], axis=1)
    summed = jnp.zeros(fresh_rows.shape, f32)
    for offset in range(CONV):
        summed = summed + padded[:, offset : offset + NEW].astype(f32) * conv_taps[offset].astype(
            f32
        )
    return (jax.nn.silu(summed), padded)


def one_hot(rows, cols, target):
    row = lax.broadcasted_iota(jnp.int32, (rows, cols), 0)
    col = lax.broadcasted_iota(jnp.int32, (rows, cols), 1)
    return jnp.where(row == target(col), 1.0, 0.0).astype(bf16)


def mm(a, b):
    return lax.dot_general(a, b, (((1,), (0,)), ((), ())), preferred_element_type=f32)


def mm_t(a, b):
    return lax.dot_general(a, b, (((1,), (1,)), ((), ())), preferred_element_type=f32)


def normed_rows(rows, gain):
    widened = rows.astype(f32)
    squares = jnp.sum(widened * widened, axis=1, keepdims=True)
    return (widened * gain).astype(bf16), squares


def step_lanes(at_ref, normed, squares, step_w):
    step = mm(normed, step_w)
    lane = lax.broadcasted_iota(jnp.int32, step.shape, 1)
    return jnp.where(lane == at_ref[2], squares, step)


def first_projection(at_ref, plane_ref, gain_ref, gate_ref, value_ref, step_ref, out_ref):
    plane = plane_ref[...]

    def token_source(col):
        i = col % 8
        return jnp.where(i < 3, 12 * ((col // 8) % ZN) + 3 * (col // 128) + i, -1)

    def vector_source(col):
        j = col % 8 - 3
        n = 8 * ((col // 8) % ZN) + 2 * (col // 128) + j % 2
        return jnp.where((j >= 0) & (j < 4), 128 * (j // 2) + n, -1)

    rows = mm(one_hot(192, 512, token_source), plane).astype(bf16)
    vector_w = mm(one_hot(256, 512, vector_source), plane).astype(bf16)
    normed, squares = normed_rows(rows, gain_ref[0:1])
    parts = [
        mm(normed, gate_ref[0]),
        mm(normed, value_ref[0]),
        mm_t(normed, vector_w),
        step_lanes(at_ref, normed, squares, step_ref[0]),
    ]
    at = 0
    for part in parts:
        width = part.shape[1]
        out_ref[:, :, at : at + width] = part.astype(bf16).reshape(DN, 24, width)
        at += width


def second_projection(at_ref, rows_ref, gain_ref, step_ref, w0, w1, w2, w3, out_ref):
    y = at_ref[1]
    normed, squares = normed_rows(rows_ref[...], gain_ref[1:2])
    pieces = [w0, w1, w2, w3]

    def source(col):
        j = col % 4
        n = 8 * ((col // 4) % ZN) + 2 * ((y - col // 64) % YN) + j % 2
        return 128 * (j // 2) + n

    stacked = jnp.concatenate([w[384:448] for w in pieces], axis=0)
    vector_w = mm(one_hot(256, 256, source), stacked).astype(bf16)
    vector = mm_t(normed, vector_w).astype(bf16)
    extra = step_lanes(at_ref, normed, squares, step_ref[0]).astype(bf16)
    for k, w in enumerate(pieces):
        to = (y - k) % YN
        for n in range(2):
            total = jnp.zeros((64, 128), f32)
            for b in range(4):
                total += mm(
                    normed[:, 128 * b : 128 * b + 128],
                    w[128 * n : 128 * n + 128, 128 * b : 128 * b + 128],
                )
            out_ref[to, :, 128 * n : 128 * n + 128] = total.astype(bf16)
        out_ref[to, :, 256:512] = vector
        out_ref[to, :, 512:640] = extra


def out_projection(at_ref, mixed_ref, w0, w1, w2, w3, *rest, first_row):
    y = at_ref[1]
    total = jnp.zeros((64, 512), f32)
    for k, w in enumerate([w0, w1, w2, w3]):
        total += mm(mixed_ref[(y - k) % YN], w[first_row : first_row + 128])
    if len(rest) == 1:
        rest[0][...] = total.astype(bf16)
        return
    returned_ref, out_ref = rest
    slot = one_hot(64, ZN, lambda col: 4 * col + 3)
    halves = []
    for nl in range(2):
        row = lax.broadcasted_iota(jnp.int32, (ZN, 128), 0)
        col = lax.broadcasted_iota(jnp.int32, (ZN, 128), 1)
        chosen = jnp.where(col == 8 * row + 2 * y + nl, 1.0, 0.0).astype(bf16)
        halves.append(mm_t(chosen, returned_ref[...]).astype(bf16))
    tail = jnp.concatenate(halves, axis=1)
    out_ref[:, 256:512] = total[:, 256:512].astype(bf16)
    out_ref[:, 0:256] = (total[:, 0:256] + mm(slot, tail)).astype(bf16)


def call(kernel, shape, *args):
    space = [pl.BlockSpec(memory_space=pltpu.SMEM)]
    space += [pl.BlockSpec(memory_space=pltpu.VMEM)] * (len(args) - 1)
    return pl.pallas_call(
        kernel,
        out_shape=jax.ShapeDtypeStruct(shape, bf16),
        in_specs=space,
        out_specs=pl.BlockSpec(memory_space=pltpu.VMEM),
        compiler_params=pltpu.CompilerParams(vmem_limit_bytes=8 << 20),
    )(*args)


def around_y(value):
    pieces = [value]
    for k in range(1, YN):
        pieces.append(lax.ppermute(value, "y", [(i, (i + k) % YN) for i in range(YN)]))
    return pieces


def middle(total, head_start, square_lane, live_mask, picker, bias, rate, history, taps, vhist, vtaps, state):
    squares = lax.dynamic_slice_in_dim(total, 512 + square_lane, 1, 1)
    scaling = lax.rsqrt(squares / D + norm_floor)
    scaled = (total * scaling).astype(bf16)
    gate = scaled[:, :128]
    value_in = scaled[:, 128:256]
    vector_in = scaled[:, 256:512]
    step_in = lax.dynamic_slice_in_dim(scaled, 512 + head_start, 2, 1)
    step = (
        jax.nn.softplus(step_in.astype(f32).reshape(SEQ, NEW, 2) + bias) * live_mask[:, :, None]
    )
    value_conv, padded_value = short_conv(history, value_in.reshape(SEQ, NEW, 128), taps)
    vector_conv, padded_vector = short_conv(vhist, vector_in.reshape(SEQ, NEW, 256), vtaps)
    write = vector_conv[:, :, :128]
    read = vector_conv[:, :, 128:]
    values = value_conv.reshape(SEQ, NEW, 2, HEAD_DIM)
    cumulative = jnp.cumsum(step * rate, axis=1)
    causal = jnp.tril(jnp.ones((NEW, NEW), dtype=bool))[None, :, :, None]
    log_gap = cumulative[:, :, None] - cumulative[:, None, :]
    decays = jnp.where(causal, jnp.exp(-jnp.where(causal, log_gap, 0.0)), 0.0)
    scores = jnp.einsum("stn,sun->stu", read, write)
    weights = scores[..., None] * decays * step[:, None]
    within = jnp.einsum("stur,surp->strp", weights, values)
    carried = jnp.einsum("stn,srpn->strp", read, state) * jnp.exp(-cumulative)[..., None]
    ending = jnp.exp(cumulative - cumulative[:, -1:]) * step
    weighted = values * ending[..., None]
    fresh = jnp.einsum("surp,sun->srpn", weighted, write)
    next_state = state * jnp.exp(-cumulative[:, -1])[..., None, None] + fresh
    output = (within + carried).reshape(SEQ, NEW, 128)
    gated = (
        output * jax.nn.silu(gate.astype(f32).reshape(SEQ, NEW, 128)) * live_mask[:, :, None]
    )
    mixed = gated.astype(bf16)
    next_value = jnp.einsum(
        "sjk,skc->sjc", picker, padded_value, preferred_element_type=f32
    ).astype(bf16)
    next_vector = jnp.einsum(
        "sjk,skc->sjc", picker, padded_vector, preferred_element_type=f32
    ).astype(bf16)
    return mixed, next_state, next_value, next_vector


def send_mixed(mixed):
    rows = mixed.reshape(2, YN, 3, 128).transpose(1, 0, 2, 3)
    rows = jnp.pad(rows, ((0, 0), (0, 0), (0, 1), (0, 0))).reshape(YN, 1, 8, 128)
    rows = jnp.broadcast_to(rows, (YN, DN, 8, 128)).reshape(YN * DN, 8, 128)
    return exchange(rows, ("y", "dp")).reshape(YN, DN * 8, 128)


def body(
    tokens,
    lengths,
    norm_gain,
    gate_weight,
    value_weight,
    vector_weight,
    step_weight,
    step_bias,
    decay_rate,
    value_taps,
    vector_taps,
    out_weight,
    recurrent_state,
    value_history,
    vector_history,
):
    z = lax.axis_index("z")
    y = lax.axis_index("y")
    head_start = 8 * z + 2 * y
    square_lane = (8 * z + 64) % HEADS
    live_mask = (jnp.arange(NEW, dtype=jnp.int32)[None, :] < lengths[:, None]).astype(f32)
    kept_rows = lengths[:, None] + jnp.arange(CONV - 1, dtype=jnp.int32)[None, :]
    picker = (
        kept_rows[:, :, None] == jnp.arange(CONV - 1 + NEW, dtype=jnp.int32)[None, None, :]
    ).astype(bf16)

    vector_cols = vector_weight.transpose(0, 2, 3, 1).reshape(2, 2, 2, GROUPS, 512)
    vector_cols = vector_cols.transpose(3, 0, 1, 2, 4).reshape(GROUPS, 8, 512)
    small = jnp.concatenate([vector_history.reshape(72, 32), vector_taps.reshape(16, 32)], axis=0)
    small = small.reshape(88, 2, GROUPS).transpose(2, 1, 0).reshape(GROUPS, 1, 176)
    small = jnp.pad(small, ((0, 0), (0, 0), (0, 512 - 176)))
    first = jnp.concatenate(
        [copies(tokens, ZN), vector_cols[:, :4], small, vector_cols[:, 4:]], axis=1
    )
    at = jnp.stack([z, y, square_lane]).astype(jnp.int32)
    first = exchange(first, "z")
    own_out = around_y(out_weight[0])
    plane = exchange(copies(first[:, :8], YN), "y")

    small = plane[:, :, 7, :176].reshape(YN, ZN, 2, 88).transpose(3, 1, 0, 2).reshape(88, 128)
    vhist = small[:72].reshape(2, SEQ, 3, 256)
    vtaps = small[72:].reshape(2, CONV, 256)

    def mid(total, layer):
        return middle(
            total,
            head_start,
            square_lane,
            live_mask,
            picker,
            step_bias[layer],
            decay_rate[layer],
            value_history[layer],
            value_taps[layer],
            vhist[layer],
            vtaps[layer],
            recurrent_state[layer],
        )

    part = call(
        first_projection,
        (DN, 24, COLS),
        at,
        plane.reshape(512, 512),
        norm_gain,
        gate_weight[:1],
        value_weight[:1],
        step_weight[:1],
    )
    part = exchange(part, "dp")
    total = jnp.sum(part.astype(f32), axis=0)
    mixed, state0, value0, vector0 = mid(total, 0)
    mixed = send_mixed(mixed)
    update = call(
        functools.partial(out_projection, first_row=0), (64, 512), at, mixed, *own_out
    )

    def lanes(w):
        return w.reshape(4, 128, 128).transpose(1, 0, 2).reshape(128, 512)

    later = jnp.concatenate(
        [
            lanes(gate_weight[1]),
            lanes(value_weight[1]),
            out_weight[1],
            first[:, 8:].reshape(64, 512),
        ],
        axis=0,
    )
    update, later = lax.optimization_barrier((update, later))
    update = exchange(update.reshape(ZN, 4, 512), "z")
    later = around_y(later)
    update = jnp.sum(update.astype(f32), axis=0)[:3]
    token_rows = (tokens.astype(f32) + update).astype(bf16)

    quarter = exchange(copies(jnp.pad(token_rows, ((0, 1), (0, 0))), ZN), "z").reshape(64, 512)
    part = call(
        second_projection, (YN, 64, COLS), at, quarter, norm_gain, step_weight[1:], *later
    )
    part = exchange(part.reshape(YN * DN, 8, COLS), ("y", "dp")).reshape(YN, DN, 8, COLS)
    total = jnp.sum(part.astype(f32), axis=1).reshape(YN, 2, 4, COLS)[:, :, :3]
    total = total.transpose(1, 0, 2, 3).reshape(24, COLS)
    mixed, state1, value1, vector1 = mid(total, 1)
    mixed, vector1 = lax.optimization_barrier((mixed, vector1))
    mixed = send_mixed(mixed)
    returned = jnp.stack([vector0, vector1]).reshape(72, 128)
    returned = jnp.pad(returned, ((0, 56), (0, 0)))
    update = call(
        functools.partial(out_projection, first_row=256), (64, 512), at, mixed, *later, returned
    )
    update = exchange(update.reshape(ZN, 4, 512), "z")
    token_rows = (
        token_rows.astype(f32) + jnp.sum(update[:, :3].astype(f32), axis=0)
    ).astype(bf16)
    returned = update[:, 3, :256].reshape(GROUPS, 2, 128)[:, :, :72].transpose(2, 1, 0)
    next_vector = returned.reshape(2, SEQ, 3, 2, 32)
    return (
        token_rows,
        jnp.stack([state0, state1]),
        jnp.stack([value0, value1]),
        next_vector,
    )


def solution(mesh):
    grid = Mesh(mesh.devices.reshape(ZN, YN, DN), ("z", "y", "dp"))
    tp = ("z", "y")
    return jax.shard_map(
        body,
        mesh=grid,
        in_specs=(
            P(tp, "dp"),
            P("dp"),
            P(None, "dp"),
            P(None, "dp", tp),
            P(None, "dp", tp),
            P(None, "dp", None, tp),
            P(None, "dp", None),
            P(None, tp),
            P(None, tp),
            P(None, None, tp),
            P(None, None, None, tp),
            P(None, tp, "dp"),
            P(None, "dp", tp, None, None),
            P(None, "dp", None, tp),
            P(None, "dp", None, None, tp),
        ),
        out_specs=(
            P(tp, "dp"),
            P(None, "dp", tp, None, None),
            P(None, "dp", None, tp),
            P(None, "dp", None, None, tp),
        ),
        check_vma=False,
    )
```

```python
import functools

import jax
import jax.numpy as jnp
from jax import lax
from jax.experimental import pallas as pl
from jax.experimental.pallas import tpu as pltpu
from jax.sharding import Mesh, PartitionSpec as P

D = 4096
HEADS = 128
HEAD_DIM = 64
STATE = 128
GROUPS = 16
CONV = 4
NEW = 4
LAYERS = 2
norm_floor = 0.1

ZN, YN, DN = 16, 4, 8
SEQ = 6
bf16 = jnp.bfloat16
f32 = jnp.float32
COLS = 640


def exchange(pieces, axis):
    return lax.all_to_all(pieces, axis, 0, 0, tiled=True)


def copies(value, peers):
    return jnp.broadcast_to(value[None], (peers, *value.shape))


def one_hot(rows, cols, target):
    row = lax.broadcasted_iota(jnp.int32, (rows, cols), 0)
    col = lax.broadcasted_iota(jnp.int32, (rows, cols), 1)
    return jnp.where(row == target(col), 1.0, 0.0).astype(bf16)


def mm(a, b):
    return lax.dot_general(a, b, (((1,), (0,)), ((), ())), preferred_element_type=f32)


def mm_t(a, b):
    return lax.dot_general(a, b, (((1,), (1,)), ((), ())), preferred_element_type=f32)


def normed_rows(rows, gain):
    widened = rows.astype(f32)
    squares = jnp.sum(widened * widened, axis=1, keepdims=True)
    return (widened * gain).astype(bf16), squares


def step_lanes(at_ref, normed, squares, step_w):
    step = mm(normed, step_w)
    lane = lax.broadcasted_iota(jnp.int32, step.shape, 1)
    return jnp.where(lane == at_ref[2], squares, step)


def first_projection(at_ref, plane_ref, gain_ref, gate_ref, value_ref, step_ref, out_ref):
    plane = plane_ref[...]

    def token_source(col):
        i = col % 8
        return jnp.where(i < 3, 12 * ((col // 8) % ZN) + 3 * (col // 128) + i, -1)

    def vector_source(col):
        j = col % 8 - 4
        n = 8 * ((col // 8) % ZN) + 2 * (col // 128) + j % 2
        return jnp.where((j >= 0) & (j < 4), 128 * (j // 2) + n, -1)

    rows = mm(one_hot(192, 512, token_source), plane).astype(bf16)
    vector_w = mm(one_hot(256, 512, vector_source), plane).astype(bf16)
    normed, squares = normed_rows(rows, gain_ref[0:1])
    parts = [
        mm(normed, gate_ref[0]),
        mm(normed, value_ref[0]),
        mm_t(normed, vector_w),
        step_lanes(at_ref, normed, squares, step_ref[0]),
    ]
    at = 0
    for part in parts:
        width = part.shape[1]
        out_ref[:, :, at : at + width] = part.astype(bf16).reshape(DN, 24, width)
        at += width


def second_projection(at_ref, rows_ref, gain_ref, step_ref, w0, w1, w2, w3, out_ref):
    y = at_ref[1]
    normed, squares = normed_rows(rows_ref[...], gain_ref[1:2])
    pieces = [w0, w1, w2, w3]

    def source(col):
        j = col % 4
        n = 8 * ((col // 4) % ZN) + 2 * ((y - col // 64) % YN) + j % 2
        return 128 * (j // 2) + n

    stacked = jnp.concatenate([w[384:448] for w in pieces], axis=0)
    vector_w = mm(one_hot(256, 256, source), stacked).astype(bf16)
    vector = mm_t(normed, vector_w).astype(bf16)
    extra = step_lanes(at_ref, normed, squares, step_ref[0]).astype(bf16)
    for k, w in enumerate(pieces):
        to = (y - k) % YN
        for n in range(2):
            total = jnp.zeros((64, 128), f32)
            for b in range(4):
                total += mm(
                    normed[:, 128 * b : 128 * b + 128],
                    w[128 * n : 128 * n + 128, 128 * b : 128 * b + 128],
                )
            out_ref[to, :, 128 * n : 128 * n + 128] = total.astype(bf16)
        out_ref[to, :, 256:512] = vector
        out_ref[to, :, 512:640] = extra


def out_projection(at_ref, mixed_ref, w0, w1, w2, w3, *rest, first_row):
    y = at_ref[1]
    total = jnp.zeros((64, 512), f32)
    for k, w in enumerate([w0, w1, w2, w3]):
        total += mm(mixed_ref[(y - k) % YN], w[first_row : first_row + 128])
    if len(rest) == 1:
        rest[0][...] = total.astype(bf16).reshape(ZN, 4, 512)
        return
    returned_ref, out_ref = rest
    returned = jnp.concatenate(
        [returned_ref[:, 0:128], returned_ref[:, 128:256], jnp.zeros((32, 128), bf16)], axis=0
    )
    slot = one_hot(64, ZN, lambda col: 4 * col + 3)
    halves = []
    for nl in range(2):
        row = lax.broadcasted_iota(jnp.int32, (ZN, 128), 0)
        col = lax.broadcasted_iota(jnp.int32, (ZN, 128), 1)
        chosen = jnp.where(col == 8 * row + 2 * y + nl, 1.0, 0.0).astype(bf16)
        halves.append(mm_t(chosen, returned).astype(bf16))
    tail = jnp.concatenate(halves, axis=1)
    left = (total[:, 0:256] + mm(slot, tail)).astype(bf16)
    whole = jnp.concatenate([left, total[:, 256:512].astype(bf16)], axis=1)
    out_ref[...] = whole.reshape(ZN, 4, 512)


def row_col(shape):
    return (
        lax.broadcasted_iota(jnp.int32, shape, 0),
        lax.broadcasted_iota(jnp.int32, shape, 1),
    )


def silu(x):
    return x * jax.nn.sigmoid(x)


def lengths_column(len_ref):
    row = lax.broadcasted_iota(jnp.int32, (8, 1), 0)
    lens = jnp.zeros((8, 1), jnp.int32)
    for s in range(SEQ):
        lens = jnp.where(row == s, len_ref[s], lens)
    return lens


def place_first(col):
    return 8 * (col % NEW) + col // NEW


def place_second(col):
    i = col % 4
    n = 12 * ((col // 4) % 2) + 3 * (col // 8) + i
    return jnp.where(i < 3, 8 * (n % NEW) + n // NEW, -1)


def conv(history_ref, fresh, taps_ref):
    rows = [history_ref[k].astype(f32) for k in range(CONV - 1)]
    rows += [fresh[8 * t : 8 * t + 8] for t in range(NEW)]
    taps = [taps_ref[k : k + 1].astype(f32) for k in range(CONV)]
    return [silu(sum(rows[t + k] * taps[k] for k in range(CONV))) for t in range(NEW)]


def middle(
    at_ref,
    len_ref,
    bias_ref,
    rate_ref,
    part_ref,
    history_ref,
    taps_ref,
    vhist_ref,
    vtaps_ref,
    state_ref,
    msg_ref,
    keep_ref,
    write_ref,
    decay_ref,
    fresh_ref,
    *,
    layer,
):
    if layer == 0:
        total = sum(part_ref[d].astype(f32) for d in range(DN))
        place = one_hot(32, 24, place_first)
    else:
        rows = [sum(part_ref[y, d].astype(f32) for d in range(DN)) for y in range(YN)]
        total = jnp.concatenate(rows, axis=0)
        place = one_hot(32, 32, place_second)
    tail = total[:, 512:640]
    _, lane = row_col(tail.shape)
    squares = jnp.sum(jnp.where(lane == at_ref[2], tail, 0.0), axis=1, keepdims=True)
    scaled = (total * lax.rsqrt(squares / D + norm_floor)).astype(bf16)
    rows = mm(place, scaled)
    fresh_ref[...] = rows[:, 128:512].astype(bf16)
    gate = rows[:, 0:128]

    head = 8 * at_ref[0] + 2 * at_ref[1]
    tail = rows[:, 512:640]
    _, lane = row_col(tail.shape)
    first = jnp.sum(jnp.where(lane == head, tail, 0.0), axis=1, keepdims=True)
    second = jnp.sum(jnp.where(lane == head + 1, tail, 0.0), axis=1, keepdims=True)
    left = lane < HEAD_DIM
    raw = jnp.where(left, first + bias_ref[layer, 0], second + bias_ref[layer, 1])
    rate = jnp.where(left[:8], rate_ref[layer, 0], rate_ref[layer, 1])
    soft = jnp.maximum(raw, 0.0) + jnp.log1p(jnp.exp(-jnp.abs(raw)))
    lens = lengths_column(len_ref)
    live = [jnp.where(lens > t, 1.0, 0.0) for t in range(NEW)]
    step = [soft[8 * t : 8 * t + 8] * live[t] for t in range(NEW)]
    cumulative = []
    for t in range(NEW):
        grown = step[t] * rate
        cumulative.append(grown if t == 0 else cumulative[-1] + grown)

    values = conv(history_ref, rows[:, 128:256], taps_ref)
    vectors = conv(vhist_ref, rows[:, 256:512], vtaps_ref)
    write = [v[:, 0:128] for v in vectors]
    read = [v[:, 128:256] for v in vectors]
    stepped = [values[t] * step[t] for t in range(NEW)]

    reads = jnp.concatenate(read, axis=0).astype(bf16)
    row, _ = row_col((32, 128))
    carried = jnp.zeros((32, 128), f32)
    for s in range(SEQ):
        carried = jnp.where(row % 8 == s, mm_t(reads, state_ref[s].astype(bf16)), carried)

    mixed = []
    for t in range(NEW):
        y = jnp.exp(-cumulative[t]) * carried[8 * t : 8 * t + 8]
        for u in range(t + 1):
            score = jnp.sum(read[t] * write[u], axis=1, keepdims=True)
            y = y + score * jnp.exp(cumulative[u] - cumulative[t]) * stepped[u]
        mixed.append(y * silu(gate[8 * t : 8 * t + 8]) * live[t])
    mixed = jnp.concatenate(mixed, axis=0).astype(bf16)
    row, col = row_col((32, 32))
    i = row % 4
    n = 12 * ((row // 4) % 2) + 3 * (row // 8) + i
    pick = (col == 8 * (n % NEW) + n // NEW) & (i < 3)
    ordered = mm(jnp.where(pick, 1.0, 0.0).astype(bf16), mixed).astype(bf16)
    for y in range(YN):
        for d in range(DN):
            msg_ref[y * DN + d] = ordered[8 * y : 8 * y + 8]

    last = cumulative[-1]
    for t in range(NEW):
        keep_ref[8 * t : 8 * t + 8] = jnp.exp(cumulative[t] - last) * stepped[t]
        write_ref[8 * t : 8 * t + 8] = write[t]
    decay_ref[...] = jnp.exp(-last)


def finish(
    len_ref,
    keep_ref,
    write_ref,
    decay_ref,
    fresh_ref,
    history_ref,
    vhist_ref,
    state_ref,
    next_ref,
    value_ref,
    vector_ref,
):
    kept = jnp.transpose(keep_ref[...])
    _, col = row_col(kept.shape)
    write = write_ref[...].astype(bf16)
    for s in range(SEQ):
        fresh = mm(jnp.where(col % 8 == s, kept, 0.0).astype(bf16), write)
        for h in range(2):
            at = slice(HEAD_DIM * h, HEAD_DIM * h + HEAD_DIM)
            decay = decay_ref[s : s + 1, HEAD_DIM * h : HEAD_DIM * h + 1]
            next_ref[s, at] = state_ref[s, at] * decay + fresh[at]
    lens = lengths_column(len_ref)
    for out_ref, old_ref, lo, hi in (
        (value_ref, history_ref, 0, 128),
        (vector_ref, vhist_ref, 128, 384),
    ):
        rows = [old_ref[k].astype(f32) for k in range(CONV - 1)]
        rows += [fresh_ref[8 * t : 8 * t + 8, lo:hi].astype(f32) for t in range(NEW)]
        for k in range(CONV - 1):
            chosen = rows[k + 1]
            for r in range(k + 2, k + NEW + 1):
                chosen = jnp.where(lens + k == r, rows[r], chosen)
            out_ref[k] = chosen.astype(bf16)


def call(kernel, shapes, scalars, *args):
    vmem = pl.BlockSpec(memory_space=pltpu.VMEM)
    space = [pl.BlockSpec(memory_space=pltpu.SMEM)] * scalars
    space += [vmem] * (len(args) - scalars)
    outs = [jax.ShapeDtypeStruct(shape, dtype) for shape, dtype in shapes]
    results = pl.pallas_call(
        kernel,
        out_shape=outs,
        in_specs=space,
        out_specs=[vmem] * len(outs),
        compiler_params=pltpu.CompilerParams(vmem_limit_bytes=12 << 20),
    )(*args)
    return results[0] if len(outs) == 1 else results


def around_y(value):
    pieces = [value]
    for k in range(1, YN):
        pieces.append(lax.ppermute(value, "y", [(i, (i + k) % YN) for i in range(YN)]))
    return pieces


def body(
    tokens,
    lengths,
    norm_gain,
    gate_weight,
    value_weight,
    vector_weight,
    step_weight,
    step_bias,
    decay_rate,
    value_taps,
    vector_taps,
    out_weight,
    recurrent_state,
    value_history,
    vector_history,
):
    z = lax.axis_index("z")
    y = lax.axis_index("y")
    square_lane = (8 * z + 64) % HEADS
    vector_cols = vector_weight.transpose(0, 2, 3, 1).reshape(2, 2, 2, GROUPS, 512)
    vector_cols = vector_cols.transpose(3, 0, 1, 2, 4).reshape(GROUPS, 8, 512)
    small = jnp.concatenate([vector_history.reshape(72, 32), vector_taps.reshape(16, 32)], axis=0)
    small = small.reshape(88, 2, GROUPS).transpose(2, 1, 0).reshape(GROUPS, 1, 176)
    small = jnp.pad(small, ((0, 0), (0, 0), (0, 512 - 176)))
    first = jnp.concatenate([copies(tokens, ZN), small], axis=1).reshape(ZN, 1, 4, 512)
    first = jnp.concatenate([first, vector_cols.reshape(ZN, 2, 4, 512)], axis=1)
    at = jnp.stack([z, y, square_lane]).astype(jnp.int32)
    first, own_out = lax.optimization_barrier((first, out_weight[0]))
    first = exchange(first, "z")
    own_out = around_y(own_out)
    plane = exchange(copies(first[:, :2], YN), "y").reshape(YN, ZN, 8, 512)

    small = plane[:, :, 3, :176].reshape(YN, ZN, 2, 88).transpose(3, 1, 0, 2).reshape(88, 128)
    vhist = small[:72].reshape(2, SEQ, 3, 256).transpose(0, 2, 1, 3)
    vhist = jnp.pad(vhist, ((0, 0), (0, 0), (0, 2), (0, 0)))
    vtaps = small[72:].reshape(2, CONV, 256)
    history = jnp.pad(value_history.transpose(0, 2, 1, 3), ((0, 0), (0, 0), (0, 2), (0, 0)))
    states = [recurrent_state[layer].reshape(SEQ, 128, 128) for layer in range(LAYERS)]

    def mid(part, layer):
        old = (history[layer], vhist[layer])
        msg, keep, write, decay, fresh = call(
            functools.partial(middle, layer=layer),
            [
                ((YN * DN, 8, 128), bf16),
                ((32, 128), f32),
                ((32, 128), f32),
                ((8, 128), f32),
                ((32, 384), bf16),
            ],
            4,
            at,
            lengths,
            step_bias,
            decay_rate,
            part,
            history[layer],
            value_taps[layer],
            vhist[layer],
            vtaps[layer],
            states[layer],
        )
        after = call(
            finish,
            [((SEQ, 128, 128), f32), ((3, 8, 128), bf16), ((3, 8, 256), bf16)],
            1,
            lengths,
            keep,
            write,
            decay,
            fresh,
            *old,
            states[layer],
        )
        return exchange(msg, ("y", "dp")).reshape(YN, DN * 8, 128), after

    part = call(
        first_projection,
        [((DN, 24, COLS), bf16)],
        1,
        at,
        plane.reshape(512, 512),
        norm_gain,
        gate_weight[:1],
        value_weight[:1],
        step_weight[:1],
    )
    part = exchange(part, "dp")
    mixed, (state0, value0, vector0) = mid(part, 0)
    update = call(
        functools.partial(out_projection, first_row=0),
        [((ZN, 4, 512), bf16)],
        1,
        at,
        mixed,
        *own_out,
    )

    def lanes(w):
        return w.reshape(4, 128, 128).transpose(1, 0, 2).reshape(128, 512)

    later = jnp.concatenate(
        [
            lanes(gate_weight[1]),
            lanes(value_weight[1]),
            out_weight[1],
            first[:, 2].reshape(64, 512),
        ],
        axis=0,
    )
    update, later = lax.optimization_barrier((update, later))
    update = exchange(update, "z")
    later = around_y(later)
    update = jnp.sum(update.astype(f32), axis=0)[:3]
    token_rows = (tokens.astype(f32) + update).astype(bf16)

    quarter = exchange(copies(jnp.pad(token_rows, ((0, 1), (0, 0))), ZN), "z").reshape(64, 512)
    part = call(
        second_projection,
        [((YN, 64, COLS), bf16)],
        1,
        at,
        quarter,
        norm_gain,
        step_weight[1:],
        *later,
    )
    part = exchange(part.reshape(YN * DN, 8, COLS), ("y", "dp")).reshape(YN, DN, 8, COLS)
    mixed, (state1, value1, vector1) = mid(part, 1)
    update = call(
        functools.partial(out_projection, first_row=256),
        [((ZN, 4, 512), bf16)],
        1,
        at,
        mixed,
        *later,
        jnp.concatenate([vector0, vector1], axis=0).reshape(48, 256),
    )
    update = exchange(update, "z")
    token_rows = (
        token_rows.astype(f32) + jnp.sum(update[:, :3].astype(f32), axis=0)
    ).astype(bf16)
    returned = update[:, 3, :256].reshape(GROUPS, 2, 128)[:, :, :96]
    returned = returned.reshape(GROUPS, 2, 2, 2, 3, 8)[..., :SEQ].transpose(3, 5, 4, 2, 1, 0)
    next_vector = returned.reshape(2, SEQ, 3, 2, 32)
    return (
        token_rows,
        jnp.stack([state0, state1]).reshape(recurrent_state.shape),
        jnp.stack([value0, value1])[:, :, :SEQ].transpose(0, 2, 1, 3),
        next_vector,
    )


def solution(mesh):
    grid = Mesh(mesh.devices.reshape(ZN, YN, DN), ("z", "y", "dp"))
    tp = ("z", "y")
    return jax.shard_map(
        body,
        mesh=grid,
        in_specs=(
            P(tp, "dp"),
            P("dp"),
            P(None, "dp"),
            P(None, "dp", tp),
            P(None, "dp", tp),
            P(None, "dp", None, tp),
            P(None, "dp", None),
            P(None, tp),
            P(None, tp),
            P(None, None, tp),
            P(None, None, None, tp),
            P(None, tp, "dp"),
            P(None, "dp", tp, None, None),
            P(None, "dp", None, tp),
            P(None, "dp", None, None, tp),
        ),
        out_specs=(
            P(tp, "dp"),
            P(None, "dp", tp, None, None),
            P(None, "dp", None, tp),
            P(None, "dp", None, None, tp),
        ),
        check_vma=False,
    )
```

```python
import functools

import jax
import jax.numpy as jnp
from jax import lax
from jax.experimental import pallas as pl
from jax.experimental.pallas import tpu as pltpu
from jax.sharding import Mesh, PartitionSpec as P

D = 4096
HEADS = 128
HEAD_DIM = 64
GROUPS = 16
CONV = 4
NEW = 4
LAYERS = 2
norm_floor = 0.1

ZN, YN, DN = 16, 4, 8
SEQ = 6
bf16 = jnp.bfloat16
f32 = jnp.float32
COLS = 640


def exchange(pieces, axis):
    return lax.all_to_all(pieces, axis, 0, 0, tiled=True)


def copies(value, peers):
    return jnp.broadcast_to(value[None], (peers, *value.shape))


def one_hot(rows, cols, target):
    row = lax.broadcasted_iota(jnp.int32, (rows, cols), 0)
    col = lax.broadcasted_iota(jnp.int32, (rows, cols), 1)
    return jnp.where(row == target(col), 1.0, 0.0).astype(bf16)


def mm(a, b):
    return lax.dot_general(a, b, (((1,), (0,)), ((), ())), preferred_element_type=f32)


def mm_t(a, b):
    return lax.dot_general(a, b, (((1,), (1,)), ((), ())), preferred_element_type=f32)


def normed_rows(rows, gain):
    widened = rows.astype(f32)
    squares = jnp.sum(widened * widened, axis=1, keepdims=True)
    return (widened * gain).astype(bf16), squares


def step_lanes(at_ref, normed, squares, step_w):
    step = mm(normed, step_w)
    lane = lax.broadcasted_iota(jnp.int32, step.shape, 1)
    return jnp.where(lane == at_ref[2], squares, step)


def first_projection(at_ref, plane_ref, gain_ref, gate_ref, value_ref, step_ref, out_ref):
    plane = plane_ref[...]

    def token_source(col):
        i = col % 8
        return jnp.where(i < 3, 12 * ((col // 8) % ZN) + 3 * (col // 128) + i, -1)

    def vector_source(col):
        j = col % 8 - 4
        n = 8 * ((col // 8) % ZN) + 2 * (col // 128) + j % 2
        return jnp.where((j >= 0) & (j < 4), 128 * (j // 2) + n, -1)

    rows = mm(one_hot(192, 512, token_source), plane).astype(bf16)
    vector_w = mm(one_hot(256, 512, vector_source), plane).astype(bf16)
    normed, squares = normed_rows(rows, gain_ref[0:1])
    parts = [
        mm(normed, gate_ref[0]),
        mm(normed, value_ref[0]),
        mm_t(normed, vector_w),
        step_lanes(at_ref, normed, squares, step_ref[0]),
    ]
    at = 0
    for part in parts:
        width = part.shape[1]
        out_ref[:, :, at : at + width] = part.astype(bf16).reshape(DN, 24, width)
        at += width


def second_projection(at_ref, rows_ref, gain_ref, step_ref, w0, w1, w2, w3, out_ref):
    y = at_ref[1]
    normed, squares = normed_rows(rows_ref[...], gain_ref[1:2])
    pieces = [w0, w1, w2, w3]

    def source(col):
        j = col % 4
        n = 8 * ((col // 4) % ZN) + 2 * ((y - col // 64) % YN) + j % 2
        return 128 * (j // 2) + n

    stacked = jnp.concatenate([w[384:448] for w in pieces], axis=0)
    vector_w = mm(one_hot(256, 256, source), stacked).astype(bf16)
    vector = mm_t(normed, vector_w).astype(bf16)
    extra = step_lanes(at_ref, normed, squares, step_ref[1]).astype(bf16)
    for k, w in enumerate(pieces):
        to = (y - k) % YN
        for n in range(2):
            total = jnp.zeros((64, 128), f32)
            for b in range(4):
                total += mm(
                    normed[:, 128 * b : 128 * b + 128],
                    w[128 * n : 128 * n + 128, 128 * b : 128 * b + 128],
                )
            out_ref[to, :, 128 * n : 128 * n + 128] = total.astype(bf16)
        out_ref[to, :, 256:512] = vector
        out_ref[to, :, 512:640] = extra


def out_projection(at_ref, mixed_ref, w0, w1, w2, w3, *rest, first_row):
    y = at_ref[1]
    total = jnp.zeros((64, 512), f32)
    for k, w in enumerate([w0, w1, w2, w3]):
        total += mm(mixed_ref[(y - k) % YN], w[first_row : first_row + 128])
    if len(rest) == 1:
        rest[0][...] = total.astype(bf16).reshape(ZN, 4, 512)
        return
    returned_ref, out_ref = rest
    returned = jnp.concatenate(
        [returned_ref[:, 0:128], returned_ref[:, 128:256], jnp.zeros((32, 128), bf16)], axis=0
    )
    slot = one_hot(64, ZN, lambda col: 4 * col + 3)
    halves = []
    for nl in range(2):
        row = lax.broadcasted_iota(jnp.int32, (ZN, 128), 0)
        col = lax.broadcasted_iota(jnp.int32, (ZN, 128), 1)
        chosen = jnp.where(col == 8 * row + 2 * y + nl, 1.0, 0.0).astype(bf16)
        halves.append(mm_t(chosen, returned).astype(bf16))
    tail = jnp.concatenate(halves, axis=1)
    left = (total[:, 0:256] + mm(slot, tail)).astype(bf16)
    whole = jnp.concatenate([left, total[:, 256:512].astype(bf16)], axis=1)
    out_ref[...] = whole.reshape(ZN, 4, 512)


def row_col(shape):
    return (
        lax.broadcasted_iota(jnp.int32, shape, 0),
        lax.broadcasted_iota(jnp.int32, shape, 1),
    )


def silu(x):
    return x * jax.nn.sigmoid(x)


def lengths_column(at_ref):
    row = lax.broadcasted_iota(jnp.int32, (8, 1), 0)
    lens = jnp.zeros((8, 1), jnp.int32)
    for s in range(SEQ):
        lens = jnp.where(row == s, at_ref[3 + s], lens)
    return lens


def place_first(col):
    return 8 * (col % NEW) + col // NEW


def place_second(col):
    i = col % 4
    n = 12 * ((col // 4) % 2) + 3 * (col // 8) + i
    return jnp.where(i < 3, 8 * (n % NEW) + n // NEW, -1)


def conv(history_ref, fresh, taps_ref, layer):
    rows = [history_ref[layer, k].astype(f32) for k in range(CONV - 1)]
    rows += [fresh[8 * t : 8 * t + 8] for t in range(NEW)]
    taps = [taps_ref[layer, k : k + 1].astype(f32) for k in range(CONV)]
    return [silu(sum(rows[t + k] * taps[k] for k in range(CONV))) for t in range(NEW)]


def prepare(
    token_hbm,
    weight_hbm,
    history_hbm,
    taps_hbm,
    out_ref,
    token_ref,
    weight_ref,
    history_ref,
    taps_ref,
    stack_ref,
    sems,
):
    moves = [
        pltpu.make_async_copy(source, target, sems.at[n])
        for n, (source, target) in enumerate(
            (
                (history_hbm, history_ref),
                (taps_hbm, taps_ref),
                (token_hbm, token_ref),
                (weight_hbm, weight_ref),
            )
        )
    ]
    for move in moves:
        move.start()
    for move in moves[:3]:
        move.wait()
    stack_ref[...] = jnp.zeros((128, 32), f32)
    at = 0
    for layer in range(LAYERS):
        for s in range(SEQ):
            for k in range(CONV - 1):
                stack_ref[at : at + 2] = history_ref[layer, s, k].astype(f32)
                at += 2
    for layer in range(LAYERS):
        for k in range(CONV):
            stack_ref[at : at + 2] = taps_ref[layer, k].astype(f32)
            at += 2
    turned = jnp.transpose(stack_ref[...])
    tokens = jnp.concatenate([token_ref[...].astype(f32), jnp.zeros((1, 512), f32)], axis=0)
    row, _ = row_col((4, 512))
    for g in range(GROUPS):
        both = [turned[g : g + 1], turned[GROUPS + g : GROUPS + g + 1], jnp.zeros((1, 256), f32)]
        tail = jnp.broadcast_to(jnp.concatenate(both, axis=1), (4, 512))
        out_ref[g, 0] = jnp.where(row == 3, tail, tokens).astype(bf16)

    def source(col):
        c = col % 32
        return 4 * (c % GROUPS) + 2 * (col // 32) + c // GROUPS

    order = one_hot(64, 64, source)
    moves[3].wait()
    for layer in range(LAYERS):
        cols = weight_ref[layer].reshape(64, 512)
        out_ref[:, 1 + layer] = mm(order, cols).astype(bf16).reshape(GROUPS, 4, 512)


def unpack(plane_ref, vhist_ref, vtaps_ref):
    def source(col):
        return jnp.where(col % 8 == 3, 4 * ((col // 8) % ZN) + col // 128, -1)

    small = mm(one_hot(64, 512, source), plane_ref[:, 0:256])
    spread = jnp.zeros((128, 128), f32)
    row, col = row_col((64, 128))
    for nl in range(2):
        turned = jnp.transpose(small[:, 128 * nl : 128 * nl + 128]).astype(bf16)
        spread += mm(turned, jnp.where(col == 2 * row + nl, 1.0, 0.0).astype(bf16))

    def order(m):
        kind = m // 2
        old = 24 * (2 * (m // 36) + m % 2) + 8 * (kind % 3) + (kind // 3) % SEQ
        tap = 96 + 8 * (2 * ((m - 72) // 8) + m % 2) + (kind - 36) % CONV
        return jnp.where(m < 72, old, jnp.where(m < 88, tap, -1))

    rows = mm(one_hot(128, 128, order), spread.astype(bf16)).astype(bf16)
    for layer in range(LAYERS):
        for rw in range(2):
            lanes = slice(128 * rw, 128 * rw + 128)
            for k in range(CONV - 1):
                at = 24 * (2 * layer + rw) + 8 * k
                vhist_ref[layer, k, :, lanes] = rows[at : at + 8]
            at = 96 + 8 * (2 * layer + rw)
            vtaps_ref[layer, :, lanes] = rows[at : at + 8]


def middle(
    at_ref,
    scale_ref,
    part_ref,
    history_ref,
    vhist_ref,
    vtaps_ref,
    state_ref,
    msg_ref,
    keep_ref,
    write_ref,
    decay_ref,
    fresh_ref,
    *,
    layer,
):
    if layer == 0:
        total = sum(part_ref[d].astype(f32) for d in range(DN))
        place = one_hot(32, 24, place_first)
    else:
        rows = [sum(part_ref[y, d].astype(f32) for d in range(DN)) for y in range(YN)]
        total = jnp.concatenate(rows, axis=0)
        place = one_hot(32, 32, place_second)
    tail = total[:, 512:640]
    _, lane = row_col(tail.shape)
    squares = jnp.sum(jnp.where(lane == at_ref[2], tail, 0.0), axis=1, keepdims=True)
    scaled = (total * lax.rsqrt(squares / D + norm_floor)).astype(bf16)
    rows = mm(place, scaled)
    fresh_ref[...] = rows[:, 128:512].astype(bf16)
    gate = rows[:, 0:128]

    head = 8 * at_ref[0] + 2 * at_ref[1]
    tail = rows[:, 512:640]
    _, lane = row_col(tail.shape)
    first = jnp.sum(jnp.where(lane == head, tail, 0.0), axis=1, keepdims=True)
    second = jnp.sum(jnp.where(lane == head + 1, tail, 0.0), axis=1, keepdims=True)
    left = lane < HEAD_DIM
    raw = jnp.where(left, first + scale_ref[2 * layer], second + scale_ref[2 * layer + 1])
    rate = jnp.where(left[:8], scale_ref[4 + 2 * layer], scale_ref[5 + 2 * layer])
    soft = jnp.maximum(raw, 0.0) + jnp.log1p(jnp.exp(-jnp.abs(raw)))
    lens = lengths_column(at_ref)
    live = [jnp.where(lens > t, 1.0, 0.0) for t in range(NEW)]
    step = [soft[8 * t : 8 * t + 8] * live[t] for t in range(NEW)]
    cumulative = []
    for t in range(NEW):
        grown = step[t] * rate
        cumulative.append(grown if t == 0 else cumulative[-1] + grown)

    values = conv(history_ref, rows[:, 128:256], history_ref.at[:, 3], layer)
    vectors = conv(vhist_ref, rows[:, 256:512], vtaps_ref, layer)
    write = [v[:, 0:128] for v in vectors]
    read = [v[:, 128:256] for v in vectors]
    stepped = [values[t] * step[t] for t in range(NEW)]

    reads = jnp.concatenate(read, axis=0).astype(bf16)
    row, _ = row_col((32, 128))
    carried = jnp.zeros((32, 128), f32)
    for s in range(SEQ):
        carried = jnp.where(row % 8 == s, mm_t(reads, state_ref[layer, s].astype(bf16)), carried)

    mixed = []
    for t in range(NEW):
        y = jnp.exp(-cumulative[t]) * carried[8 * t : 8 * t + 8]
        for u in range(t + 1):
            score = jnp.sum(read[t] * write[u], axis=1, keepdims=True)
            y = y + score * jnp.exp(cumulative[u] - cumulative[t]) * stepped[u]
        mixed.append(y * silu(gate[8 * t : 8 * t + 8]) * live[t])
    mixed = jnp.concatenate(mixed, axis=0).astype(bf16)
    row, col = row_col((32, 32))
    i = row % 4
    n = 12 * ((row // 4) % 2) + 3 * (row // 8) + i
    pick = (col == 8 * (n % NEW) + n // NEW) & (i < 3)
    ordered = mm(jnp.where(pick, 1.0, 0.0).astype(bf16), mixed).astype(bf16)
    for y in range(YN):
        for d in range(DN):
            msg_ref[y * DN + d] = ordered[8 * y : 8 * y + 8]

    last = cumulative[-1]
    for t in range(NEW):
        keep_ref[8 * t : 8 * t + 8] = jnp.exp(cumulative[t] - last) * stepped[t]
        write_ref[8 * t : 8 * t + 8] = write[t]
    decay_ref[...] = jnp.exp(-last)


def finish(
    at_ref,
    keep_ref,
    write_ref,
    decay_ref,
    fresh_ref,
    history_ref,
    vhist_ref,
    state_ref,
    next_ref,
    value_ref,
    vector_ref,
    *,
    layer,
):
    kept = jnp.transpose(keep_ref[...])
    _, col = row_col(kept.shape)
    write = write_ref[...].astype(bf16)
    for s in range(SEQ):
        fresh = mm(jnp.where(col % 8 == s, kept, 0.0).astype(bf16), write)
        for h in range(2):
            at = slice(HEAD_DIM * h, HEAD_DIM * h + HEAD_DIM)
            decay = decay_ref[s : s + 1, HEAD_DIM * h : HEAD_DIM * h + 1]
            next_ref[s, at] = state_ref[layer, s, at] * decay + fresh[at]
    lens = lengths_column(at_ref)
    for out_ref, old_ref, lo, hi in (
        (value_ref, history_ref, 0, 128),
        (vector_ref, vhist_ref, 128, 384),
    ):
        rows = [old_ref[layer, k].astype(f32) for k in range(CONV - 1)]
        rows += [fresh_ref[8 * t : 8 * t + 8, lo:hi].astype(f32) for t in range(NEW)]
        for k in range(CONV - 1):
            chosen = rows[k + 1]
            for r in range(k + 2, k + NEW + 1):
                chosen = jnp.where(lens + k == r, rows[r], chosen)
            out_ref[k] = chosen.astype(bf16)


def call(kernel, shapes, scalars, *args):
    vmem = pl.BlockSpec(memory_space=pltpu.VMEM)
    space = [pl.BlockSpec(memory_space=pltpu.SMEM)] * scalars
    space += [vmem] * (len(args) - scalars)
    outs = [jax.ShapeDtypeStruct(shape, dtype) for shape, dtype in shapes]
    results = pl.pallas_call(
        kernel,
        out_shape=outs,
        in_specs=space,
        out_specs=[vmem] * len(outs),
        compiler_params=pltpu.CompilerParams(vmem_limit_bytes=12 << 20),
    )(*args)
    return results[0] if len(outs) == 1 else results


def from_y(value, k):
    return lax.ppermute(value, "y", [(i, (i + k) % YN) for i in range(YN)])


def around_y(value):
    return [value, *(from_y(value, k) for k in range(1, YN))]


def body(
    tokens,
    lengths,
    norm_gain,
    gate_weight,
    value_weight,
    vector_weight,
    step_weight,
    step_bias,
    decay_rate,
    value_taps,
    vector_taps,
    out_weight,
    recurrent_state,
    value_history,
    vector_history,
):
    z = lax.axis_index("z")
    y = lax.axis_index("y")
    square_lane = (8 * z + 64) % HEADS
    first = pl.pallas_call(
        prepare,
        out_shape=jax.ShapeDtypeStruct((ZN, 3, 4, 512), bf16),
        in_specs=[pl.BlockSpec(memory_space=pltpu.MemorySpace.HBM)] * 4,
        out_specs=pl.BlockSpec(memory_space=pltpu.VMEM),
        scratch_shapes=[
            pltpu.VMEM((3, 512), bf16),
            pltpu.VMEM((2, 2, 32, 512), bf16),
            pltpu.VMEM((2, SEQ, 3, 2, 32), bf16),
            pltpu.VMEM((2, CONV, 2, 32), bf16),
            pltpu.VMEM((128, 32), f32),
            pltpu.SemaphoreType.DMA((4,)),
        ],
    )(tokens, vector_weight.transpose(0, 2, 3, 1), vector_history, vector_taps)
    first, own_out = lax.optimization_barrier((first, out_weight))
    first = exchange(first, "z")
    at = jnp.concatenate([jnp.stack([z, y, square_lane]), lengths]).astype(jnp.int32)
    scale = jnp.concatenate([step_bias.reshape(4), decay_rate.reshape(4)])
    own_out = around_y(own_out[0])
    plane = exchange(copies(first[:, :2], YN), "y").reshape(512, 512)
    vhist, vtaps = call(unpack, [((2, 3, 8, 256), bf16), ((2, 8, 256), bf16)], 0, plane)
    history = jnp.pad(value_history.transpose(0, 2, 1, 3), ((0, 0), (0, 1), (0, 2), (0, 0)))
    history += jnp.pad(value_taps[:, None], ((0, 0), (3, 0), (0, 4), (0, 0)))
    gain = jnp.pad(norm_gain, ((0, 6), (0, 0)))
    states = recurrent_state.reshape(LAYERS, SEQ, 128, 128)

    def mid(part, layer):
        old = (history, vhist)
        msg, keep, write, decay, fresh = call(
            functools.partial(middle, layer=layer),
            [
                ((YN * DN, 8, 128), bf16),
                ((32, 128), f32),
                ((32, 128), f32),
                ((8, 128), f32),
                ((32, 384), bf16),
            ],
            2,
            at,
            scale,
            part,
            history,
            vhist,
            vtaps,
            states,
        )
        after = call(
            functools.partial(finish, layer=layer),
            [((SEQ, 128, 128), f32), ((3, 8, 128), bf16), ((3, 8, 256), bf16)],
            1,
            at,
            keep,
            write,
            decay,
            fresh,
            *old,
            states,
        )
        return exchange(msg, ("y", "dp")).reshape(YN, DN * 8, 128), after

    part = call(
        first_projection,
        [((DN, 24, COLS), bf16)],
        1,
        at,
        plane,
        gain,
        gate_weight,
        value_weight,
        step_weight,
    )
    part = exchange(part, "dp")
    mixed, (state0, value0, vector0) = mid(part, 0)
    update = call(
        functools.partial(out_projection, first_row=0),
        [((ZN, 4, 512), bf16)],
        1,
        at,
        mixed,
        *own_out,
    )

    def lanes(w):
        return w.reshape(4, 128, 128).transpose(1, 0, 2).reshape(128, 512)

    later = jnp.concatenate(
        [
            lanes(gate_weight[1]),
            lanes(value_weight[1]),
            out_weight[1],
            first[:, 2].reshape(64, 512),
        ],
        axis=0,
    )
    update, later = lax.optimization_barrier((update, later))
    update = exchange(update, "z")
    pieces = [later, from_y(later, 1), from_y(later, 2)]
    update = jnp.sum(update.astype(f32), axis=0)[:3]
    token_rows = (tokens.astype(f32) + update).astype(bf16)
    quarter = copies(jnp.pad(token_rows, ((0, 1), (0, 0))), ZN)
    quarter, last = lax.optimization_barrier((quarter, later))
    quarter = exchange(quarter, "z")
    last = from_y(last, 3)
    quarter = quarter.reshape(64, 512)
    later = [*pieces, last]
    part = call(
        second_projection,
        [((YN, 64, COLS), bf16)],
        1,
        at,
        quarter,
        gain,
        step_weight,
        *later,
    )
    part = exchange(part.reshape(YN * DN, 8, COLS), ("y", "dp")).reshape(YN, DN, 8, COLS)
    mixed, (state1, value1, vector1) = mid(part, 1)
    update = call(
        functools.partial(out_projection, first_row=256),
        [((ZN, 4, 512), bf16)],
        1,
        at,
        mixed,
        *later,
        jnp.concatenate([vector0, vector1], axis=0).reshape(48, 256),
    )
    update = exchange(update, "z")
    token_rows = (
        token_rows.astype(f32) + jnp.sum(update[:, :3].astype(f32), axis=0)
    ).astype(bf16)
    returned = update[:, 3, :256].reshape(GROUPS, 2, 128)[:, :, :96]
    returned = returned.reshape(GROUPS, 2, 2, 2, 3, 8)[..., :SEQ].transpose(3, 5, 4, 2, 1, 0)
    next_vector = returned.reshape(2, SEQ, 3, 2, 32)
    return (
        token_rows,
        jnp.stack([state0, state1]).reshape(recurrent_state.shape),
        jnp.stack([value0, value1])[:, :, :SEQ].transpose(0, 2, 1, 3),
        next_vector,
    )


def solution(mesh):
    grid = Mesh(mesh.devices.reshape(ZN, YN, DN), ("z", "y", "dp"))
    tp = ("z", "y")
    return jax.shard_map(
        body,
        mesh=grid,
        in_specs=(
            P(tp, "dp"),
            P("dp"),
            P(None, "dp"),
            P(None, "dp", tp),
            P(None, "dp", tp),
            P(None, "dp", None, tp),
            P(None, "dp", None),
            P(None, tp),
            P(None, tp),
            P(None, None, tp),
            P(None, None, None, tp),
            P(None, tp, "dp"),
            P(None, "dp", tp, None, None),
            P(None, "dp", None, tp),
            P(None, "dp", None, None, tp),
        ),
        out_specs=(
            P(tp, "dp"),
            P(None, "dp", tp, None, None),
            P(None, "dp", None, tp),
            P(None, "dp", None, None, tp),
        ),
        check_vma=False,
    )
```

```python
import functools

import jax
import jax.numpy as jnp
from jax import lax
from jax.experimental import pallas as pl
from jax.experimental.pallas import tpu as pltpu
from jax.sharding import Mesh, PartitionSpec as P

D = 4096
HEADS = 128
HEAD_DIM = 64
GROUPS = 16
CONV = 4
NEW = 4
LAYERS = 2
norm_floor = 0.1

ZN, YN, DN = 16, 4, 8
SEQ = 6
bf16 = jnp.bfloat16
f32 = jnp.float32
COLS = 640


def exchange(pieces, axis):
    return lax.all_to_all(pieces, axis, 0, 0, tiled=True)


def copies(value, peers):
    return jnp.broadcast_to(value[None], (peers, *value.shape))


def one_hot(rows, cols, target):
    row = lax.broadcasted_iota(jnp.int32, (rows, cols), 0)
    col = lax.broadcasted_iota(jnp.int32, (rows, cols), 1)
    return jnp.where(row == target(col), 1.0, 0.0).astype(bf16)


def mm(a, b):
    return lax.dot_general(a, b, (((1,), (0,)), ((), ())), preferred_element_type=f32)


def mm_t(a, b):
    return lax.dot_general(a, b, (((1,), (1,)), ((), ())), preferred_element_type=f32)


def normed_rows(rows, gain):
    widened = rows.astype(f32)
    squares = jnp.sum(widened * widened, axis=1, keepdims=True)
    return (widened * gain).astype(bf16), squares


def step_lanes(at_ref, normed, squares, step_w):
    step = mm(normed, step_w)
    lane = lax.broadcasted_iota(jnp.int32, step.shape, 1)
    return jnp.where(lane == at_ref[2], squares, step)


def first_projection(at_ref, plane_ref, misc_ref, gate_ref, value_ref, step_ref, out_ref):
    plane = plane_ref[...]

    def token_source(col):
        i = col % 8
        return jnp.where(i < 3, 12 * ((col // 8) % ZN) + 3 * (col // 128) + i, -1)

    def vector_source(col):
        j = col % 8 - 4
        n = 8 * ((col // 8) % ZN) + 2 * (col // 128) + j % 2
        return jnp.where((j >= 0) & (j < 4), 128 * (j // 2) + n, -1)

    rows = mm(one_hot(192, 512, token_source), plane).astype(bf16)
    vector_w = mm(one_hot(256, 512, vector_source), plane).astype(bf16)
    normed, squares = normed_rows(rows, gain_row(misc_ref, 0))
    parts = [
        mm(normed, gate_ref[0]),
        mm(normed, value_ref[0]),
        mm_t(normed, vector_w),
        step_lanes(at_ref, normed, squares, step_ref[0]),
    ]
    at = 0
    for part in parts:
        width = part.shape[1]
        out_ref[:, :, at : at + width] = part.astype(bf16).reshape(DN, 24, width)
        at += width


def second_projection(at_ref, rows_ref, misc_ref, step_ref, w0, w1, w2, w3, out_ref):
    y = at_ref[1]
    normed, squares = normed_rows(rows_ref[...], gain_row(misc_ref, 1))
    pieces = [w0, w1, w2, w3]

    def source(col):
        j = col % 4
        n = 8 * ((col // 4) % ZN) + 2 * ((y - col // 64) % YN) + j % 2
        return 128 * (j // 2) + n

    stacked = jnp.concatenate(
        [
            jnp.concatenate([w[1024 + 64 * b : 1088 + 64 * b] for b in range(4)], axis=1)
            for w in pieces
        ],
        axis=0,
    )
    vector_w = mm(one_hot(256, 256, source), stacked).astype(bf16)
    vector = mm_t(normed, vector_w).astype(bf16)
    extra = step_lanes(at_ref, normed, squares, step_ref[0]).astype(bf16)
    for k, w in enumerate(pieces):
        to = (y - k) % YN
        for n in range(2):
            total = mm(normed, w[512 * n : 512 * n + 512])
            out_ref[to, :, 128 * n : 128 * n + 128] = total.astype(bf16)
        out_ref[to, :, 256:512] = vector
        out_ref[to, :, 512:640] = extra


def out_projection(at_ref, mixed_ref, w0, w1, w2, w3, *rest, first_row):
    y = at_ref[1]
    total = jnp.zeros((64, 512), f32)
    for k, w in enumerate([w0, w1, w2, w3]):
        total += mm(mixed_ref[(y - k) % YN], w[first_row : first_row + 128])
    if len(rest) == 1:
        rest[0][...] = total.astype(bf16).reshape(ZN, 4, 512)
        return
    returned_ref, out_ref = rest
    returned = jnp.concatenate(
        [returned_ref[:, 0:128], returned_ref[:, 128:256], jnp.zeros((32, 128), bf16)], axis=0
    )
    slot = one_hot(64, ZN, lambda col: 4 * col + 3)
    halves = []
    for nl in range(2):
        row = lax.broadcasted_iota(jnp.int32, (ZN, 128), 0)
        col = lax.broadcasted_iota(jnp.int32, (ZN, 128), 1)
        chosen = jnp.where(col == 8 * row + 2 * y + nl, 1.0, 0.0).astype(bf16)
        halves.append(mm_t(chosen, returned).astype(bf16))
    tail = jnp.concatenate(halves, axis=1)
    left = (total[:, 0:256] + mm(slot, tail)).astype(bf16)
    whole = jnp.concatenate([left, total[:, 256:512].astype(bf16)], axis=1)
    out_ref[...] = whole.reshape(ZN, 4, 512)


def row_col(shape):
    return (
        lax.broadcasted_iota(jnp.int32, shape, 0),
        lax.broadcasted_iota(jnp.int32, shape, 1),
    )


def silu(x):
    return x * jax.nn.sigmoid(x)


def place_first(col):
    return 8 * (col % NEW) + col // NEW


def place_second(col):
    i = col % 4
    n = 12 * ((col // 4) % 2) + 3 * (col // 8) + i
    return jnp.where(i < 3, 8 * (n % NEW) + n // NEW, -1)


def conv(old, taps, fresh):
    rows = old + [fresh[8 * t : 8 * t + 8] for t in range(NEW)]
    return [silu(sum(rows[t + k] * taps[k] for k in range(CONV))) for t in range(NEW)]


def old_values(misc_ref, layer):
    return [misc_ref[32 * layer + 8 * k : 32 * layer + 8 * k + 8] for k in range(CONV - 1)]


def old_vectors(vhist_ref, layer):
    return [vhist_ref[layer, k].astype(f32) for k in range(CONV - 1)]


def setup(
    len_ref,
    gain_hbm,
    bias_hbm,
    rate_hbm,
    taps_hbm,
    history_hbm,
    gate_hbm,
    value_hbm,
    misc_ref,
    base_ref,
    gain_ref,
    bias_ref,
    rate_ref,
    taps_ref,
    history_ref,
    sems,
):
    pairs = (
        (gain_hbm, gain_ref),
        (bias_hbm, bias_ref),
        (rate_hbm, rate_ref),
        (taps_hbm, taps_ref),
        (history_hbm, history_ref),
        (gate_hbm.at[1], base_ref.at[0:512]),
        (value_hbm.at[1], base_ref.at[512:1024]),
    )
    moves = [pltpu.make_async_copy(a, b, sems.at[n]) for n, (a, b) in enumerate(pairs)]
    for move in moves:
        move.start()
    row, lane = row_col((8, 128))
    lens = jnp.zeros((8, 128), f32)
    for s in range(SEQ):
        lens = jnp.where(row == s, len_ref[s].astype(f32), lens)
    misc_ref[0:64] = jnp.zeros((64, 128), f32)
    misc_ref[64:72] = lens
    misc_ref[72:80] = jnp.zeros((8, 128), f32)
    for move in moves:
        move.wait()
    left = lane[0:1] < HEAD_DIM
    for layer in range(LAYERS):
        for n, ref in enumerate((bias_ref, rate_ref)):
            both = jnp.where(left, ref[layer : layer + 1, 0:1], ref[layer : layer + 1, 1:2])
            misc_ref[72 + 2 * layer + n : 73 + 2 * layer + n] = both
        for b in range(4):
            part = gain_ref[layer : layer + 1, 128 * b : 128 * b + 128]
            misc_ref[80 + 4 * layer + b : 81 + 4 * layer + b] = part
        for k in range(CONV - 1):
            at = 32 * layer + 8 * k
            for s in range(SEQ):
                misc_ref[at + s : at + s + 1] = history_ref[s, k, layer : layer + 1].astype(f32)
        at = 32 * layer + 24
        misc_ref[at : at + CONV] = taps_ref[layer].astype(f32)


def gain_row(misc_ref, layer):
    parts = [misc_ref[80 + 4 * layer + b : 81 + 4 * layer + b] for b in range(4)]
    return jnp.concatenate(parts, axis=1)


def prepare(
    token_hbm,
    weight_hbm,
    history_hbm,
    taps_hbm,
    out_ref,
    token_ref,
    weight_ref,
    history_ref,
    taps_ref,
    stack_ref,
    sems,
):
    moves = [
        pltpu.make_async_copy(source, target, sems.at[n])
        for n, (source, target) in enumerate(
            (
                (history_hbm, history_ref),
                (taps_hbm, taps_ref),
                (token_hbm, token_ref),
                (weight_hbm, weight_ref),
            )
        )
    ]
    for move in moves:
        move.start()
    for move in moves[:3]:
        move.wait()
    stack_ref[...] = jnp.zeros((128, 32), f32)
    at = 0
    for layer in range(LAYERS):
        for s in range(SEQ):
            for k in range(CONV - 1):
                stack_ref[at : at + 2] = history_ref[layer, s, k].astype(f32)
                at += 2
    for layer in range(LAYERS):
        for k in range(CONV):
            stack_ref[at : at + 2] = taps_ref[layer, k].astype(f32)
            at += 2
    turned = jnp.transpose(stack_ref[...])
    tokens = jnp.concatenate([token_ref[...].astype(f32), jnp.zeros((1, 512), f32)], axis=0)
    row, _ = row_col((4, 512))
    for g in range(GROUPS):
        both = [turned[g : g + 1], turned[GROUPS + g : GROUPS + g + 1], jnp.zeros((1, 256), f32)]
        tail = jnp.broadcast_to(jnp.concatenate(both, axis=1), (4, 512))
        out_ref[g, 0] = jnp.where(row == 3, tail, tokens).astype(bf16)

    def source(col):
        c = col % 32
        return 4 * (c % GROUPS) + 2 * (col // 32) + c // GROUPS

    order = one_hot(64, 64, source)
    moves[3].wait()
    for layer in range(LAYERS):
        cols = weight_ref[layer].reshape(64, 512)
        out_ref[:, 1 + layer] = mm(order, cols).astype(bf16).reshape(GROUPS, 4, 512)


def unpack(plane_ref, vhist_ref, vtaps_ref):
    def source(col):
        return jnp.where(col % 8 == 3, 4 * ((col // 8) % ZN) + col // 128, -1)

    small = mm(one_hot(64, 512, source), plane_ref[:, 0:256])
    spread = jnp.zeros((128, 128), f32)
    row, col = row_col((64, 128))
    for nl in range(2):
        turned = jnp.transpose(small[:, 128 * nl : 128 * nl + 128]).astype(bf16)
        spread += mm(turned, jnp.where(col == 2 * row + nl, 1.0, 0.0).astype(bf16))

    def order(m):
        kind = m // 2
        old = 24 * (2 * (m // 36) + m % 2) + 8 * (kind % 3) + (kind // 3) % SEQ
        tap = 96 + 8 * (2 * ((m - 72) // 8) + m % 2) + (kind - 36) % CONV
        return jnp.where(m < 72, old, jnp.where(m < 88, tap, -1))

    rows = mm(one_hot(128, 128, order), spread.astype(bf16)).astype(bf16)
    for layer in range(LAYERS):
        for rw in range(2):
            lanes = slice(128 * rw, 128 * rw + 128)
            for k in range(CONV - 1):
                at = 24 * (2 * layer + rw) + 8 * k
                vhist_ref[layer, k, :, lanes] = rows[at : at + 8]
            at = 96 + 8 * (2 * layer + rw)
            vtaps_ref[layer, :, lanes] = rows[at : at + 8]


def middle(
    at_ref,
    part_ref,
    misc_ref,
    vhist_ref,
    vtaps_ref,
    state_ref,
    msg_ref,
    keep_ref,
    write_ref,
    decay_ref,
    fresh_ref,
    *,
    layer,
):
    if layer == 0:
        total = sum(part_ref[d].astype(f32) for d in range(DN))
        place = one_hot(32, 24, place_first)
    else:
        rows = [sum(part_ref[y, d].astype(f32) for d in range(DN)) for y in range(YN)]
        total = jnp.concatenate(rows, axis=0)
        place = one_hot(32, 32, place_second)
    tail = total[:, 512:640]
    _, lane = row_col(tail.shape)
    squares = jnp.sum(jnp.where(lane == at_ref[2], tail, 0.0), axis=1, keepdims=True)
    scaled = (total * lax.rsqrt(squares / D + norm_floor)).astype(bf16)
    rows = mm(place, scaled)
    fresh_ref[...] = rows[:, 128:512].astype(bf16)
    gate = rows[:, 0:128]

    head = 8 * at_ref[0] + 2 * at_ref[1]
    tail = rows[:, 512:640]
    _, lane = row_col(tail.shape)
    first = jnp.sum(jnp.where(lane == head, tail, 0.0), axis=1, keepdims=True)
    second = jnp.sum(jnp.where(lane == head + 1, tail, 0.0), axis=1, keepdims=True)
    left = lane < HEAD_DIM
    at = 72 + 2 * layer
    raw = jnp.where(left, first, second) + misc_ref[at : at + 1]
    rate = misc_ref[at + 1 : at + 2]
    soft = jnp.maximum(raw, 0.0) + jnp.log1p(jnp.exp(-jnp.abs(raw)))
    lens = misc_ref[64:72, 0:1]
    live = [jnp.where(lens > t, 1.0, 0.0) for t in range(NEW)]
    step = [soft[8 * t : 8 * t + 8] * live[t] for t in range(NEW)]
    cumulative = []
    for t in range(NEW):
        grown = step[t] * rate
        cumulative.append(grown if t == 0 else cumulative[-1] + grown)

    at = 32 * layer + 24
    taps = [misc_ref[at + k : at + k + 1] for k in range(CONV)]
    values = conv(old_values(misc_ref, layer), taps, rows[:, 128:256])
    taps = [vtaps_ref[layer, k : k + 1].astype(f32) for k in range(CONV)]
    vectors = conv(old_vectors(vhist_ref, layer), taps, rows[:, 256:512])
    write = [v[:, 0:128] for v in vectors]
    read = [v[:, 128:256] for v in vectors]
    stepped = [values[t] * step[t] for t in range(NEW)]

    reads = jnp.concatenate(read, axis=0).astype(bf16)
    row, _ = row_col((32, 128))
    carried = jnp.zeros((32, 128), f32)
    for s in range(SEQ):
        carried = jnp.where(row % 8 == s, mm_t(reads, state_ref[0, s].astype(bf16)), carried)

    mixed = []
    for t in range(NEW):
        y = jnp.exp(-cumulative[t]) * carried[8 * t : 8 * t + 8]
        for u in range(t + 1):
            score = jnp.sum(read[t] * write[u], axis=1, keepdims=True)
            y = y + score * jnp.exp(cumulative[u] - cumulative[t]) * stepped[u]
        mixed.append(y * silu(gate[8 * t : 8 * t + 8]) * live[t])
    mixed = jnp.concatenate(mixed, axis=0).astype(bf16)
    row, col = row_col((32, 32))
    i = row % 4
    n = 12 * ((row // 4) % 2) + 3 * (row // 8) + i
    pick = (col == 8 * (n % NEW) + n // NEW) & (i < 3)
    ordered = mm(jnp.where(pick, 1.0, 0.0).astype(bf16), mixed).astype(bf16)
    for y in range(YN):
        for d in range(DN):
            msg_ref[y * DN + d] = ordered[8 * y : 8 * y + 8]

    last = cumulative[-1]
    for t in range(NEW):
        keep_ref[8 * t : 8 * t + 8] = jnp.exp(cumulative[t] - last) * stepped[t]
        write_ref[8 * t : 8 * t + 8] = write[t]
    decay_ref[...] = jnp.exp(-last)


def finish(
    misc_ref,
    keep_ref,
    write_ref,
    decay_ref,
    fresh_ref,
    vhist_ref,
    state_ref,
    *rest,
    layer,
):
    next_ref, value_ref, vector_ref = rest[-3:]
    kept = jnp.transpose(keep_ref[...])
    _, col = row_col(kept.shape)
    write = write_ref[...].astype(bf16)
    for s in range(SEQ):
        fresh = mm(jnp.where(col % 8 == s, kept, 0.0).astype(bf16), write)
        for h in range(2):
            at = slice(HEAD_DIM * h, HEAD_DIM * h + HEAD_DIM)
            decay = decay_ref[s : s + 1, HEAD_DIM * h : HEAD_DIM * h + 1]
            next_ref[0, s, at] = state_ref[0, s, at] * decay + fresh[at]
    lens = misc_ref[64:72, 0:1]
    for out_ref, old, lo, hi in (
        (value_ref, old_values(misc_ref, layer), 0, 128),
        (vector_ref, old_vectors(vhist_ref, layer), 128, 384),
    ):
        rows = old + [fresh_ref[8 * t : 8 * t + 8, lo:hi].astype(f32) for t in range(NEW)]
        for k in range(CONV - 1):
            chosen = rows[k + 1]
            for r in range(k + 2, k + NEW + 1):
                chosen = jnp.where(lens + k == r, rows[r], chosen)
            out_ref[k] = chosen.astype(bf16)


def call(kernel, shapes, scalars, *args):
    vmem = pl.BlockSpec(memory_space=pltpu.VMEM)
    space = [pl.BlockSpec(memory_space=pltpu.SMEM)] * scalars
    space += [vmem] * (len(args) - scalars)
    outs = [jax.ShapeDtypeStruct(shape, dtype) for shape, dtype in shapes]
    results = pl.pallas_call(
        kernel,
        out_shape=outs,
        in_specs=space,
        out_specs=[vmem] * len(outs),
        compiler_params=pltpu.CompilerParams(vmem_limit_bytes=12 << 20),
    )(*args)
    return results[0] if len(outs) == 1 else results


def close(layer, *args):
    vmem = pl.BlockSpec(memory_space=pltpu.VMEM)
    block = pl.BlockSpec((1, SEQ, 128, 128), lambda i: (layer, 0, 0, 0))
    space = [vmem] * 7 + [pl.BlockSpec(memory_space=pl.ANY)] * (len(args) - 7)
    return pl.pallas_call(
        functools.partial(finish, layer=layer),
        grid=(1,),
        out_shape=[
            jax.ShapeDtypeStruct((LAYERS, SEQ, 128, 128), f32),
            jax.ShapeDtypeStruct((3, 8, 128), bf16),
            jax.ShapeDtypeStruct((3, 8, 256), bf16),
        ],
        in_specs=space,
        out_specs=[block, vmem, vmem],
        input_output_aliases={7: 0} if layer else {},
        compiler_params=pltpu.CompilerParams(vmem_limit_bytes=12 << 20),
    )(*args)


def from_y(value, k):
    return lax.ppermute(value, "y", [(i, (i + k) % YN) for i in range(YN)])


def body(
    tokens,
    lengths,
    norm_gain,
    gate_weight,
    value_weight,
    vector_weight,
    step_weight,
    step_bias,
    decay_rate,
    value_taps,
    vector_taps,
    out_weight,
    recurrent_state,
    value_history,
    vector_history,
):
    z = lax.axis_index("z")
    y = lax.axis_index("y")
    square_lane = (8 * z + 64) % HEADS
    first = pl.pallas_call(
        prepare,
        out_shape=jax.ShapeDtypeStruct((ZN, 3, 4, 512), bf16),
        in_specs=[pl.BlockSpec(memory_space=pltpu.MemorySpace.HBM)] * 4,
        out_specs=pl.BlockSpec(memory_space=pltpu.VMEM),
        scratch_shapes=[
            pltpu.VMEM((3, 512), bf16),
            pltpu.VMEM((2, 2, 32, 512), bf16),
            pltpu.VMEM((2, SEQ, 3, 2, 32), bf16),
            pltpu.VMEM((2, CONV, 2, 32), bf16),
            pltpu.VMEM((128, 32), f32),
            pltpu.SemaphoreType.DMA((4,)),
        ],
    )(tokens, vector_weight.transpose(0, 2, 3, 1), vector_history, vector_taps)
    first, outs, lens = lax.optimization_barrier(
        (first, out_weight.reshape(256, 512), lengths)
    )
    first = exchange(first, "z")
    out_2 = from_y(outs, 2)
    at = jnp.stack([z, y, square_lane]).astype(jnp.int32)
    misc, base = pl.pallas_call(
        setup,
        out_shape=[jax.ShapeDtypeStruct((88, 128), f32), jax.ShapeDtypeStruct((1280, 128), bf16)],
        in_specs=[pl.BlockSpec(memory_space=pltpu.SMEM)]
        + [pl.BlockSpec(memory_space=pltpu.MemorySpace.HBM)] * 7,
        out_specs=[pl.BlockSpec(memory_space=pltpu.VMEM)] * 2,
        scratch_shapes=[
            pltpu.VMEM((2, 512), f32),
            pltpu.VMEM((2, 2), f32),
            pltpu.VMEM((2, 2), f32),
            pltpu.VMEM((2, CONV, 128), bf16),
            pltpu.VMEM((SEQ, 3, 2, 128), bf16),
            pltpu.SemaphoreType.DMA((7,)),
        ],
    )(
        lens,
        norm_gain,
        step_bias,
        decay_rate,
        value_taps,
        value_history.transpose(1, 2, 0, 3),
        gate_weight,
        value_weight,
    )
    plane = exchange(copies(first[:, :2], YN), "y").reshape(512, 512)
    out_1 = from_y(outs, 1)
    out_3 = from_y(outs, 3)
    outs = [outs, out_1, out_2, out_3]
    blocks = first[:, 2].reshape(64, 4, 128).transpose(1, 0, 2).reshape(256, 128)
    later = lax.dynamic_update_slice(base, blocks, (1024, 0))
    vhist, vtaps = call(unpack, [((2, 3, 8, 256), bf16), ((2, 8, 256), bf16)], 0, plane)
    states = [recurrent_state[n : n + 1].reshape(1, SEQ, 128, 128) for n in range(LAYERS)]

    def mid(part, layer, *done):
        msg, keep, write, decay, fresh = call(
            functools.partial(middle, layer=layer),
            [
                ((YN * DN, 8, 128), bf16),
                ((32, 128), f32),
                ((32, 128), f32),
                ((8, 128), f32),
                ((32, 384), bf16),
            ],
            1,
            at,
            part,
            misc,
            vhist,
            vtaps,
            states[layer],
        )
        after = close(layer, misc, keep, write, decay, fresh, vhist, states[layer], *done)
        msg = exchange(msg, ("y", "dp"))
        return msg.reshape(YN, DN * 8, 128), after

    part = call(
        first_projection,
        [((DN, 24, COLS), bf16)],
        1,
        at,
        plane,
        misc,
        gate_weight,
        value_weight,
        step_weight,
    )
    part = exchange(part, "dp")
    later_2 = from_y(later, 2)
    mixed, (state, value0, vector0) = mid(part, 0)
    later_3 = from_y(later, 3)
    update = call(
        functools.partial(out_projection, first_row=0),
        [((ZN, 4, 512), bf16)],
        1,
        at,
        mixed,
        *outs,
    )
    update = exchange(update, "z")
    later_1 = from_y(later, 1)
    update = jnp.sum(update.astype(f32), axis=0)[:3]
    token_rows = (tokens.astype(f32) + update).astype(bf16)
    quarter = copies(jnp.pad(token_rows, ((0, 1), (0, 0))), ZN)
    quarter = exchange(quarter, "z").reshape(64, 512)
    later = [later, later_1, later_2, later_3]
    part = call(
        second_projection,
        [((YN, 64, COLS), bf16)],
        1,
        at,
        quarter,
        misc,
        step_weight[1:],
        *later,
    )
    part = exchange(part.reshape(YN * DN, 8, COLS), ("y", "dp")).reshape(YN, DN, 8, COLS)
    mixed, (state, value1, vector1) = mid(part, 1, state)
    update = call(
        functools.partial(out_projection, first_row=128),
        [((ZN, 4, 512), bf16)],
        1,
        at,
        mixed,
        *outs,
        jnp.concatenate([vector0, vector1], axis=0).reshape(48, 256),
    )
    update = exchange(update, "z")
    token_rows = (
        token_rows.astype(f32) + jnp.sum(update[:, :3].astype(f32), axis=0)
    ).astype(bf16)
    returned = update[:, 3, :256].reshape(GROUPS, 2, 128)[:, :, :96]
    returned = returned.reshape(GROUPS, 2, 2, 2, 3, 8)[..., :SEQ].transpose(3, 5, 4, 2, 1, 0)
    next_vector = returned.reshape(2, SEQ, 3, 2, 32)
    return (
        token_rows,
        state.reshape(recurrent_state.shape),
        jnp.stack([value0, value1])[:, :, :SEQ].transpose(0, 2, 1, 3),
        next_vector,
    )


def solution(mesh):
    grid = Mesh(mesh.devices.reshape(ZN, YN, DN), ("z", "y", "dp"))
    tp = ("z", "y")

    return jax.shard_map(
        body,
        mesh=grid,
        in_specs=(
            P(tp, "dp"),
            P("dp"),
            P(None, "dp"),
            P(None, "dp", tp),
            P(None, "dp", tp),
            P(None, "dp", None, tp),
            P(None, "dp", None),
            P(None, tp),
            P(None, tp),
            P(None, None, tp),
            P(None, None, None, tp),
            P(None, tp, "dp"),
            P(None, "dp", tp, None, None),
            P(None, "dp", None, tp),
            P(None, "dp", None, None, tp),
        ),
        out_specs=(
            P(tp, "dp"),
            P(None, "dp", tp, None, None),
            P(None, "dp", None, tp),
            P(None, "dp", None, None, tp),
        ),
        check_vma=False,
    )
```

```python
import functools

import jax
import jax.numpy as jnp
from jax import lax
from jax.experimental import pallas as pl
from jax.experimental.pallas import tpu as pltpu
from jax.sharding import Mesh, PartitionSpec as P

D = 4096
HEADS = 128
HEAD_DIM = 64
GROUPS = 16
CONV = 4
NEW = 4
LAYERS = 2
norm_floor = 0.1

ZN, YN, DN = 16, 4, 8
SEQ = 6
bf16 = jnp.bfloat16
f32 = jnp.float32
COLS = 640


def exchange(pieces, axis):
    return lax.all_to_all(pieces, axis, 0, 0, tiled=True)


def copies(value, peers):
    return jnp.broadcast_to(value[None], (peers, *value.shape))


def one_hot(rows, cols, target):
    row = lax.broadcasted_iota(jnp.int32, (rows, cols), 0)
    col = lax.broadcasted_iota(jnp.int32, (rows, cols), 1)
    return jnp.where(row == target(col), 1.0, 0.0).astype(bf16)


def mm(a, b):
    return lax.dot_general(a, b, (((1,), (0,)), ((), ())), preferred_element_type=f32)


def mm_t(a, b):
    return lax.dot_general(a, b, (((1,), (1,)), ((), ())), preferred_element_type=f32)


def normed_rows(rows, gain):
    widened = rows.astype(f32)
    squares = jnp.sum(widened * widened, axis=1, keepdims=True)
    return (widened * gain).astype(bf16), squares


def square_lane():
    return (8 * lax.axis_index("z") + 64) % HEADS


def step_lanes(normed, squares, step_w):
    step = mm(normed, step_w)
    lane = lax.broadcasted_iota(jnp.int32, step.shape, 1)
    return jnp.where(lane == square_lane(), squares, step)


def first_projection(plane_ref, misc_ref, weight_ref, out_ref):
    plane = plane_ref[...].reshape(512, 512)

    def token_source(col):
        i = col % 8
        return jnp.where(i < 3, 12 * ((col // 8) % ZN) + 3 * (col // 128) + i, -1)

    def vector_source(col):
        j = col % 8 - 4
        n = 8 * ((col // 8) % ZN) + 2 * (col // 128) + j % 2
        return jnp.where((j >= 0) & (j < 4), 128 * (j // 2) + n, -1)

    rows = mm(one_hot(192, 512, token_source), plane).astype(bf16)
    vector_w = mm(one_hot(256, 512, vector_source), plane).astype(bf16)
    normed, squares = normed_rows(rows, gain_row(misc_ref, 0))
    parts = [
        mm(normed, weight_ref[:, 0:128]),
        mm(normed, weight_ref[:, 128:256]),
        mm_t(normed, vector_w),
        step_lanes(normed, squares, weight_ref[:, 256:384]),
    ]
    at = 0
    for part in parts:
        width = part.shape[1]
        out_ref[:, :, at : at + width] = part.astype(bf16).reshape(DN, 24, width)
        at += width


def second_projection(rows_ref, misc_ref, step_ref, w0, w1, w2, w3, out_ref):
    y = lax.axis_index("y")
    normed, squares = normed_rows(rows_ref[...], gain_row(misc_ref, 1))
    pieces = [w0, w1, w2, w3]

    def source(col):
        j = col % 4
        n = 8 * ((col // 4) % ZN) + 2 * ((y - col // 64) % YN) + j % 2
        return 128 * (j // 2) + n

    stacked = jnp.concatenate(
        [
            jnp.concatenate([w[1024 + 64 * b : 1088 + 64 * b] for b in range(4)], axis=1)
            for w in pieces
        ],
        axis=0,
    )
    vector_w = mm(one_hot(256, 256, source), stacked).astype(bf16)
    vector = mm_t(normed, vector_w).astype(bf16)
    extra = step_lanes(normed, squares, step_ref[0]).astype(bf16)
    for k, w in enumerate(pieces):
        to = (y - k) % YN
        for n in range(2):
            total = mm(normed, w[512 * n : 512 * n + 512])
            out_ref[to, :, 128 * n : 128 * n + 128] = total.astype(bf16)
        out_ref[to, :, 256:512] = vector
        out_ref[to, :, 512:640] = extra


def out_projection(mixed_ref, w0, w1, w2, w3, *rest, first_row):
    y = lax.axis_index("y")
    total = jnp.zeros((64, 512), f32)
    for k, w in enumerate([w0, w1, w2, w3]):
        total += mm(mixed_ref[(y - k) % YN], w[first_row : first_row + 128])
    if len(rest) == 1:
        rest[0][...] = total.astype(bf16).reshape(ZN, 4, 512)
        return
    returned_ref, out_ref = rest
    returned = jnp.concatenate(
        [returned_ref[:, 0:128], returned_ref[:, 128:256], jnp.zeros((32, 128), bf16)], axis=0
    )
    slot = one_hot(64, ZN, lambda col: 4 * col + 3)
    halves = []
    for nl in range(2):
        row = lax.broadcasted_iota(jnp.int32, (ZN, 128), 0)
        col = lax.broadcasted_iota(jnp.int32, (ZN, 128), 1)
        chosen = jnp.where(col == 8 * row + 2 * y + nl, 1.0, 0.0).astype(bf16)
        halves.append(mm_t(chosen, returned).astype(bf16))
    tail = jnp.concatenate(halves, axis=1)
    left = (total[:, 0:256] + mm(slot, tail)).astype(bf16)
    whole = jnp.concatenate([left, total[:, 256:512].astype(bf16)], axis=1)
    out_ref[...] = whole.reshape(ZN, 4, 512)


def row_col(shape):
    return (
        lax.broadcasted_iota(jnp.int32, shape, 0),
        lax.broadcasted_iota(jnp.int32, shape, 1),
    )


def silu(x):
    return x * jax.nn.sigmoid(x)


def place_first(col):
    return 8 * (col % NEW) + col // NEW


def place_second(col):
    i = col % 4
    n = 12 * ((col // 4) % 2) + 3 * (col // 8) + i
    return jnp.where(i < 3, 8 * (n % NEW) + n // NEW, -1)


def conv(old, taps, fresh):
    rows = old + [fresh[8 * t : 8 * t + 8] for t in range(NEW)]
    return [silu(sum(rows[t + k] * taps[k] for k in range(CONV))) for t in range(NEW)]


def old_values(misc_ref, layer):
    return [misc_ref[32 * layer + 8 * k : 32 * layer + 8 * k + 8] for k in range(CONV - 1)]


def old_vectors(vhist_ref, layer):
    return [vhist_ref[layer, k].astype(f32) for k in range(CONV - 1)]


def setup(
    len_ref,
    gain_hbm,
    bias_hbm,
    rate_hbm,
    taps_hbm,
    history_hbm,
    gate_hbm,
    value_hbm,
    misc_ref,
    base_ref,
    gain_ref,
    bias_ref,
    rate_ref,
    taps_ref,
    history_ref,
    sems,
):
    pairs = (
        (gain_hbm, gain_ref),
        (bias_hbm, bias_ref),
        (rate_hbm, rate_ref),
        (taps_hbm, taps_ref),
        (history_hbm, history_ref),
        (gate_hbm.at[1], base_ref.at[0:512]),
        (value_hbm.at[1], base_ref.at[512:1024]),
    )
    moves = [pltpu.make_async_copy(a, b, sems.at[n]) for n, (a, b) in enumerate(pairs)]
    for move in moves:
        move.start()
    row, lane = row_col((8, 128))
    lens = jnp.zeros((8, 128), f32)
    for s in range(SEQ):
        lens = jnp.where(row == s, len_ref[s].astype(f32), lens)
    misc_ref[0:64] = jnp.zeros((64, 128), f32)
    misc_ref[64:72] = lens
    misc_ref[72:80] = jnp.zeros((8, 128), f32)
    for move in moves:
        move.wait()
    left = lane[0:1] < HEAD_DIM
    for layer in range(LAYERS):
        for n, ref in enumerate((bias_ref, rate_ref)):
            both = jnp.where(left, ref[layer : layer + 1, 0:1], ref[layer : layer + 1, 1:2])
            misc_ref[72 + 2 * layer + n : 73 + 2 * layer + n] = both
        for b in range(4):
            part = gain_ref[layer : layer + 1, 128 * b : 128 * b + 128]
            misc_ref[80 + 4 * layer + b : 81 + 4 * layer + b] = part
        for k in range(CONV - 1):
            at = 32 * layer + 8 * k
            for s in range(SEQ):
                misc_ref[at + s : at + s + 1] = history_ref[s, k, layer : layer + 1].astype(f32)
        at = 32 * layer + 24
        misc_ref[at : at + CONV] = taps_ref[layer].astype(f32)


def gain_row(misc_ref, layer):
    parts = [misc_ref[80 + 4 * layer + b : 81 + 4 * layer + b] for b in range(4)]
    return jnp.concatenate(parts, axis=1)


def prepare(
    token_hbm,
    weight_hbm,
    history_hbm,
    taps_hbm,
    out_ref,
    token_ref,
    weight_ref,
    history_ref,
    taps_ref,
    stack_ref,
    sems,
):
    moves = [
        pltpu.make_async_copy(source, target, sems.at[n])
        for n, (source, target) in enumerate(
            (
                (history_hbm, history_ref),
                (taps_hbm, taps_ref),
                (token_hbm, token_ref),
                (weight_hbm, weight_ref),
            )
        )
    ]
    for move in moves:
        move.start()
    for move in moves[:3]:
        move.wait()
    stack_ref[...] = jnp.zeros((128, 32), f32)
    at = 0
    for layer in range(LAYERS):
        for s in range(SEQ):
            for k in range(CONV - 1):
                stack_ref[at : at + 2] = history_ref[layer, s, k].astype(f32)
                at += 2
    for layer in range(LAYERS):
        for k in range(CONV):
            stack_ref[at : at + 2] = taps_ref[layer, k].astype(f32)
            at += 2
    turned = jnp.transpose(stack_ref[...])
    tokens = jnp.concatenate([token_ref[...].astype(f32), jnp.zeros((1, 512), f32)], axis=0)
    row, _ = row_col((4, 512))
    for g in range(GROUPS):
        both = [turned[g : g + 1], turned[GROUPS + g : GROUPS + g + 1], jnp.zeros((1, 256), f32)]
        tail = jnp.broadcast_to(jnp.concatenate(both, axis=1), (4, 512))
        out_ref[g, 0] = jnp.where(row == 3, tail, tokens).astype(bf16)

    def source(col):
        c = col % 32
        return 4 * (c % GROUPS) + 2 * (col // 32) + c // GROUPS

    order = one_hot(64, 64, source)
    moves[3].wait()
    for layer in range(LAYERS):
        cols = weight_ref[layer].reshape(64, 512)
        out_ref[:, 1 + layer] = mm(order, cols).astype(bf16).reshape(GROUPS, 4, 512)


def unpack(plane_ref, vhist_ref, vtaps_ref):
    def source(col):
        return jnp.where(col % 8 == 3, 4 * ((col // 8) % ZN) + col // 128, -1)

    small = mm(one_hot(64, 512, source), plane_ref[:, :, 0:256].reshape(512, 256))
    spread = jnp.zeros((128, 128), f32)
    row, col = row_col((64, 128))
    for nl in range(2):
        turned = jnp.transpose(small[:, 128 * nl : 128 * nl + 128]).astype(bf16)
        spread += mm(turned, jnp.where(col == 2 * row + nl, 1.0, 0.0).astype(bf16))

    def order(m):
        kind = m // 2
        old = 24 * (2 * (m // 36) + m % 2) + 8 * (kind % 3) + (kind // 3) % SEQ
        tap = 96 + 8 * (2 * ((m - 72) // 8) + m % 2) + (kind - 36) % CONV
        return jnp.where(m < 72, old, jnp.where(m < 88, tap, -1))

    rows = mm(one_hot(128, 128, order), spread.astype(bf16)).astype(bf16)
    for layer in range(LAYERS):
        for rw in range(2):
            lanes = slice(128 * rw, 128 * rw + 128)
            for k in range(CONV - 1):
                at = 24 * (2 * layer + rw) + 8 * k
                vhist_ref[layer, k, :, lanes] = rows[at : at + 8]
            at = 96 + 8 * (2 * layer + rw)
            vtaps_ref[layer, :, lanes] = rows[at : at + 8]


def middle(
    part_ref,
    misc_ref,
    vhist_ref,
    vtaps_ref,
    state_ref,
    msg_ref,
    keep_ref,
    write_ref,
    decay_ref,
    fresh_ref,
    *,
    layer,
):
    if layer == 0:
        total = sum(part_ref[d].astype(f32) for d in range(DN))
        place = one_hot(32, 24, place_first)
    else:
        rows = [sum(part_ref[y, d].astype(f32) for d in range(DN)) for y in range(YN)]
        total = jnp.concatenate(rows, axis=0)
        place = one_hot(32, 32, place_second)
    tail = total[:, 512:640]
    _, lane = row_col(tail.shape)
    squares = jnp.sum(jnp.where(lane == square_lane(), tail, 0.0), axis=1, keepdims=True)
    scaled = (total * lax.rsqrt(squares / D + norm_floor)).astype(bf16)
    rows = mm(place, scaled)
    fresh_ref[...] = rows[:, 128:512].astype(bf16)
    gate = rows[:, 0:128]

    head = 8 * lax.axis_index("z") + 2 * lax.axis_index("y")
    tail = rows[:, 512:640]
    _, lane = row_col(tail.shape)
    first = jnp.sum(jnp.where(lane == head, tail, 0.0), axis=1, keepdims=True)
    second = jnp.sum(jnp.where(lane == head + 1, tail, 0.0), axis=1, keepdims=True)
    left = lane < HEAD_DIM
    at = 72 + 2 * layer
    raw = jnp.where(left, first, second) + misc_ref[at : at + 1]
    rate = misc_ref[at + 1 : at + 2]
    soft = jnp.maximum(raw, 0.0) + jnp.log1p(jnp.exp(-jnp.abs(raw)))
    lens = misc_ref[64:72, 0:1]
    live = [jnp.where(lens > t, 1.0, 0.0) for t in range(NEW)]
    step = [soft[8 * t : 8 * t + 8] * live[t] for t in range(NEW)]
    cumulative = []
    for t in range(NEW):
        grown = step[t] * rate
        cumulative.append(grown if t == 0 else cumulative[-1] + grown)

    at = 32 * layer + 24
    taps = [misc_ref[at + k : at + k + 1] for k in range(CONV)]
    values = conv(old_values(misc_ref, layer), taps, rows[:, 128:256])
    taps = [vtaps_ref[layer, k : k + 1].astype(f32) for k in range(CONV)]
    vectors = conv(old_vectors(vhist_ref, layer), taps, rows[:, 256:512])
    write = [v[:, 0:128] for v in vectors]
    read = [v[:, 128:256] for v in vectors]
    stepped = [values[t] * step[t] for t in range(NEW)]

    reads = jnp.concatenate(read, axis=0).astype(bf16)
    row, _ = row_col((32, 128))
    carried = jnp.zeros((32, 128), f32)
    for s in range(SEQ):
        carried = jnp.where(row % 8 == s, mm_t(reads, state_ref[0, s].astype(bf16)), carried)

    mixed = []
    for t in range(NEW):
        y = jnp.exp(-cumulative[t]) * carried[8 * t : 8 * t + 8]
        for u in range(t + 1):
            score = jnp.sum(read[t] * write[u], axis=1, keepdims=True)
            y = y + score * jnp.exp(cumulative[u] - cumulative[t]) * stepped[u]
        mixed.append(y * silu(gate[8 * t : 8 * t + 8]) * live[t])
    mixed = jnp.concatenate(mixed, axis=0).astype(bf16)
    row, col = row_col((32, 32))
    i = row % 4
    n = 12 * ((row // 4) % 2) + 3 * (row // 8) + i
    pick = (col == 8 * (n % NEW) + n // NEW) & (i < 3)
    ordered = mm(jnp.where(pick, 1.0, 0.0).astype(bf16), mixed).astype(bf16)
    for y in range(YN):
        for d in range(DN):
            msg_ref[y * DN + d] = ordered[8 * y : 8 * y + 8]

    last = cumulative[-1]
    for t in range(NEW):
        keep_ref[8 * t : 8 * t + 8] = jnp.exp(cumulative[t] - last) * stepped[t]
        write_ref[8 * t : 8 * t + 8] = write[t]
    decay_ref[...] = jnp.exp(-last)


def finish(
    misc_ref,
    keep_ref,
    write_ref,
    decay_ref,
    fresh_ref,
    vhist_ref,
    state_ref,
    *rest,
    layer,
):
    next_ref, value_ref, vector_ref = rest[-3:]
    kept = jnp.transpose(keep_ref[...])
    _, col = row_col(kept.shape)
    write = write_ref[...].astype(bf16)
    for s in range(SEQ):
        fresh = mm(jnp.where(col % 8 == s, kept, 0.0).astype(bf16), write)
        for h in range(2):
            at = slice(HEAD_DIM * h, HEAD_DIM * h + HEAD_DIM)
            decay = decay_ref[s : s + 1, HEAD_DIM * h : HEAD_DIM * h + 1]
            next_ref[0, s, at] = state_ref[0, s, at] * decay + fresh[at]
    lens = misc_ref[64:72, 0:1]
    for out_ref, old, lo, hi in (
        (value_ref, old_values(misc_ref, layer), 0, 128),
        (vector_ref, old_vectors(vhist_ref, layer), 128, 384),
    ):
        rows = old + [fresh_ref[8 * t : 8 * t + 8, lo:hi].astype(f32) for t in range(NEW)]
        for k in range(CONV - 1):
            chosen = rows[k + 1]
            for r in range(k + 2, k + NEW + 1):
                chosen = jnp.where(lens + k == r, rows[r], chosen)
            out_ref[k] = chosen.astype(bf16)


def call(kernel, shapes, *args):
    vmem = pl.BlockSpec(memory_space=pltpu.VMEM)
    outs = [jax.ShapeDtypeStruct(shape, dtype) for shape, dtype in shapes]
    results = pl.pallas_call(
        kernel,
        out_shape=outs,
        in_specs=[vmem] * len(args),
        out_specs=[vmem] * len(outs),
        compiler_params=pltpu.CompilerParams(vmem_limit_bytes=12 << 20),
    )(*args)
    return results[0] if len(outs) == 1 else results


def ending(update_ref, token_ref, out_ref, vector_ref):
    total = sum(update_ref[z].astype(f32) for z in range(ZN))
    out_ref[...] = (total[0:3] + token_ref[...].astype(f32)).astype(bf16)
    rows = [update_ref[z, 3:4, 0:256].astype(f32) for z in range(ZN)]
    rows = jnp.concatenate(rows, axis=0)
    both = jnp.concatenate(
        [jnp.transpose(rows[:, 0:128]), jnp.transpose(rows[:, 128:256])], axis=1
    )
    for layer in range(LAYERS):
        for k in range(CONV - 1):
            for s in range(SEQ):
                at = 24 * layer + 8 * k + s
                pair = jnp.concatenate([both[at : at + 1], both[48 + at : 49 + at]], axis=0)
                vector_ref[layer, s, k] = pair.astype(bf16)


def close(layer, *args):
    vmem = pl.BlockSpec(memory_space=pltpu.VMEM)
    block = pl.BlockSpec((1, SEQ, 128, 128), lambda i: (layer, 0, 0, 0))
    space = [vmem] * 7 + [pl.BlockSpec(memory_space=pl.ANY)] * (len(args) - 7)
    return pl.pallas_call(
        functools.partial(finish, layer=layer),
        grid=(1,),
        out_shape=[
            jax.ShapeDtypeStruct((LAYERS, SEQ, 128, 128), f32),
            jax.ShapeDtypeStruct((3, 8, 128), bf16),
            jax.ShapeDtypeStruct((3, 8, 256), bf16),
        ],
        in_specs=space,
        out_specs=[block, vmem, vmem],
        input_output_aliases={7: 0} if layer else {},
        compiler_params=pltpu.CompilerParams(vmem_limit_bytes=12 << 20),
    )(*args)


def from_y(value, k):
    return lax.ppermute(value, "y", [(i, (i + k) % YN) for i in range(YN)])


def body(
    tokens,
    lengths,
    norm_gain,
    gate_weight,
    value_weight,
    vector_weight,
    step_weight,
    step_bias,
    decay_rate,
    value_taps,
    vector_taps,
    out_weight,
    recurrent_state,
    value_history,
    vector_history,
):
    first = pl.pallas_call(
        prepare,
        out_shape=jax.ShapeDtypeStruct((ZN, 3, 4, 512), bf16),
        in_specs=[pl.BlockSpec(memory_space=pltpu.MemorySpace.HBM)] * 4,
        out_specs=pl.BlockSpec(memory_space=pltpu.VMEM),
        scratch_shapes=[
            pltpu.VMEM((3, 512), bf16),
            pltpu.VMEM((2, 2, 32, 512), bf16),
            pltpu.VMEM((2, SEQ, 3, 2, 32), bf16),
            pltpu.VMEM((2, CONV, 2, 32), bf16),
            pltpu.VMEM((128, 32), f32),
            pltpu.SemaphoreType.DMA((4,)),
        ],
    )(tokens, vector_weight.transpose(0, 2, 3, 1), vector_history, vector_taps)
    first, outs, lens = lax.optimization_barrier(
        (first, out_weight.reshape(256, 512), lengths)
    )
    first = exchange(first, "z")
    early = jnp.concatenate([gate_weight[0], value_weight[0], step_weight[0]], axis=1)
    out_2 = from_y(outs, 2)
    out_3 = from_y(outs, 3)
    misc, base = pl.pallas_call(
        setup,
        out_shape=[jax.ShapeDtypeStruct((88, 128), f32), jax.ShapeDtypeStruct((1280, 128), bf16)],
        in_specs=[pl.BlockSpec(memory_space=pltpu.SMEM)]
        + [pl.BlockSpec(memory_space=pltpu.MemorySpace.HBM)] * 7,
        out_specs=[pl.BlockSpec(memory_space=pltpu.VMEM)] * 2,
        scratch_shapes=[
            pltpu.VMEM((2, 512), f32),
            pltpu.VMEM((2, 2), f32),
            pltpu.VMEM((2, 2), f32),
            pltpu.VMEM((2, CONV, 128), bf16),
            pltpu.VMEM((SEQ, 3, 2, 128), bf16),
            pltpu.SemaphoreType.DMA((7,)),
        ],
    )(
        lens,
        norm_gain,
        step_bias,
        decay_rate,
        value_taps,
        value_history.transpose(1, 2, 0, 3),
        gate_weight,
        value_weight,
    )
    plane = exchange(copies(first[:, :2], YN), "y").reshape(128, 4, 512)
    out_1 = from_y(outs, 1)
    outs = [outs, out_1, out_2, out_3]
    blocks = first[:, 2].reshape(64, 4, 128).transpose(1, 0, 2).reshape(256, 128)
    later = lax.dynamic_update_slice(base, blocks, (1024, 0))
    vhist, vtaps = call(unpack, [((2, 3, 8, 256), bf16), ((2, 8, 256), bf16)], plane)

    def mid(part, layer, old, *done):
        msg, keep, write, decay, fresh = call(
            functools.partial(middle, layer=layer),
            [
                ((YN * DN, 8, 128), bf16),
                ((32, 128), f32),
                ((32, 128), f32),
                ((8, 128), f32),
                ((32, 384), bf16),
            ],
                        part,
            misc,
            vhist,
            vtaps,
            old,
        )
        after = close(layer, misc, keep, write, decay, fresh, vhist, old, *done)
        msg = exchange(msg, ("y", "dp"))
        return msg.reshape(YN, DN * 8, 128), after

    part = call(
        first_projection,
        [((DN, 24, COLS), bf16)],
                plane,
        misc,
        early,
    )
    old = recurrent_state[:1]
    part = exchange(part, "dp")
    later_2 = from_y(later, 2)
    mixed, (state, value0, vector0) = mid(part, 0, old.reshape(1, SEQ, 128, 128))
    later_3 = from_y(later, 3)
    update = call(
        functools.partial(out_projection, first_row=0),
        [((ZN, 4, 512), bf16)],
                mixed,
        *outs,
    )
    update = exchange(update, "z")
    later_1 = from_y(later, 1)
    update = jnp.sum(update.astype(f32), axis=0)[:3]
    token_rows = (tokens.astype(f32) + update).astype(bf16)
    quarter = copies(jnp.pad(token_rows, ((0, 1), (0, 0))), ZN)
    quarter, old = lax.optimization_barrier((quarter, recurrent_state))
    quarter = exchange(quarter, "z").reshape(64, 512)
    old = old[1:].reshape(1, SEQ, 128, 128)
    later = [later, later_1, later_2, later_3]
    part = call(
        second_projection,
        [((YN, 64, COLS), bf16)],
                quarter,
        misc,
        step_weight[1:],
        *later,
    )
    part = exchange(part.reshape(YN * DN, 8, COLS), ("y", "dp")).reshape(YN, DN, 8, COLS)
    mixed, (state, value1, vector1) = mid(part, 1, old, state)
    update = call(
        functools.partial(out_projection, first_row=128),
        [((ZN, 4, 512), bf16)],
                mixed,
        *outs,
        jnp.concatenate([vector0, vector1], axis=0).reshape(48, 256),
    )
    update = exchange(update, "z")
    token_rows, next_vector = call(
        ending,
        [((3, 512), bf16), ((LAYERS, SEQ, CONV - 1, 2, 32), bf16)],
        update,
        token_rows,
    )
    return (
        token_rows,
        state.reshape(recurrent_state.shape),
        jnp.stack([value0, value1])[:, :, :SEQ].transpose(0, 2, 1, 3),
        next_vector,
    )


def solution(mesh):
    grid = Mesh(mesh.devices.reshape(ZN, YN, DN), ("z", "y", "dp"))
    tp = ("z", "y")

    return jax.shard_map(
        body,
        mesh=grid,
        in_specs=(
            P(tp, "dp"),
            P("dp"),
            P(None, "dp"),
            P(None, "dp", tp),
            P(None, "dp", tp),
            P(None, "dp", None, tp),
            P(None, "dp", None),
            P(None, tp),
            P(None, tp),
            P(None, None, tp),
            P(None, None, None, tp),
            P(None, tp, "dp"),
            P(None, "dp", tp, None, None),
            P(None, "dp", None, tp),
            P(None, "dp", None, None, tp),
        ),
        out_specs=(
            P(tp, "dp"),
            P(None, "dp", tp, None, None),
            P(None, "dp", None, tp),
            P(None, "dp", None, None, tp),
        ),
        check_vma=False,
    )
```

```python
import functools

import jax
import jax.numpy as jnp
from jax import lax
from jax.experimental import pallas as pl
from jax.experimental.pallas import tpu as pltpu
from jax.sharding import Mesh, PartitionSpec as P

D = 4096
HEADS = 128
HEAD_DIM = 64
GROUPS = 16
CONV = 4
NEW = 4
LAYERS = 2
norm_floor = 0.1

ZN, YN, DN = 16, 4, 8
SEQ = 6
bf16 = jnp.bfloat16
f32 = jnp.float32
COLS = 640


def exchange(pieces, axis):
    return lax.all_to_all(pieces, axis, 0, 0, tiled=True)


def copies(value, peers):
    return jnp.broadcast_to(value[None], (peers, *value.shape))


def one_hot(rows, cols, target):
    row = lax.broadcasted_iota(jnp.int32, (rows, cols), 0)
    col = lax.broadcasted_iota(jnp.int32, (rows, cols), 1)
    return jnp.where(row == target(col), 1.0, 0.0).astype(bf16)


def mm(a, b):
    return lax.dot_general(a, b, (((1,), (0,)), ((), ())), preferred_element_type=f32)


def mm_t(a, b):
    return lax.dot_general(a, b, (((1,), (1,)), ((), ())), preferred_element_type=f32)


def normed_rows(rows, gain):
    widened = rows.astype(f32)
    squares = jnp.sum(widened * widened, axis=1, keepdims=True)
    return (widened * gain).astype(bf16), squares


def square_lane():
    return (8 * lax.axis_index("z") + 64) % HEADS


def step_lanes(normed, squares, step_w):
    step = mm(normed, step_w)
    lane = lax.broadcasted_iota(jnp.int32, step.shape, 1)
    return jnp.where(lane == square_lane(), squares, step)


def first_projection(plane_ref, misc_ref, weight_ref, out_ref):
    plane = plane_ref[...].reshape(512, 512)

    def token_source(col):
        i = col % 8
        return jnp.where(i < 3, 12 * ((col // 8) % ZN) + 3 * (col // 128) + i, -1)

    def vector_source(col):
        j = col % 8 - 4
        n = 8 * ((col // 8) % ZN) + 2 * (col // 128) + j % 2
        return jnp.where((j >= 0) & (j < 4), 128 * (j // 2) + n, -1)

    rows = mm(one_hot(192, 512, token_source), plane).astype(bf16)
    vector_w = mm(one_hot(256, 512, vector_source), plane).astype(bf16)
    normed, squares = normed_rows(rows, gain_row(misc_ref, 0))
    parts = [
        mm(normed, weight_ref[:, 0:128]),
        mm(normed, weight_ref[:, 128:256]),
        mm_t(normed, vector_w),
        step_lanes(normed, squares, weight_ref[:, 256:384]),
    ]
    at = 0
    for part in parts:
        width = part.shape[1]
        out_ref[:, :, at : at + width] = part.astype(bf16).reshape(DN, 24, width)
        at += width


def second_projection(rows_ref, misc_ref, step_ref, w0, w1, w2, w3, out_ref):
    y = lax.axis_index("y")
    normed, squares = normed_rows(rows_ref[...], gain_row(misc_ref, 1))
    pieces = [w0, w1, w2, w3]

    def source(col):
        j = col % 4
        n = 8 * ((col // 4) % ZN) + 2 * ((y - col // 64) % YN) + j % 2
        return 128 * (j // 2) + n

    stacked = jnp.concatenate(
        [
            jnp.concatenate([w[1024 + 64 * b : 1088 + 64 * b] for b in range(4)], axis=1)
            for w in pieces
        ],
        axis=0,
    )
    vector_w = mm(one_hot(256, 256, source), stacked).astype(bf16)
    vector = mm_t(normed, vector_w).astype(bf16)
    extra = step_lanes(normed, squares, step_ref[0]).astype(bf16)
    for k, w in enumerate(pieces):
        to = (y - k) % YN
        for n in range(2):
            total = mm(normed, w[512 * n : 512 * n + 512])
            out_ref[to, :, 128 * n : 128 * n + 128] = total.astype(bf16)
        out_ref[to, :, 256:512] = vector
        out_ref[to, :, 512:640] = extra


def out_projection(mixed_ref, w0, w1, w2, w3, *rest, first_row):
    y = lax.axis_index("y")
    total = jnp.zeros((64, 512), f32)
    for k, w in enumerate([w0, w1, w2, w3]):
        total += mm(mixed_ref[(y - k) % YN], w[first_row : first_row + 128])
    if len(rest) == 1:
        rest[0][...] = total.astype(bf16).reshape(ZN, 4, 512)
        return
    returned_ref, out_ref = rest
    returned = jnp.concatenate(
        [returned_ref[:, 0:128], returned_ref[:, 128:256], jnp.zeros((32, 128), bf16)], axis=0
    )
    slot = one_hot(64, ZN, lambda col: 4 * col + 3)
    halves = []
    for nl in range(2):
        row = lax.broadcasted_iota(jnp.int32, (ZN, 128), 0)
        col = lax.broadcasted_iota(jnp.int32, (ZN, 128), 1)
        chosen = jnp.where(col == 8 * row + 2 * y + nl, 1.0, 0.0).astype(bf16)
        halves.append(mm_t(chosen, returned).astype(bf16))
    tail = jnp.concatenate(halves, axis=1)
    left = (total[:, 0:256] + mm(slot, tail)).astype(bf16)
    whole = jnp.concatenate([left, total[:, 256:512].astype(bf16)], axis=1)
    out_ref[...] = whole.reshape(ZN, 4, 512)


def row_col(shape):
    return (
        lax.broadcasted_iota(jnp.int32, shape, 0),
        lax.broadcasted_iota(jnp.int32, shape, 1),
    )


def silu(x):
    return x * jax.nn.sigmoid(x)


def place_first(col):
    return 8 * (col % NEW) + col // NEW


def place_second(col):
    i = col % 4
    n = 12 * ((col // 4) % 2) + 3 * (col // 8) + i
    return jnp.where(i < 3, 8 * (n % NEW) + n // NEW, -1)


def conv(old, taps, fresh):
    rows = old + [fresh[8 * t : 8 * t + 8] for t in range(NEW)]
    return [silu(sum(rows[t + k] * taps[k] for k in range(CONV))) for t in range(NEW)]


def old_values(misc_ref, layer):
    return [misc_ref[32 * layer + 8 * k : 32 * layer + 8 * k + 8] for k in range(CONV - 1)]


def old_vectors(vhist_ref, layer):
    return [vhist_ref[layer, k].astype(f32) for k in range(CONV - 1)]


def setup(
    len_ref,
    gain_hbm,
    bias_hbm,
    rate_hbm,
    taps_hbm,
    history_hbm,
    gate_hbm,
    value_hbm,
    misc_ref,
    base_ref,
    gain_ref,
    bias_ref,
    rate_ref,
    taps_ref,
    history_ref,
    sems,
):
    pairs = (
        (gain_hbm, gain_ref),
        (bias_hbm, bias_ref),
        (rate_hbm, rate_ref),
        (taps_hbm, taps_ref),
        (history_hbm, history_ref),
        (gate_hbm.at[1], base_ref.at[0:512]),
        (value_hbm.at[1], base_ref.at[512:1024]),
    )
    moves = [pltpu.make_async_copy(a, b, sems.at[n]) for n, (a, b) in enumerate(pairs)]
    for move in moves:
        move.start()
    row, lane = row_col((8, 128))
    lens = jnp.zeros((8, 128), f32)
    for s in range(SEQ):
        lens = jnp.where(row == s, len_ref[s].astype(f32), lens)
    misc_ref[0:64] = jnp.zeros((64, 128), f32)
    misc_ref[64:72] = lens
    misc_ref[72:80] = jnp.zeros((8, 128), f32)
    for move in moves:
        move.wait()
    left = lane[0:1] < HEAD_DIM
    for layer in range(LAYERS):
        for n, ref in enumerate((bias_ref, rate_ref)):
            both = jnp.where(left, ref[layer : layer + 1, 0:1], ref[layer : layer + 1, 1:2])
            misc_ref[72 + 2 * layer + n : 73 + 2 * layer + n] = both
        for b in range(4):
            part = gain_ref[layer : layer + 1, 128 * b : 128 * b + 128]
            misc_ref[80 + 4 * layer + b : 81 + 4 * layer + b] = part
        for k in range(CONV - 1):
            at = 32 * layer + 8 * k
            for s in range(SEQ):
                misc_ref[at + s : at + s + 1] = history_ref[s, k, layer : layer + 1].astype(f32)
        at = 32 * layer + 24
        misc_ref[at : at + CONV] = taps_ref[layer].astype(f32)


def gain_row(misc_ref, layer):
    parts = [misc_ref[80 + 4 * layer + b : 81 + 4 * layer + b] for b in range(4)]
    return jnp.concatenate(parts, axis=1)


def prepare(
    token_hbm,
    weight_hbm,
    history_hbm,
    taps_hbm,
    out_ref,
    token_ref,
    weight_ref,
    history_ref,
    taps_ref,
    stack_ref,
    sems,
):
    moves = [
        pltpu.make_async_copy(source, target, sems.at[n])
        for n, (source, target) in enumerate(
            (
                (history_hbm, history_ref),
                (taps_hbm, taps_ref),
                (token_hbm, token_ref),
                (weight_hbm, weight_ref),
            )
        )
    ]
    for move in moves:
        move.start()
    for move in moves[:3]:
        move.wait()
    stack_ref[...] = jnp.zeros((128, 32), f32)
    at = 0
    for layer in range(LAYERS):
        for s in range(SEQ):
            for k in range(CONV - 1):
                stack_ref[at : at + 2] = history_ref[layer, s, k].astype(f32)
                at += 2
    for layer in range(LAYERS):
        for k in range(CONV):
            stack_ref[at : at + 2] = taps_ref[layer, k].astype(f32)
            at += 2
    turned = jnp.transpose(stack_ref[...])
    tokens = jnp.concatenate([token_ref[...].astype(f32), jnp.zeros((1, 512), f32)], axis=0)
    row, _ = row_col((4, 512))
    for g in range(GROUPS):
        both = [turned[g : g + 1], turned[GROUPS + g : GROUPS + g + 1], jnp.zeros((1, 256), f32)]
        tail = jnp.broadcast_to(jnp.concatenate(both, axis=1), (4, 512))
        out_ref[g, 0] = jnp.where(row == 3, tail, tokens).astype(bf16)

    def source(col):
        c = col % 32
        return 4 * (c % GROUPS) + 2 * (col // 32) + c // GROUPS

    order = one_hot(64, 64, source)
    moves[3].wait()
    for layer in range(LAYERS):
        cols = weight_ref[layer].reshape(64, 512)
        out_ref[:, 1 + layer] = mm(order, cols).astype(bf16).reshape(GROUPS, 4, 512)


def unpack(plane_ref, vhist_ref, vtaps_ref):
    def source(col):
        return jnp.where(col % 8 == 3, 4 * ((col // 8) % ZN) + col // 128, -1)

    small = mm(one_hot(64, 512, source), plane_ref[:, :, 0:256].reshape(512, 256))
    spread = jnp.zeros((128, 128), f32)
    row, col = row_col((64, 128))
    for nl in range(2):
        turned = jnp.transpose(small[:, 128 * nl : 128 * nl + 128]).astype(bf16)
        spread += mm(turned, jnp.where(col == 2 * row + nl, 1.0, 0.0).astype(bf16))

    def order(m):
        kind = m // 2
        old = 24 * (2 * (m // 36) + m % 2) + 8 * (kind % 3) + (kind // 3) % SEQ
        tap = 96 + 8 * (2 * ((m - 72) // 8) + m % 2) + (kind - 36) % CONV
        return jnp.where(m < 72, old, jnp.where(m < 88, tap, -1))

    rows = mm(one_hot(128, 128, order), spread.astype(bf16)).astype(bf16)
    for layer in range(LAYERS):
        for rw in range(2):
            lanes = slice(128 * rw, 128 * rw + 128)
            for k in range(CONV - 1):
                at = 24 * (2 * layer + rw) + 8 * k
                vhist_ref[layer, k, :, lanes] = rows[at : at + 8]
            at = 96 + 8 * (2 * layer + rw)
            vtaps_ref[layer, :, lanes] = rows[at : at + 8]


def middle(
    part_ref,
    misc_ref,
    vhist_ref,
    vtaps_ref,
    state_ref,
    msg_ref,
    keep_ref,
    write_ref,
    decay_ref,
    fresh_ref,
    *,
    layer,
):
    if layer == 0:
        total = sum(part_ref[d].astype(f32) for d in range(DN))
        place = one_hot(32, 24, place_first)
    else:
        rows = [sum(part_ref[y, d].astype(f32) for d in range(DN)) for y in range(YN)]
        total = jnp.concatenate(rows, axis=0)
        place = one_hot(32, 32, place_second)
    tail = total[:, 512:640]
    _, lane = row_col(tail.shape)
    squares = jnp.sum(jnp.where(lane == square_lane(), tail, 0.0), axis=1, keepdims=True)
    scaled = (total * lax.rsqrt(squares / D + norm_floor)).astype(bf16)
    rows = mm(place, scaled)
    fresh_ref[...] = rows[:, 128:512].astype(bf16)
    gate = rows[:, 0:128]

    head = 8 * lax.axis_index("z") + 2 * lax.axis_index("y")
    tail = rows[:, 512:640]
    _, lane = row_col(tail.shape)
    first = jnp.sum(jnp.where(lane == head, tail, 0.0), axis=1, keepdims=True)
    second = jnp.sum(jnp.where(lane == head + 1, tail, 0.0), axis=1, keepdims=True)
    left = lane < HEAD_DIM
    at = 72 + 2 * layer
    raw = jnp.where(left, first, second) + misc_ref[at : at + 1]
    rate = misc_ref[at + 1 : at + 2]
    soft = jnp.maximum(raw, 0.0) + jnp.log1p(jnp.exp(-jnp.abs(raw)))
    lens = misc_ref[64:72, 0:1]
    live = [jnp.where(lens > t, 1.0, 0.0) for t in range(NEW)]
    step = [soft[8 * t : 8 * t + 8] * live[t] for t in range(NEW)]
    cumulative = []
    for t in range(NEW):
        grown = step[t] * rate
        cumulative.append(grown if t == 0 else cumulative[-1] + grown)

    at = 32 * layer + 24
    taps = [misc_ref[at + k : at + k + 1] for k in range(CONV)]
    values = conv(old_values(misc_ref, layer), taps, rows[:, 128:256])
    taps = [vtaps_ref[layer, k : k + 1].astype(f32) for k in range(CONV)]
    vectors = conv(old_vectors(vhist_ref, layer), taps, rows[:, 256:512])
    write = [v[:, 0:128] for v in vectors]
    read = [v[:, 128:256] for v in vectors]
    stepped = [values[t] * step[t] for t in range(NEW)]

    reads = jnp.concatenate(read, axis=0).astype(bf16)
    row, _ = row_col((32, 128))
    carried = jnp.zeros((32, 128), f32)
    for s in range(SEQ):
        carried = jnp.where(row % 8 == s, mm_t(reads, state_ref[0, s].astype(bf16)), carried)

    mixed = []
    for t in range(NEW):
        y = jnp.exp(-cumulative[t]) * carried[8 * t : 8 * t + 8]
        for u in range(t + 1):
            score = jnp.sum(read[t] * write[u], axis=1, keepdims=True)
            y = y + score * jnp.exp(cumulative[u] - cumulative[t]) * stepped[u]
        mixed.append(y * silu(gate[8 * t : 8 * t + 8]) * live[t])
    mixed = jnp.concatenate(mixed, axis=0).astype(bf16)
    row, col = row_col((32, 32))
    i = row % 4
    n = 12 * ((row // 4) % 2) + 3 * (row // 8) + i
    pick = (col == 8 * (n % NEW) + n // NEW) & (i < 3)
    ordered = mm(jnp.where(pick, 1.0, 0.0).astype(bf16), mixed).astype(bf16)
    for y in range(YN):
        for d in range(DN):
            msg_ref[y * DN + d] = ordered[8 * y : 8 * y + 8]

    last = cumulative[-1]
    for t in range(NEW):
        keep_ref[8 * t : 8 * t + 8] = jnp.exp(cumulative[t] - last) * stepped[t]
        write_ref[8 * t : 8 * t + 8] = write[t]
    decay_ref[...] = jnp.exp(-last)


def finish(
    misc_ref,
    keep_ref,
    write_ref,
    decay_ref,
    fresh_ref,
    vhist_ref,
    state_ref,
    *rest,
    layer,
):
    next_ref, value_ref, vector_ref = rest[-3:]
    kept = jnp.transpose(keep_ref[...])
    _, col = row_col(kept.shape)
    write = write_ref[...].astype(bf16)
    for s in range(SEQ):
        fresh = mm(jnp.where(col % 8 == s, kept, 0.0).astype(bf16), write)
        for h in range(2):
            at = slice(HEAD_DIM * h, HEAD_DIM * h + HEAD_DIM)
            decay = decay_ref[s : s + 1, HEAD_DIM * h : HEAD_DIM * h + 1]
            next_ref[0, s, at] = state_ref[0, s, at] * decay + fresh[at]
    lens = misc_ref[64:72, 0:1]
    for out_ref, old, lo, hi in (
        (value_ref, old_values(misc_ref, layer), 0, 128),
        (vector_ref, old_vectors(vhist_ref, layer), 128, 384),
    ):
        rows = old + [fresh_ref[8 * t : 8 * t + 8, lo:hi].astype(f32) for t in range(NEW)]
        for k in range(CONV - 1):
            chosen = rows[k + 1]
            for r in range(k + 2, k + NEW + 1):
                chosen = jnp.where(lens + k == r, rows[r], chosen)
            out_ref[k] = chosen.astype(bf16)


def call(kernel, shapes, *args):
    vmem = pl.BlockSpec(memory_space=pltpu.VMEM)
    outs = [jax.ShapeDtypeStruct(shape, dtype) for shape, dtype in shapes]
    results = pl.pallas_call(
        kernel,
        out_shape=outs,
        in_specs=[vmem] * len(args),
        out_specs=[vmem] * len(outs),
        compiler_params=pltpu.CompilerParams(vmem_limit_bytes=12 << 20),
    )(*args)
    return results[0] if len(outs) == 1 else results


def ending(update_ref, token_ref, out_ref, vector_ref):
    total = sum(update_ref[z].astype(f32) for z in range(ZN))
    out_ref[...] = (total[0:3] + token_ref[...].astype(f32)).astype(bf16)
    rows = [update_ref[z, 3:4, 0:256].astype(f32) for z in range(ZN)]
    rows = jnp.concatenate(rows, axis=0)
    both = jnp.concatenate(
        [jnp.transpose(rows[:, 0:128]), jnp.transpose(rows[:, 128:256])], axis=1
    )
    for layer in range(LAYERS):
        for k in range(CONV - 1):
            for s in range(SEQ):
                at = 24 * layer + 8 * k + s
                pair = jnp.concatenate([both[at : at + 1], both[48 + at : 49 + at]], axis=0)
                vector_ref[layer, s, k] = pair.astype(bf16)


def close(layer, *args):
    vmem = pl.BlockSpec(memory_space=pltpu.VMEM)
    block = pl.BlockSpec((1, SEQ, 128, 128), lambda i: (layer, 0, 0, 0))
    space = [vmem] * 7 + [pl.BlockSpec(memory_space=pl.ANY)] * (len(args) - 7)
    return pl.pallas_call(
        functools.partial(finish, layer=layer),
        grid=(1,),
        out_shape=[
            jax.ShapeDtypeStruct((LAYERS, SEQ, 128, 128), f32),
            jax.ShapeDtypeStruct((3, 8, 128), bf16),
            jax.ShapeDtypeStruct((3, 8, 256), bf16),
        ],
        in_specs=space,
        out_specs=[block, vmem, vmem],
        input_output_aliases={7: 0} if layer else {},
        compiler_params=pltpu.CompilerParams(vmem_limit_bytes=12 << 20),
    )(*args)


def from_y(value, k):
    return lax.ppermute(value, "y", [(i, (i + k) % YN) for i in range(YN)])


def body(
    tokens,
    lengths,
    norm_gain,
    gate_weight,
    value_weight,
    vector_weight,
    step_weight,
    step_bias,
    decay_rate,
    value_taps,
    vector_taps,
    out_weight,
    recurrent_state,
    value_history,
    vector_history,
):
    first = pl.pallas_call(
        prepare,
        out_shape=jax.ShapeDtypeStruct((ZN, 3, 4, 512), bf16),
        in_specs=[pl.BlockSpec(memory_space=pltpu.MemorySpace.HBM)] * 4,
        out_specs=pl.BlockSpec(memory_space=pltpu.VMEM),
        scratch_shapes=[
            pltpu.VMEM((3, 512), bf16),
            pltpu.VMEM((2, 2, 32, 512), bf16),
            pltpu.VMEM((2, SEQ, 3, 2, 32), bf16),
            pltpu.VMEM((2, CONV, 2, 32), bf16),
            pltpu.VMEM((128, 32), f32),
            pltpu.SemaphoreType.DMA((4,)),
        ],
    )(tokens, vector_weight.transpose(0, 2, 3, 1), vector_history, vector_taps)
    first, outs, lens = lax.optimization_barrier(
        (first, out_weight.reshape(256, 512), lengths)
    )
    first = exchange(first, "z")
    early = jnp.concatenate([gate_weight[0], value_weight[0], step_weight[0]], axis=1)
    out_2 = from_y(outs, 2)
    out_3 = from_y(outs, 3)
    misc, base = pl.pallas_call(
        setup,
        out_shape=[jax.ShapeDtypeStruct((88, 128), f32), jax.ShapeDtypeStruct((1280, 128), bf16)],
        in_specs=[pl.BlockSpec(memory_space=pltpu.SMEM)]
        + [pl.BlockSpec(memory_space=pltpu.MemorySpace.HBM)] * 7,
        out_specs=[pl.BlockSpec(memory_space=pltpu.VMEM)] * 2,
        scratch_shapes=[
            pltpu.VMEM((2, 512), f32),
            pltpu.VMEM((2, 2), f32),
            pltpu.VMEM((2, 2), f32),
            pltpu.VMEM((2, CONV, 128), bf16),
            pltpu.VMEM((SEQ, 3, 2, 128), bf16),
            pltpu.SemaphoreType.DMA((7,)),
        ],
    )(
        lens,
        norm_gain,
        step_bias,
        decay_rate,
        value_taps,
        value_history.transpose(1, 2, 0, 3),
        gate_weight,
        value_weight,
    )
    plane = exchange(copies(first[:, :2], YN), "y").reshape(128, 4, 512)
    out_1 = from_y(outs, 1)
    outs = [outs, out_1, out_2, out_3]
    blocks = first[:, 2].reshape(64, 4, 128).transpose(1, 0, 2).reshape(256, 128)
    later = lax.dynamic_update_slice(base, blocks, (1024, 0))
    vhist, vtaps = call(unpack, [((2, 3, 8, 256), bf16), ((2, 8, 256), bf16)], plane)

    def mid(part, layer, pieces, old, *done):
        msg, keep, write, decay, fresh = call(
            functools.partial(middle, layer=layer),
            [
                ((YN * DN, 8, 128), bf16),
                ((32, 128), f32),
                ((32, 128), f32),
                ((8, 128), f32),
                ((32, 384), bf16),
            ],
                        part,
            misc,
            vhist,
            vtaps,
            old,
        )
        after = close(layer, misc, keep, write, decay, fresh, vhist, old, *done)
        msg, pieces = lax.optimization_barrier((msg, pieces))
        msg = exchange(msg, ("y", "dp"))
        return msg.reshape(YN, DN * 8, 128), pieces, after

    part = call(
        first_projection,
        [((DN, 24, COLS), bf16)],
                plane,
        misc,
        early,
    )
    old = recurrent_state[:1]
    part = exchange(part, "dp")
    later_2 = from_y(later, 2)
    mixed, outs, (state, value0, vector0) = mid(part, 0, outs, old.reshape(1, SEQ, 128, 128))
    later_3 = from_y(later, 3)
    update = call(
        functools.partial(out_projection, first_row=0),
        [((ZN, 4, 512), bf16)],
                mixed,
        *outs,
    )
    update = exchange(update, "z")
    later_1 = from_y(later, 1)
    update = jnp.sum(update.astype(f32), axis=0)[:3]
    token_rows = (tokens.astype(f32) + update).astype(bf16)
    quarter = copies(jnp.pad(token_rows, ((0, 1), (0, 0))), ZN)
    quarter, old = lax.optimization_barrier((quarter, recurrent_state))
    quarter = exchange(quarter, "z").reshape(64, 512)
    old = old[1:].reshape(1, SEQ, 128, 128)
    later = [later, later_1, later_2, later_3]
    part = call(
        second_projection,
        [((YN, 64, COLS), bf16)],
                quarter,
        misc,
        step_weight[1:],
        *later,
    )
    part = exchange(part.reshape(YN * DN, 8, COLS), ("y", "dp"))
    part = part.reshape(YN, DN, 8, COLS)
    mixed, outs, (state, value1, vector1) = mid(part, 1, outs, old, state)
    update = call(
        functools.partial(out_projection, first_row=128),
        [((ZN, 4, 512), bf16)],
                mixed,
        *outs,
        jnp.concatenate([vector0, vector1], axis=0).reshape(48, 256),
    )
    update = exchange(update, "z")
    token_rows, next_vector = call(
        ending,
        [((3, 512), bf16), ((LAYERS, SEQ, CONV - 1, 2, 32), bf16)],
        update,
        token_rows,
    )
    return (
        token_rows,
        state.reshape(recurrent_state.shape),
        jnp.stack([value0, value1])[:, :, :SEQ].transpose(0, 2, 1, 3),
        next_vector,
    )


def solution(mesh):
    grid = Mesh(mesh.devices.reshape(ZN, YN, DN), ("z", "y", "dp"))
    tp = ("z", "y")

    return jax.shard_map(
        body,
        mesh=grid,
        in_specs=(
            P(tp, "dp"),
            P("dp"),
            P(None, "dp"),
            P(None, "dp", tp),
            P(None, "dp", tp),
            P(None, "dp", None, tp),
            P(None, "dp", None),
            P(None, tp),
            P(None, tp),
            P(None, None, tp),
            P(None, None, None, tp),
            P(None, tp, "dp"),
            P(None, "dp", tp, None, None),
            P(None, "dp", None, tp),
            P(None, "dp", None, None, tp),
        ),
        out_specs=(
            P(tp, "dp"),
            P(None, "dp", tp, None, None),
            P(None, "dp", None, tp),
            P(None, "dp", None, None, tp),
        ),
        check_vma=False,
    )
```

```python
import functools

import jax
import jax.numpy as jnp
from jax import lax
from jax.experimental import pallas as pl
from jax.experimental.pallas import tpu as pltpu
from jax.sharding import Mesh, PartitionSpec as P

D = 4096
HEADS = 128
HEAD_DIM = 64
GROUPS = 16
CONV = 4
NEW = 4
LAYERS = 2
norm_floor = 0.1

ZN, YN, DN = 16, 4, 8
SEQ = 6
bf16 = jnp.bfloat16
f32 = jnp.float32
COLS = 640


def exchange(pieces, axis):
    return lax.all_to_all(pieces, axis, 0, 0, tiled=True)


def copies(value, peers):
    return jnp.broadcast_to(value[None], (peers, *value.shape))


def one_hot(rows, cols, target):
    row = lax.broadcasted_iota(jnp.int32, (rows, cols), 0)
    col = lax.broadcasted_iota(jnp.int32, (rows, cols), 1)
    return jnp.where(row == target(col), 1.0, 0.0).astype(bf16)


def mm(a, b):
    return lax.dot_general(a, b, (((1,), (0,)), ((), ())), preferred_element_type=f32)


def mm_t(a, b):
    return lax.dot_general(a, b, (((1,), (1,)), ((), ())), preferred_element_type=f32)


def normed_rows(rows, gain):
    widened = rows.astype(f32)
    squares = jnp.sum(widened * widened, axis=1, keepdims=True)
    return (widened * gain).astype(bf16), squares


def square_lane():
    return (8 * lax.axis_index("z") + 64) % HEADS


def step_lanes(normed, squares, step_w):
    step = mm(normed, step_w)
    lane = lax.broadcasted_iota(jnp.int32, step.shape, 1)
    return jnp.where(lane == square_lane(), squares, step)


def first_projection(plane_ref, misc_ref, weight_ref, out_ref):
    plane = plane_ref[...].reshape(512, 512)

    def token_source(col):
        i = col % 8
        return jnp.where(i < 3, 12 * ((col // 8) % ZN) + 3 * (col // 128) + i, -1)

    def vector_source(col):
        j = col % 8 - 4
        n = 8 * ((col // 8) % ZN) + 2 * (col // 128) + j % 2
        return jnp.where((j >= 0) & (j < 4), 128 * (j // 2) + n, -1)

    rows = mm(one_hot(192, 512, token_source), plane).astype(bf16)
    vector_w = mm(one_hot(256, 512, vector_source), plane).astype(bf16)
    normed, squares = normed_rows(rows, gain_row(misc_ref, 0))
    parts = [
        mm(normed, weight_ref[:, 0:128]),
        mm(normed, weight_ref[:, 128:256]),
        mm_t(normed, vector_w),
        step_lanes(normed, squares, weight_ref[:, 256:384]),
    ]
    at = 0
    for part in parts:
        width = part.shape[1]
        out_ref[:, :, at : at + width] = part.astype(bf16).reshape(DN, 24, width)
        at += width


def second_projection(rows_ref, misc_ref, step_ref, w0, w1, w2, w3, out_ref):
    y = lax.axis_index("y")
    normed, squares = normed_rows(rows_ref[...], gain_row(misc_ref, 1))
    pieces = [w0, w1, w2, w3]

    def source(col):
        j = col % 4
        n = 8 * ((col // 4) % ZN) + 2 * ((y - col // 64) % YN) + j % 2
        return 128 * (j // 2) + n

    stacked = jnp.concatenate(
        [
            jnp.concatenate([w[1024 + 64 * b : 1088 + 64 * b] for b in range(4)], axis=1)
            for w in pieces
        ],
        axis=0,
    )
    vector_w = mm(one_hot(256, 256, source), stacked).astype(bf16)
    vector = mm_t(normed, vector_w).astype(bf16)
    extra = step_lanes(normed, squares, step_ref[0]).astype(bf16)
    for k, w in enumerate(pieces):
        to = (y - k) % YN
        for n in range(2):
            total = mm(normed, w[512 * n : 512 * n + 512])
            out_ref[to, :, 128 * n : 128 * n + 128] = total.astype(bf16)
        out_ref[to, :, 256:512] = vector
        out_ref[to, :, 512:640] = extra


def out_projection(mixed_ref, w0, w1, w2, w3, *rest, first_row):
    y = lax.axis_index("y")
    total = jnp.zeros((64, 512), f32)
    for k, w in enumerate([w0, w1, w2, w3]):
        total += mm(mixed_ref[(y - k) % YN], w[first_row : first_row + 128])
    if len(rest) == 1:
        rest[0][...] = total.astype(bf16).reshape(ZN, 4, 512)
        return
    *vector_refs, out_ref = rest
    old = [ref[k] for ref in vector_refs for k in range(CONV - 1)]
    returned = [v[:, 0:128].astype(f32) for v in old] + [v[:, 128:256].astype(f32) for v in old]
    returned = jnp.concatenate([*returned, jnp.zeros((32, 128), f32)], axis=0).astype(bf16)
    slot = one_hot(64, ZN, lambda col: 4 * col + 3)
    halves = []
    for nl in range(2):
        row = lax.broadcasted_iota(jnp.int32, (ZN, 128), 0)
        col = lax.broadcasted_iota(jnp.int32, (ZN, 128), 1)
        chosen = jnp.where(col == 8 * row + 2 * y + nl, 1.0, 0.0).astype(bf16)
        halves.append(mm_t(chosen, returned).astype(bf16))
    tail = jnp.concatenate(halves, axis=1)
    left = (total[:, 0:256] + mm(slot, tail)).astype(bf16)
    whole = jnp.concatenate([left, total[:, 256:512].astype(bf16)], axis=1)
    out_ref[...] = whole.reshape(ZN, 4, 512)


def row_col(shape):
    return (
        lax.broadcasted_iota(jnp.int32, shape, 0),
        lax.broadcasted_iota(jnp.int32, shape, 1),
    )


def silu(x):
    return x * jax.nn.sigmoid(x)


def place_first(col):
    return 8 * (col % NEW) + col // NEW


def place_second(col):
    i = col % 4
    n = 12 * ((col // 4) % 2) + 3 * (col // 8) + i
    return jnp.where(i < 3, 8 * (n % NEW) + n // NEW, -1)


def conv(old, taps, fresh):
    rows = old + [fresh[8 * t : 8 * t + 8] for t in range(NEW)]
    return [silu(sum(rows[t + k] * taps[k] for k in range(CONV))) for t in range(NEW)]


def old_values(misc_ref, layer):
    return [misc_ref[32 * layer + 8 * k : 32 * layer + 8 * k + 8] for k in range(CONV - 1)]


def old_vectors(vhist_ref, layer):
    return [vhist_ref[layer, k].astype(f32) for k in range(CONV - 1)]


def setup(
    len_ref,
    gain_hbm,
    bias_hbm,
    rate_hbm,
    taps_hbm,
    history_hbm,
    gate_hbm,
    value_hbm,
    misc_ref,
    base_ref,
    gain_ref,
    bias_ref,
    rate_ref,
    taps_ref,
    history_ref,
    sems,
):
    pairs = (
        (gain_hbm, gain_ref),
        (bias_hbm, bias_ref),
        (rate_hbm, rate_ref),
        (taps_hbm, taps_ref),
        (history_hbm, history_ref),
        (gate_hbm.at[1], base_ref.at[0:512]),
        (value_hbm.at[1], base_ref.at[512:1024]),
    )
    moves = [pltpu.make_async_copy(a, b, sems.at[n]) for n, (a, b) in enumerate(pairs)]
    for move in moves:
        move.start()
    row, lane = row_col((8, 128))
    lens = jnp.zeros((8, 128), f32)
    for s in range(SEQ):
        lens = jnp.where(row == s, len_ref[s].astype(f32), lens)
    misc_ref[0:64] = jnp.zeros((64, 128), f32)
    misc_ref[64:72] = lens
    misc_ref[72:80] = jnp.zeros((8, 128), f32)
    for move in moves:
        move.wait()
    left = lane[0:1] < HEAD_DIM
    for layer in range(LAYERS):
        for n, ref in enumerate((bias_ref, rate_ref)):
            both = jnp.where(left, ref[layer : layer + 1, 0:1], ref[layer : layer + 1, 1:2])
            misc_ref[72 + 2 * layer + n : 73 + 2 * layer + n] = both
        for b in range(4):
            part = gain_ref[layer : layer + 1, 128 * b : 128 * b + 128]
            misc_ref[80 + 4 * layer + b : 81 + 4 * layer + b] = part
        for k in range(CONV - 1):
            at = 32 * layer + 8 * k
            for s in range(SEQ):
                misc_ref[at + s : at + s + 1] = history_ref[s, k, layer : layer + 1].astype(f32)
        at = 32 * layer + 24
        misc_ref[at : at + CONV] = taps_ref[layer].astype(f32)


def gain_row(misc_ref, layer):
    parts = [misc_ref[80 + 4 * layer + b : 81 + 4 * layer + b] for b in range(4)]
    return jnp.concatenate(parts, axis=1)


def prepare(
    token_hbm,
    weight_hbm,
    history_hbm,
    taps_hbm,
    out_ref,
    token_ref,
    weight_ref,
    history_ref,
    taps_ref,
    stack_ref,
    sems,
):
    moves = [
        pltpu.make_async_copy(source, target, sems.at[n])
        for n, (source, target) in enumerate(
            (
                (history_hbm, history_ref),
                (taps_hbm, taps_ref),
                (token_hbm, token_ref),
                (weight_hbm, weight_ref),
            )
        )
    ]
    for move in moves:
        move.start()
    for move in moves[:3]:
        move.wait()
    stack_ref[...] = jnp.zeros((128, 32), f32)
    at = 0
    for layer in range(LAYERS):
        for s in range(SEQ):
            for k in range(CONV - 1):
                stack_ref[at : at + 2] = history_ref[layer, s, k].astype(f32)
                at += 2
    for layer in range(LAYERS):
        for k in range(CONV):
            stack_ref[at : at + 2] = taps_ref[layer, k].astype(f32)
            at += 2
    turned = jnp.transpose(stack_ref[...])
    tokens = jnp.concatenate([token_ref[...].astype(f32), jnp.zeros((1, 512), f32)], axis=0)
    row, _ = row_col((4, 512))
    for g in range(GROUPS):
        both = [turned[g : g + 1], turned[GROUPS + g : GROUPS + g + 1], jnp.zeros((1, 256), f32)]
        tail = jnp.broadcast_to(jnp.concatenate(both, axis=1), (4, 512))
        out_ref[g, 0] = jnp.where(row == 3, tail, tokens).astype(bf16)

    def source(col):
        c = col % 32
        return 4 * (c % GROUPS) + 2 * (col // 32) + c // GROUPS

    order = one_hot(64, 64, source)
    moves[3].wait()
    for layer in range(LAYERS):
        cols = weight_ref[layer].reshape(64, 512)
        out_ref[:, 1 + layer] = mm(order, cols).astype(bf16).reshape(GROUPS, 4, 512)


def unpack(plane_ref, vhist_ref, vtaps_ref):
    def source(col):
        return jnp.where(col % 8 == 3, 4 * ((col // 8) % ZN) + col // 128, -1)

    small = mm(one_hot(64, 512, source), plane_ref[:, :, 0:256].reshape(512, 256))
    spread = jnp.zeros((128, 128), f32)
    row, col = row_col((64, 128))
    for nl in range(2):
        turned = jnp.transpose(small[:, 128 * nl : 128 * nl + 128]).astype(bf16)
        spread += mm(turned, jnp.where(col == 2 * row + nl, 1.0, 0.0).astype(bf16))

    def order(m):
        kind = m // 2
        old = 24 * (2 * (m // 36) + m % 2) + 8 * (kind % 3) + (kind // 3) % SEQ
        tap = 96 + 8 * (2 * ((m - 72) // 8) + m % 2) + (kind - 36) % CONV
        return jnp.where(m < 72, old, jnp.where(m < 88, tap, -1))

    rows = mm(one_hot(128, 128, order), spread.astype(bf16)).astype(bf16)
    for layer in range(LAYERS):
        for rw in range(2):
            lanes = slice(128 * rw, 128 * rw + 128)
            for k in range(CONV - 1):
                at = 24 * (2 * layer + rw) + 8 * k
                vhist_ref[layer, k, :, lanes] = rows[at : at + 8]
            at = 96 + 8 * (2 * layer + rw)
            vtaps_ref[layer, :, lanes] = rows[at : at + 8]


def middle(
    part_ref,
    misc_ref,
    vhist_ref,
    vtaps_ref,
    state_ref,
    msg_ref,
    keep_ref,
    write_ref,
    decay_ref,
    value_ref,
    vector_ref,
    *,
    layer,
):
    if layer == 0:
        total = sum(part_ref[d].astype(f32) for d in range(DN))
        place = one_hot(32, 24, place_first)
    else:
        rows = [sum(part_ref[y, d].astype(f32) for d in range(DN)) for y in range(YN)]
        total = jnp.concatenate(rows, axis=0)
        place = one_hot(32, 32, place_second)
    tail = total[:, 512:640]
    _, lane = row_col(tail.shape)
    squares = jnp.sum(jnp.where(lane == square_lane(), tail, 0.0), axis=1, keepdims=True)
    scaled = (total * lax.rsqrt(squares / D + norm_floor)).astype(bf16)
    rows = mm(place, scaled)
    gate = rows[:, 0:128]

    head = 8 * lax.axis_index("z") + 2 * lax.axis_index("y")
    tail = rows[:, 512:640]
    _, lane = row_col(tail.shape)
    first = jnp.sum(jnp.where(lane == head, tail, 0.0), axis=1, keepdims=True)
    second = jnp.sum(jnp.where(lane == head + 1, tail, 0.0), axis=1, keepdims=True)
    left = lane < HEAD_DIM
    at = 72 + 2 * layer
    raw = jnp.where(left, first, second) + misc_ref[at : at + 1]
    rate = misc_ref[at + 1 : at + 2]
    soft = jnp.maximum(raw, 0.0) + jnp.log1p(jnp.exp(-jnp.abs(raw)))
    lens = misc_ref[64:72, 0:1]
    live = [jnp.where(lens > t, 1.0, 0.0) for t in range(NEW)]
    step = [soft[8 * t : 8 * t + 8] * live[t] for t in range(NEW)]
    cumulative = []
    for t in range(NEW):
        grown = step[t] * rate
        cumulative.append(grown if t == 0 else cumulative[-1] + grown)

    at = 32 * layer + 24
    taps = [misc_ref[at + k : at + k + 1] for k in range(CONV)]
    values = conv(old_values(misc_ref, layer), taps, rows[:, 128:256])
    taps = [vtaps_ref[layer, k : k + 1].astype(f32) for k in range(CONV)]
    vectors = conv(old_vectors(vhist_ref, layer), taps, rows[:, 256:512])
    write = [v[:, 0:128] for v in vectors]
    read = [v[:, 128:256] for v in vectors]
    stepped = [values[t] * step[t] for t in range(NEW)]

    reads = jnp.concatenate(read, axis=0).astype(bf16)
    row, _ = row_col((32, 128))
    carried = jnp.zeros((32, 128), f32)
    for s in range(SEQ):
        carried = jnp.where(row % 8 == s, mm_t(reads, state_ref[0, s].astype(bf16)), carried)

    mixed = []
    for t in range(NEW):
        y = jnp.exp(-cumulative[t]) * carried[8 * t : 8 * t + 8]
        for u in range(t + 1):
            score = jnp.sum(read[t] * write[u], axis=1, keepdims=True)
            y = y + score * jnp.exp(cumulative[u] - cumulative[t]) * stepped[u]
        mixed.append(y * silu(gate[8 * t : 8 * t + 8]) * live[t])
    mixed = jnp.concatenate(mixed, axis=0).astype(bf16)
    row, col = row_col((32, 32))
    i = row % 4
    n = 12 * ((row // 4) % 2) + 3 * (row // 8) + i
    pick = (col == 8 * (n % NEW) + n // NEW) & (i < 3)
    ordered = mm(jnp.where(pick, 1.0, 0.0).astype(bf16), mixed).astype(bf16)
    for y in range(YN):
        for d in range(DN):
            msg_ref[y * DN + d] = ordered[8 * y : 8 * y + 8]

    last = cumulative[-1]
    for t in range(NEW):
        keep_ref[8 * t : 8 * t + 8] = jnp.exp(cumulative[t] - last) * stepped[t]
        write_ref[8 * t : 8 * t + 8] = write[t]
    decay_ref[...] = jnp.exp(-last)
    for out_ref, old, lo, hi in (
        (value_ref, old_values(misc_ref, layer), 128, 256),
        (vector_ref, old_vectors(vhist_ref, layer), 256, 512),
    ):
        padded = old + [rows[8 * t : 8 * t + 8, lo:hi] for t in range(NEW)]
        for k in range(CONV - 1):
            chosen = padded[k + 1]
            for r in range(k + 2, k + NEW + 1):
                chosen = jnp.where(lens + k == r, padded[r], chosen)
            out_ref[k] = chosen.astype(bf16)


def finish(keep_ref, write_ref, decay_ref, state_ref, *rest):
    next_ref = rest[-1]
    kept = jnp.transpose(keep_ref[...])
    _, col = row_col(kept.shape)
    write = write_ref[...].astype(bf16)
    for s in range(SEQ):
        fresh = mm(jnp.where(col % 8 == s, kept, 0.0).astype(bf16), write)
        for h in range(2):
            at = slice(HEAD_DIM * h, HEAD_DIM * h + HEAD_DIM)
            decay = decay_ref[s : s + 1, HEAD_DIM * h : HEAD_DIM * h + 1]
            next_ref[0, s, at] = state_ref[0, s, at] * decay + fresh[at]


def call(kernel, shapes, *args):
    vmem = pl.BlockSpec(memory_space=pltpu.VMEM)
    outs = [jax.ShapeDtypeStruct(shape, dtype) for shape, dtype in shapes]
    results = pl.pallas_call(
        kernel,
        out_shape=outs,
        in_specs=[vmem] * len(args),
        out_specs=[vmem] * len(outs),
        compiler_params=pltpu.CompilerParams(vmem_limit_bytes=12 << 20),
    )(*args)
    return results[0] if len(outs) == 1 else results


def ending(update_ref, token_ref, out_ref, vector_ref):
    total = sum(update_ref[z].astype(f32) for z in range(ZN))
    out_ref[...] = (total[0:3] + token_ref[...].astype(f32)).astype(bf16)
    rows = [update_ref[z, 3:4, 0:256].astype(f32) for z in range(ZN)]
    rows = jnp.concatenate(rows, axis=0)
    both = jnp.concatenate(
        [jnp.transpose(rows[:, 0:128]), jnp.transpose(rows[:, 128:256])], axis=1
    )
    for layer in range(LAYERS):
        for k in range(CONV - 1):
            for s in range(SEQ):
                at = 24 * layer + 8 * k + s
                pair = jnp.concatenate([both[at : at + 1], both[48 + at : 49 + at]], axis=0)
                vector_ref[layer, s, k] = pair.astype(bf16)


def close(layer, *args):
    vmem = pl.BlockSpec(memory_space=pltpu.VMEM)
    return pl.pallas_call(
        finish,
        grid=(1,),
        out_shape=jax.ShapeDtypeStruct((LAYERS, SEQ, 128, 128), f32),
        in_specs=[vmem] * 4 + [pl.BlockSpec(memory_space=pl.ANY)] * (len(args) - 4),
        out_specs=pl.BlockSpec((1, SEQ, 128, 128), lambda i: (layer, 0, 0, 0)),
        input_output_aliases={4: 0} if layer else {},
        compiler_params=pltpu.CompilerParams(vmem_limit_bytes=12 << 20),
    )(*args)


def from_y(value, k):
    return lax.ppermute(value, "y", [(i, (i + k) % YN) for i in range(YN)])


def body(
    tokens,
    lengths,
    norm_gain,
    gate_weight,
    value_weight,
    vector_weight,
    step_weight,
    step_bias,
    decay_rate,
    value_taps,
    vector_taps,
    out_weight,
    recurrent_state,
    value_history,
    vector_history,
):
    first = pl.pallas_call(
        prepare,
        out_shape=jax.ShapeDtypeStruct((ZN, 3, 4, 512), bf16),
        in_specs=[pl.BlockSpec(memory_space=pltpu.MemorySpace.HBM)] * 4,
        out_specs=pl.BlockSpec(memory_space=pltpu.VMEM),
        scratch_shapes=[
            pltpu.VMEM((3, 512), bf16),
            pltpu.VMEM((2, 2, 32, 512), bf16),
            pltpu.VMEM((2, SEQ, 3, 2, 32), bf16),
            pltpu.VMEM((2, CONV, 2, 32), bf16),
            pltpu.VMEM((128, 32), f32),
            pltpu.SemaphoreType.DMA((4,)),
        ],
    )(tokens, vector_weight.transpose(0, 2, 3, 1), vector_history, vector_taps)
    first, outs, lens = lax.optimization_barrier(
        (first, out_weight.reshape(256, 512), lengths)
    )
    first = exchange(first, "z")
    early = jnp.concatenate([gate_weight[0], value_weight[0], step_weight[0]], axis=1)
    out_2 = from_y(outs, 2)
    out_3 = from_y(outs, 3)
    misc, base = pl.pallas_call(
        setup,
        out_shape=[jax.ShapeDtypeStruct((88, 128), f32), jax.ShapeDtypeStruct((1280, 128), bf16)],
        in_specs=[pl.BlockSpec(memory_space=pltpu.SMEM)]
        + [pl.BlockSpec(memory_space=pltpu.MemorySpace.HBM)] * 7,
        out_specs=[pl.BlockSpec(memory_space=pltpu.VMEM)] * 2,
        scratch_shapes=[
            pltpu.VMEM((2, 512), f32),
            pltpu.VMEM((2, 2), f32),
            pltpu.VMEM((2, 2), f32),
            pltpu.VMEM((2, CONV, 128), bf16),
            pltpu.VMEM((SEQ, 3, 2, 128), bf16),
            pltpu.SemaphoreType.DMA((7,)),
        ],
    )(
        lens,
        norm_gain,
        step_bias,
        decay_rate,
        value_taps,
        value_history.transpose(1, 2, 0, 3),
        gate_weight,
        value_weight,
    )
    plane = exchange(copies(first[:, :2], YN), "y").reshape(128, 4, 512)
    out_1 = from_y(outs, 1)
    outs = [outs, out_1, out_2, out_3]
    blocks = first[:, 2].reshape(64, 4, 128).transpose(1, 0, 2).reshape(256, 128)
    later = lax.dynamic_update_slice(base, blocks, (1024, 0))
    vhist, vtaps = call(unpack, [((2, 3, 8, 256), bf16), ((2, 8, 256), bf16)], plane)

    def mid(part, layer, pieces, old, *done):
        msg, keep, write, decay, value, vector = call(
            functools.partial(middle, layer=layer),
            [
                ((YN * DN, 8, 128), bf16),
                ((32, 128), f32),
                ((32, 128), f32),
                ((8, 128), f32),
                ((3, 8, 128), bf16),
                ((3, 8, 256), bf16),
            ],
                        part,
            misc,
            vhist,
            vtaps,
            old,
        )
        after = close(layer, keep, write, decay, old, *done)
        msg, pieces = lax.optimization_barrier((msg, pieces))
        msg = exchange(msg, ("y", "dp"))
        return msg.reshape(YN, DN * 8, 128), pieces, (after, value, vector)

    part = call(
        first_projection,
        [((DN, 24, COLS), bf16)],
                plane,
        misc,
        early,
    )
    old = recurrent_state[:1]
    part = exchange(part, "dp")
    later_2 = from_y(later, 2)
    mixed, outs, (state, value0, vector0) = mid(part, 0, outs, old.reshape(1, SEQ, 128, 128))
    later_3 = from_y(later, 3)
    update = call(
        functools.partial(out_projection, first_row=0),
        [((ZN, 4, 512), bf16)],
                mixed,
        *outs,
    )
    update = exchange(update, "z")
    later_1 = from_y(later, 1)
    update = jnp.sum(update.astype(f32), axis=0)[:3]
    token_rows = (tokens.astype(f32) + update).astype(bf16)
    quarter = copies(jnp.pad(token_rows, ((0, 1), (0, 0))), ZN)
    quarter, later_state = lax.optimization_barrier((quarter, recurrent_state))
    quarter = exchange(quarter, "z").reshape(64, 512)
    later = [later, later_1, later_2, later_3]
    part = call(
        second_projection,
        [((YN, 64, COLS), bf16)],
                quarter,
        misc,
        step_weight[1:],
        *later,
    )
    part = exchange(part.reshape(YN * DN, 8, COLS), ("y", "dp"))
    part = part.reshape(YN, DN, 8, COLS)
    mixed, outs, (state, value1, vector1) = mid(part, 1, outs, later_state[1:].reshape(1, SEQ, 128, 128), state)
    update = call(
        functools.partial(out_projection, first_row=128),
        [((ZN, 4, 512), bf16)],
                mixed,
        *outs,
        vector0,
        vector1,
    )
    update = exchange(update, "z")
    token_rows, next_vector = call(
        ending,
        [((3, 512), bf16), ((LAYERS, SEQ, CONV - 1, 2, 32), bf16)],
        update,
        token_rows,
    )
    return (
        token_rows,
        state.reshape(recurrent_state.shape),
        jnp.stack([value0, value1])[:, :, :SEQ].transpose(0, 2, 1, 3),
        next_vector,
    )


def solution(mesh):
    grid = Mesh(mesh.devices.reshape(ZN, YN, DN), ("z", "y", "dp"))
    tp = ("z", "y")

    return jax.shard_map(
        body,
        mesh=grid,
        in_specs=(
            P(tp, "dp"),
            P("dp"),
            P(None, "dp"),
            P(None, "dp", tp),
            P(None, "dp", tp),
            P(None, "dp", None, tp),
            P(None, "dp", None),
            P(None, tp),
            P(None, tp),
            P(None, None, tp),
            P(None, None, None, tp),
            P(None, tp, "dp"),
            P(None, "dp", tp, None, None),
            P(None, "dp", None, tp),
            P(None, "dp", None, None, tp),
        ),
        out_specs=(
            P(tp, "dp"),
            P(None, "dp", tp, None, None),
            P(None, "dp", None, tp),
            P(None, "dp", None, None, tp),
        ),
        check_vma=False,
    )
```

```python
import functools

import jax
import jax.numpy as jnp
from jax import lax
from jax.experimental import pallas as pl
from jax.experimental.pallas import tpu as pltpu
from jax.sharding import Mesh, PartitionSpec as P

D = 4096
HEADS = 128
HEAD_DIM = 64
GROUPS = 16
CONV = 4
NEW = 4
LAYERS = 2
norm_floor = 0.1

ZN, YN, DN = 16, 4, 8
SEQ = 6
bf16 = jnp.bfloat16
f32 = jnp.float32
COLS = 640


def exchange(pieces, axis):
    return lax.all_to_all(pieces, axis, 0, 0, tiled=True)


def copies(value, peers):
    return jnp.broadcast_to(value[None], (peers, *value.shape))


def one_hot(rows, cols, target):
    row = lax.broadcasted_iota(jnp.int32, (rows, cols), 0)
    col = lax.broadcasted_iota(jnp.int32, (rows, cols), 1)
    return jnp.where(row == target(col), 1.0, 0.0).astype(bf16)


def mm(a, b):
    return lax.dot_general(a, b, (((1,), (0,)), ((), ())), preferred_element_type=f32)


def mm_t(a, b):
    return lax.dot_general(a, b, (((1,), (1,)), ((), ())), preferred_element_type=f32)


def normed_rows(rows, gain):
    widened = rows.astype(f32)
    squares = jnp.sum(widened * widened, axis=1, keepdims=True)
    return (widened * gain).astype(bf16), squares


def square_lane():
    return (8 * lax.axis_index("z") + 64) % HEADS


def step_lanes(normed, squares, step_w):
    step = mm(normed, step_w)
    lane = lax.broadcasted_iota(jnp.int32, step.shape, 1)
    return jnp.where(lane == square_lane(), squares, step)


def first_projection(plane_ref, misc_ref, weight_ref, out_ref):
    plane = plane_ref[...].reshape(512, 512)

    def token_source(col):
        i = col % 8
        return jnp.where(i < 3, 12 * ((col // 8) % ZN) + 3 * (col // 128) + i, -1)

    def vector_source(col):
        j = col % 8 - 4
        n = 8 * ((col // 8) % ZN) + 2 * (col // 128) + j % 2
        return jnp.where((j >= 0) & (j < 4), 128 * (j // 2) + n, -1)

    rows = mm(one_hot(192, 512, token_source), plane).astype(bf16)
    vector_w = mm(one_hot(256, 512, vector_source), plane).astype(bf16)
    normed, squares = normed_rows(rows, gain_row(misc_ref, 0))
    parts = [
        mm(normed, weight_ref[:, 0:128]),
        mm(normed, weight_ref[:, 128:256]),
        mm_t(normed, vector_w),
        step_lanes(normed, squares, weight_ref[:, 256:384]),
    ]
    at = 0
    for part in parts:
        width = part.shape[1]
        out_ref[:, :, at : at + width] = part.astype(bf16).reshape(DN, 24, width)
        at += width


def second_projection(rows_ref, misc_ref, step_ref, w0, w1, w2, w3, out_ref):
    y = lax.axis_index("y")
    normed, squares = normed_rows(rows_ref[...], gain_row(misc_ref, 1))
    pieces = [w0, w1, w2, w3]

    def source(col):
        j = col % 4
        n = 8 * ((col // 4) % ZN) + 2 * ((y - col // 64) % YN) + j % 2
        return 128 * (j // 2) + n

    stacked = jnp.concatenate(
        [
            jnp.concatenate([w[1024 + 64 * b : 1088 + 64 * b] for b in range(4)], axis=1)
            for w in pieces
        ],
        axis=0,
    )
    vector_w = mm(one_hot(256, 256, source), stacked).astype(bf16)
    vector = mm_t(normed, vector_w).astype(bf16)
    extra = step_lanes(normed, squares, step_ref[0]).astype(bf16)
    for k, w in enumerate(pieces):
        to = (y - k) % YN
        for n in range(2):
            total = mm(normed, w[512 * n : 512 * n + 512])
            out_ref[to, :, 128 * n : 128 * n + 128] = total.astype(bf16)
        out_ref[to, :, 256:512] = vector
        out_ref[to, :, 512:640] = extra


def out_projection(mixed_ref, w0, w1, w2, w3, *rest, first_row):
    y = lax.axis_index("y")
    total = jnp.zeros((64, 512), f32)
    for k, w in enumerate([w0, w1, w2, w3]):
        total += mm(mixed_ref[(y - k) % YN], w[first_row : first_row + 128])
    if len(rest) == 1:
        rest[0][...] = total.astype(bf16).reshape(ZN, 4, 512)
        return
    *vector_refs, out_ref = rest
    old = [ref[k] for ref in vector_refs for k in range(CONV - 1)]
    returned = [v[:, 0:128].astype(f32) for v in old] + [v[:, 128:256].astype(f32) for v in old]
    returned = jnp.concatenate([*returned, jnp.zeros((32, 128), f32)], axis=0).astype(bf16)
    slot = one_hot(64, ZN, lambda col: 4 * col + 3)
    halves = []
    for nl in range(2):
        row = lax.broadcasted_iota(jnp.int32, (ZN, 128), 0)
        col = lax.broadcasted_iota(jnp.int32, (ZN, 128), 1)
        chosen = jnp.where(col == 8 * row + 2 * y + nl, 1.0, 0.0).astype(bf16)
        halves.append(mm_t(chosen, returned).astype(bf16))
    tail = jnp.concatenate(halves, axis=1)
    left = (total[:, 0:256] + mm(slot, tail)).astype(bf16)
    whole = jnp.concatenate([left, total[:, 256:512].astype(bf16)], axis=1)
    out_ref[...] = whole.reshape(ZN, 4, 512)


def row_col(shape):
    return (
        lax.broadcasted_iota(jnp.int32, shape, 0),
        lax.broadcasted_iota(jnp.int32, shape, 1),
    )


def silu(x):
    return x * jax.nn.sigmoid(x)


def place_first(col):
    return 8 * (col % NEW) + col // NEW


def place_second(col):
    i = col % 4
    n = 12 * ((col // 4) % 2) + 3 * (col // 8) + i
    return jnp.where(i < 3, 8 * (n % NEW) + n // NEW, -1)


def conv(old, taps, fresh):
    rows = old + [fresh[8 * t : 8 * t + 8] for t in range(NEW)]
    return [silu(sum(rows[t + k] * taps[k] for k in range(CONV))) for t in range(NEW)]


def old_values(misc_ref, layer):
    return [misc_ref[32 * layer + 8 * k : 32 * layer + 8 * k + 8] for k in range(CONV - 1)]


def old_vectors(vhist_ref, layer):
    return [vhist_ref[layer, k].astype(f32) for k in range(CONV - 1)]


def setup(
    len_ref,
    gain_hbm,
    bias_hbm,
    rate_hbm,
    taps_hbm,
    history_hbm,
    gate_hbm,
    value_hbm,
    misc_ref,
    base_ref,
    gain_ref,
    bias_ref,
    rate_ref,
    taps_ref,
    history_ref,
    sems,
):
    pairs = (
        (gain_hbm, gain_ref),
        (bias_hbm, bias_ref),
        (rate_hbm, rate_ref),
        (taps_hbm, taps_ref),
        (history_hbm, history_ref),
        (gate_hbm.at[1], base_ref.at[0:512]),
        (value_hbm.at[1], base_ref.at[512:1024]),
    )
    moves = [pltpu.make_async_copy(a, b, sems.at[n]) for n, (a, b) in enumerate(pairs)]
    for move in moves:
        move.start()
    row, lane = row_col((8, 128))
    lens = jnp.zeros((8, 128), f32)
    for s in range(SEQ):
        lens = jnp.where(row == s, len_ref[s].astype(f32), lens)
    misc_ref[0:64] = jnp.zeros((64, 128), f32)
    misc_ref[64:72] = lens
    misc_ref[72:80] = jnp.zeros((8, 128), f32)
    for move in moves:
        move.wait()
    left = lane[0:1] < HEAD_DIM
    for layer in range(LAYERS):
        for n, ref in enumerate((bias_ref, rate_ref)):
            both = jnp.where(left, ref[layer : layer + 1, 0:1], ref[layer : layer + 1, 1:2])
            misc_ref[72 + 2 * layer + n : 73 + 2 * layer + n] = both
        for b in range(4):
            part = gain_ref[layer : layer + 1, 128 * b : 128 * b + 128]
            misc_ref[80 + 4 * layer + b : 81 + 4 * layer + b] = part
        for k in range(CONV - 1):
            at = 32 * layer + 8 * k
            for s in range(SEQ):
                misc_ref[at + s : at + s + 1] = history_ref[s, k, layer : layer + 1].astype(f32)
        at = 32 * layer + 24
        misc_ref[at : at + CONV] = taps_ref[layer].astype(f32)


def gain_row(misc_ref, layer):
    parts = [misc_ref[80 + 4 * layer + b : 81 + 4 * layer + b] for b in range(4)]
    return jnp.concatenate(parts, axis=1)


def prepare(
    token_hbm,
    weight_hbm,
    history_hbm,
    taps_hbm,
    out_ref,
    token_ref,
    weight_ref,
    history_ref,
    taps_ref,
    stack_ref,
    sems,
):
    moves = [
        pltpu.make_async_copy(source, target, sems.at[n])
        for n, (source, target) in enumerate(
            (
                (history_hbm, history_ref),
                (taps_hbm, taps_ref),
                (token_hbm, token_ref),
                (weight_hbm, weight_ref),
            )
        )
    ]
    for move in moves:
        move.start()
    for move in moves[:3]:
        move.wait()
    stack_ref[...] = jnp.zeros((128, 32), f32)
    at = 0
    for layer in range(LAYERS):
        for s in range(SEQ):
            for k in range(CONV - 1):
                stack_ref[at : at + 2] = history_ref[layer, s, k].astype(f32)
                at += 2
    for layer in range(LAYERS):
        for k in range(CONV):
            stack_ref[at : at + 2] = taps_ref[layer, k].astype(f32)
            at += 2
    turned = jnp.transpose(stack_ref[...])
    tokens = jnp.concatenate([token_ref[...].astype(f32), jnp.zeros((1, 512), f32)], axis=0)
    row, _ = row_col((4, 512))
    for g in range(GROUPS):
        both = [turned[g : g + 1], turned[GROUPS + g : GROUPS + g + 1], jnp.zeros((1, 256), f32)]
        tail = jnp.broadcast_to(jnp.concatenate(both, axis=1), (4, 512))
        out_ref[g, 0] = jnp.where(row == 3, tail, tokens).astype(bf16)

    def source(col):
        c = col % 32
        return 4 * (c % GROUPS) + 2 * (col // 32) + c // GROUPS

    order = one_hot(64, 64, source)
    moves[3].wait()
    for layer in range(LAYERS):
        cols = weight_ref[layer].reshape(64, 512)
        out_ref[:, 1 + layer] = mm(order, cols).astype(bf16).reshape(GROUPS, 4, 512)


def unpack(plane_ref, vhist_ref, vtaps_ref):
    def source(col):
        return jnp.where(col % 8 == 3, 4 * ((col // 8) % ZN) + col // 128, -1)

    small = mm(one_hot(64, 512, source), plane_ref[:, :, 0:256].reshape(512, 256))
    spread = jnp.zeros((128, 128), f32)
    row, col = row_col((64, 128))
    for nl in range(2):
        turned = jnp.transpose(small[:, 128 * nl : 128 * nl + 128]).astype(bf16)
        spread += mm(turned, jnp.where(col == 2 * row + nl, 1.0, 0.0).astype(bf16))

    def order(m):
        kind = m // 2
        old = 24 * (2 * (m // 36) + m % 2) + 8 * (kind % 3) + (kind // 3) % SEQ
        tap = 96 + 8 * (2 * ((m - 72) // 8) + m % 2) + (kind - 36) % CONV
        return jnp.where(m < 72, old, jnp.where(m < 88, tap, -1))

    rows = mm(one_hot(128, 128, order), spread.astype(bf16)).astype(bf16)
    for layer in range(LAYERS):
        for rw in range(2):
            lanes = slice(128 * rw, 128 * rw + 128)
            for k in range(CONV - 1):
                at = 24 * (2 * layer + rw) + 8 * k
                vhist_ref[layer, k, :, lanes] = rows[at : at + 8]
            at = 96 + 8 * (2 * layer + rw)
            vtaps_ref[layer, :, lanes] = rows[at : at + 8]


def middle(
    part_ref,
    misc_ref,
    vhist_ref,
    vtaps_ref,
    state_ref,
    msg_ref,
    keep_ref,
    write_ref,
    decay_ref,
    value_ref,
    vector_ref,
    *,
    layer,
):
    if layer == 0:
        total = sum(part_ref[d].astype(f32) for d in range(DN))
        place = one_hot(32, 24, place_first)
    else:
        rows = [sum(part_ref[y, d].astype(f32) for d in range(DN)) for y in range(YN)]
        total = jnp.concatenate(rows, axis=0)
        place = one_hot(32, 32, place_second)
    tail = total[:, 512:640]
    _, lane = row_col(tail.shape)
    squares = jnp.sum(jnp.where(lane == square_lane(), tail, 0.0), axis=1, keepdims=True)
    scaled = (total * lax.rsqrt(squares / D + norm_floor)).astype(bf16)
    rows = mm(place, scaled)
    gate = rows[:, 0:128]

    head = 8 * lax.axis_index("z") + 2 * lax.axis_index("y")
    tail = rows[:, 512:640]
    _, lane = row_col(tail.shape)
    first = jnp.sum(jnp.where(lane == head, tail, 0.0), axis=1, keepdims=True)
    second = jnp.sum(jnp.where(lane == head + 1, tail, 0.0), axis=1, keepdims=True)
    left = lane < HEAD_DIM
    at = 72 + 2 * layer
    raw = jnp.where(left, first, second) + misc_ref[at : at + 1]
    rate = misc_ref[at + 1 : at + 2]
    soft = jnp.maximum(raw, 0.0) + jnp.log1p(jnp.exp(-jnp.abs(raw)))
    lens = misc_ref[64:72, 0:1]
    live = [jnp.where(lens > t, 1.0, 0.0) for t in range(NEW)]
    step = [soft[8 * t : 8 * t + 8] * live[t] for t in range(NEW)]
    cumulative = []
    for t in range(NEW):
        grown = step[t] * rate
        cumulative.append(grown if t == 0 else cumulative[-1] + grown)

    at = 32 * layer + 24
    taps = [misc_ref[at + k : at + k + 1] for k in range(CONV)]
    values = conv(old_values(misc_ref, layer), taps, rows[:, 128:256])
    taps = [vtaps_ref[layer, k : k + 1].astype(f32) for k in range(CONV)]
    vectors = conv(old_vectors(vhist_ref, layer), taps, rows[:, 256:512])
    write = [v[:, 0:128] for v in vectors]
    read = [v[:, 128:256] for v in vectors]
    stepped = [values[t] * step[t] for t in range(NEW)]

    reads = jnp.concatenate(read, axis=0).astype(bf16)
    row, _ = row_col((32, 128))
    carried = jnp.zeros((32, 128), f32)
    for s in range(SEQ):
        carried = jnp.where(row % 8 == s, mm_t(reads, state_ref[0, s].astype(bf16)), carried)

    mixed = []
    for t in range(NEW):
        y = jnp.exp(-cumulative[t]) * carried[8 * t : 8 * t + 8]
        for u in range(t + 1):
            score = jnp.sum(read[t] * write[u], axis=1, keepdims=True)
            y = y + score * jnp.exp(cumulative[u] - cumulative[t]) * stepped[u]
        mixed.append(y * silu(gate[8 * t : 8 * t + 8]) * live[t])
    mixed = jnp.concatenate(mixed, axis=0).astype(bf16)
    row, col = row_col((32, 32))
    i = row % 4
    n = 12 * ((row // 4) % 2) + 3 * (row // 8) + i
    pick = (col == 8 * (n % NEW) + n // NEW) & (i < 3)
    ordered = mm(jnp.where(pick, 1.0, 0.0).astype(bf16), mixed).astype(bf16)
    for y in range(YN):
        for d in range(DN):
            msg_ref[y * DN + d] = ordered[8 * y : 8 * y + 8]

    last = cumulative[-1]
    for t in range(NEW):
        keep_ref[8 * t : 8 * t + 8] = jnp.exp(cumulative[t] - last) * stepped[t]
        write_ref[8 * t : 8 * t + 8] = write[t]
    decay_ref[...] = jnp.exp(-last)
    for out_ref, old, lo, hi in (
        (value_ref, old_values(misc_ref, layer), 128, 256),
        (vector_ref, old_vectors(vhist_ref, layer), 256, 512),
    ):
        padded = old + [rows[8 * t : 8 * t + 8, lo:hi] for t in range(NEW)]
        for k in range(CONV - 1):
            chosen = padded[k + 1]
            for r in range(k + 2, k + NEW + 1):
                chosen = jnp.where(lens + k == r, padded[r], chosen)
            out_ref[k] = chosen.astype(bf16)


def finish(keep_ref, write_ref, decay_ref, state_ref, *rest):
    next_ref = rest[-1]
    kept = jnp.transpose(keep_ref[...])
    _, col = row_col(kept.shape)
    write = write_ref[...].astype(bf16)
    for s in range(SEQ):
        fresh = mm(jnp.where(col % 8 == s, kept, 0.0).astype(bf16), write)
        for h in range(2):
            at = slice(HEAD_DIM * h, HEAD_DIM * h + HEAD_DIM)
            decay = decay_ref[s : s + 1, HEAD_DIM * h : HEAD_DIM * h + 1]
            next_ref[0, s, at] = state_ref[0, s, at] * decay + fresh[at]


def call(kernel, shapes, *args):
    vmem = pl.BlockSpec(memory_space=pltpu.VMEM)
    outs = [jax.ShapeDtypeStruct(shape, dtype) for shape, dtype in shapes]
    results = pl.pallas_call(
        kernel,
        out_shape=outs,
        in_specs=[vmem] * len(args),
        out_specs=[vmem] * len(outs),
        compiler_params=pltpu.CompilerParams(vmem_limit_bytes=12 << 20),
    )(*args)
    return results[0] if len(outs) == 1 else results


def ending(update_ref, token_ref, out_ref, vector_ref):
    total = sum(update_ref[z].astype(f32) for z in range(ZN))
    out_ref[...] = (total[0:3] + token_ref[0:3].astype(f32)).astype(bf16)
    rows = [update_ref[z, 3:4, 0:256].astype(f32) for z in range(ZN)]
    rows = jnp.concatenate(rows, axis=0)
    both = jnp.concatenate(
        [jnp.transpose(rows[:, 0:128]), jnp.transpose(rows[:, 128:256])], axis=1
    )
    for layer in range(LAYERS):
        for k in range(CONV - 1):
            for s in range(SEQ):
                at = 24 * layer + 8 * k + s
                pair = jnp.concatenate([both[at : at + 1], both[48 + at : 49 + at]], axis=0)
                vector_ref[layer, s, k] = pair.astype(bf16)


def close(layer, *args):
    vmem = pl.BlockSpec(memory_space=pltpu.VMEM)
    return pl.pallas_call(
        finish,
        grid=(1,),
        out_shape=jax.ShapeDtypeStruct((LAYERS, SEQ, 128, 128), f32),
        in_specs=[vmem] * 4 + [pl.BlockSpec(memory_space=pl.ANY)] * (len(args) - 4),
        out_specs=pl.BlockSpec((1, SEQ, 128, 128), lambda i: (layer, 0, 0, 0)),
        input_output_aliases={4: 0} if layer else {},
        compiler_params=pltpu.CompilerParams(vmem_limit_bytes=12 << 20),
    )(*args)


def from_y(value, k):
    return lax.ppermute(value, "y", [(i, (i + k) % YN) for i in range(YN)])


def body(
    tokens,
    lengths,
    norm_gain,
    gate_weight,
    value_weight,
    vector_weight,
    step_weight,
    step_bias,
    decay_rate,
    value_taps,
    vector_taps,
    out_weight,
    recurrent_state,
    value_history,
    vector_history,
):
    first = pl.pallas_call(
        prepare,
        out_shape=jax.ShapeDtypeStruct((ZN, 3, 4, 512), bf16),
        in_specs=[pl.BlockSpec(memory_space=pltpu.MemorySpace.HBM)] * 4,
        out_specs=pl.BlockSpec(memory_space=pltpu.VMEM),
        scratch_shapes=[
            pltpu.VMEM((3, 512), bf16),
            pltpu.VMEM((2, 2, 32, 512), bf16),
            pltpu.VMEM((2, SEQ, 3, 2, 32), bf16),
            pltpu.VMEM((2, CONV, 2, 32), bf16),
            pltpu.VMEM((128, 32), f32),
            pltpu.SemaphoreType.DMA((4,)),
        ],
    )(tokens, vector_weight.transpose(0, 2, 3, 1), vector_history, vector_taps)
    first, outs, lens = lax.optimization_barrier(
        (first, out_weight.reshape(256, 512), lengths)
    )
    first = exchange(first, "z")
    early = jnp.concatenate([gate_weight[0], value_weight[0], step_weight[0]], axis=1)
    own = jnp.pad(tokens, ((0, 1), (0, 0)))
    own = lax.optimization_barrier(own)
    out_2 = from_y(outs, 2)
    out_3 = from_y(outs, 3)
    misc, base = pl.pallas_call(
        setup,
        out_shape=[jax.ShapeDtypeStruct((88, 128), f32), jax.ShapeDtypeStruct((1280, 128), bf16)],
        in_specs=[pl.BlockSpec(memory_space=pltpu.SMEM)]
        + [pl.BlockSpec(memory_space=pltpu.MemorySpace.HBM)] * 7,
        out_specs=[pl.BlockSpec(memory_space=pltpu.VMEM)] * 2,
        scratch_shapes=[
            pltpu.VMEM((2, 512), f32),
            pltpu.VMEM((2, 2), f32),
            pltpu.VMEM((2, 2), f32),
            pltpu.VMEM((2, CONV, 128), bf16),
            pltpu.VMEM((SEQ, 3, 2, 128), bf16),
            pltpu.SemaphoreType.DMA((7,)),
        ],
    )(
        lens,
        norm_gain,
        step_bias,
        decay_rate,
        value_taps,
        value_history.transpose(1, 2, 0, 3),
        gate_weight,
        value_weight,
    )
    plane = exchange(copies(first[:, :2], YN), "y").reshape(128, 4, 512)
    out_1 = from_y(outs, 1)
    outs = [outs, out_1, out_2, out_3, own]
    blocks = first[:, 2].reshape(64, 4, 128).transpose(1, 0, 2).reshape(256, 128)
    later = lax.dynamic_update_slice(base, blocks, (1024, 0))
    vhist, vtaps = call(unpack, [((2, 3, 8, 256), bf16), ((2, 8, 256), bf16)], plane)

    def mid(part, layer, pieces, old, *done):
        msg, keep, write, decay, value, vector = call(
            functools.partial(middle, layer=layer),
            [
                ((YN * DN, 8, 128), bf16),
                ((32, 128), f32),
                ((32, 128), f32),
                ((8, 128), f32),
                ((3, 8, 128), bf16),
                ((3, 8, 256), bf16),
            ],
                        part,
            misc,
            vhist,
            vtaps,
            old,
        )
        after = close(layer, keep, write, decay, old, *done)
        msg, pieces = lax.optimization_barrier((msg, pieces))
        msg = exchange(msg, ("y", "dp"))
        return msg.reshape(YN, DN * 8, 128), pieces, (after, value, vector)

    part = call(
        first_projection,
        [((DN, 24, COLS), bf16)],
                plane,
        misc,
        early,
    )
    old = recurrent_state[:1]
    part = exchange(part, "dp")
    later_2 = from_y(later, 2)
    mixed, outs, (state, value0, vector0) = mid(part, 0, outs, old.reshape(1, SEQ, 128, 128))
    *outs, own = outs
    later_3 = from_y(later, 3)
    update = call(
        functools.partial(out_projection, first_row=0),
        [((ZN, 4, 512), bf16)],
                mixed,
        *outs,
    )
    update = exchange(update, "z")
    later_1 = from_y(later, 1)
    token_rows = (own.astype(f32) + jnp.sum(update.astype(f32), axis=0)).astype(bf16)
    quarter = copies(token_rows, ZN)
    quarter, later_state = lax.optimization_barrier((quarter, recurrent_state))
    quarter = exchange(quarter, "z").reshape(64, 512)
    later = [later, later_1, later_2, later_3]
    part = call(
        second_projection,
        [((YN, 64, COLS), bf16)],
                quarter,
        misc,
        step_weight[1:],
        *later,
    )
    part = exchange(part.reshape(YN * DN, 8, COLS), ("y", "dp"))
    part = part.reshape(YN, DN, 8, COLS)
    mixed, outs, (state, value1, vector1) = mid(part, 1, outs, later_state[1:].reshape(1, SEQ, 128, 128), state)
    update = call(
        functools.partial(out_projection, first_row=128),
        [((ZN, 4, 512), bf16)],
                mixed,
        *outs,
        vector0,
        vector1,
    )
    update = exchange(update, "z")
    token_rows, next_vector = call(
        ending,
        [((3, 512), bf16), ((LAYERS, SEQ, CONV - 1, 2, 32), bf16)],
        update,
        token_rows,
    )
    return (
        token_rows,
        state.reshape(recurrent_state.shape),
        jnp.stack([value0, value1])[:, :, :SEQ].transpose(0, 2, 1, 3),
        next_vector,
    )


def solution(mesh):
    grid = Mesh(mesh.devices.reshape(ZN, YN, DN), ("z", "y", "dp"))
    tp = ("z", "y")

    return jax.shard_map(
        body,
        mesh=grid,
        in_specs=(
            P(tp, "dp"),
            P("dp"),
            P(None, "dp"),
            P(None, "dp", tp),
            P(None, "dp", tp),
            P(None, "dp", None, tp),
            P(None, "dp", None),
            P(None, tp),
            P(None, tp),
            P(None, None, tp),
            P(None, None, None, tp),
            P(None, tp, "dp"),
            P(None, "dp", tp, None, None),
            P(None, "dp", None, tp),
            P(None, "dp", None, None, tp),
        ),
        out_specs=(
            P(tp, "dp"),
            P(None, "dp", tp, None, None),
            P(None, "dp", None, tp),
            P(None, "dp", None, None, tp),
        ),
        check_vma=False,
    )
```
